256 devices in a mesh: grp: 2 (over y), sp: 32 (over z, core), tp: 4 (over x).
Axes of the slice: x: 4, y: 2, z: 16, core: 2. Of those that a mesh axis runs over, the one named last changes fastest.
The devices are a block of a 4x16x16 slice.
Arguments:
- query_rows: bfloat16 [32768, 1024], P(('grp', 'sp'), 'tp'), parts along dimension 0, may hold values from -128 to 128
- key_rows: bfloat16 [32768, 256], P(('grp', 'sp'), 'tp'), parts along dimension 0, may hold values from -4 to 4
- value_rows: bfloat16 [32768, 256], P(('grp', 'sp'), 'tp'), parts along dimension 0, may hold values from -6 to 6
- sink_logits: float32 [16], P('tp'), may hold values from 3 to 7
- residual: bfloat16 [32768, 2048], P(('grp', 'sp', 'tp')), parts along dimension 0, may hold values from -6 to 6
- out_weight: bfloat16 [1024, 2048], P('tp'), may hold values from -0.1875 to 0.1875
- norm_gain: float32 [2048], replicated, may hold values from 0.1 to 1.9
- gate_weight: bfloat16 [128, 2048, 512], P(('sp', 'tp')), may hold values from -0.125 to 0.125
- up_weight: bfloat16 [128, 2048, 512], P(('sp', 'tp')), may hold values from -0.125 to 0.125
- down_weight: bfloat16 [128, 512, 2048], P(('sp', 'tp')), may hold values from -0.25 to 0.25
- routes: int32 [32768, 2], P(('grp', 'sp', 'tp')), parts along dimension 0, may hold values from 0 to 127, as said below
- route_weight: float32 [32768, 2], P(('grp', 'sp', 'tp')), parts along dimension 0, may hold values from 0.1 to 1
Outputs:
- layer_out: bfloat16 [32768, 2048], P(('grp', 'sp', 'tp')), parts along dimension 0
The draws below stay inside these ranges and needn't reach their ends.
There are 2 independent parts, one for each index of `grp`. The reference program is written for one: setup_inputs(seed, part) draws one part's arguments, and reference() takes and returns one part's arrays. A program takes and returns all parts, laid end to end along the dimension named above; an argument that names none is the same for every part. Nothing has to cross between parts.
Inputs may be any that keep to these rules, and one draw needn't show every extreme that they name: `routes`: A token's two experts differ and lie in the same group of 32 consecutive experts. Among the 128 tokens of one device (aligned blocks of 128 rows) no expert is named more than 4 times; in every block each expert of one group, the same group for all blocks, is named exactly 4 times.
All inputs are finite; a program needn't handle non-finite values.
Results may differ from the reference program's by a relative error of at most 0.013.
Values may be sent and summed in bfloat16 or wider, within the bound.
A program may use at most 64 MiB of HBM per device.

```python
import math
import jax
import jax.numpy as jnp
from jax import lax

D = 2048
HEADS = 16
KV = 4
HDIM = 64
WINDOW = 128
FFE = 512
GROUPS = 4
TOKENS = 16384
ROWS = 128
EXPERTS = 128
EPG = 32
CAP = 4


def shared_rows(key):
    key_part = jnp.clip(jax.random.normal(jax.random.fold_in(key, 1), (TOKENS, KV * HDIM), jnp.float32), -4.0, 4.0)
    query_part = jnp.clip(jax.random.normal(jax.random.fold_in(key, 2), (TOKENS, HEADS * HDIM), jnp.float32), -4.0, 4.0)
    return (query_part, key_part)


def draw_query_rows(key, part):
    query_part, key_part = shared_rows(jax.random.fold_in(key, 17))
    return query_part.astype(jnp.bfloat16)


def draw_key_rows(key, part):
    query_part, key_part = shared_rows(jax.random.fold_in(key, 17))
    return key_part.astype(jnp.bfloat16)


def draw_routes(key, part):
    block_count = TOKENS // ROWS
    half_rows = ROWS // 2
    full_group = jax.random.randint(jax.random.fold_in(key, 5), (), 0, GROUPS)

    def one_block(block_key):
        cuts = jnp.sort(jax.random.randint(jax.random.fold_in(block_key, 1), (GROUPS - 2,), 0, half_rows + 1))
        bounds = jnp.concatenate([jnp.zeros((1,), jnp.int32), cuts.astype(jnp.int32), jnp.full((1,), half_rows, jnp.int32)])
        other_sizes = bounds[1:] - bounds[:-1]
        others = (full_group + 1 + jnp.arange(GROUPS - 1, dtype=jnp.int32)) % GROUPS
        sizes = jnp.zeros((GROUPS,), jnp.int32).at[others].set(other_sizes).at[full_group].set(half_rows)
        ends = jnp.cumsum(sizes)
        starts = ends - sizes
        order = jax.random.permutation(jax.random.fold_in(block_key, 2), ROWS)
        places = jnp.arange(ROWS, dtype=jnp.int32)
        group_of = jnp.sum((places[:, None] >= ends[None, :]).astype(jnp.int32), axis=1)
        within = places - starts[group_of]
        group_keys = jax.vmap(lambda g: jax.random.fold_in(block_key, 10 + g))(jnp.arange(GROUPS, dtype=jnp.int32))
        perms = jax.vmap(lambda k: jax.random.permutation(k, EPG))(group_keys).astype(jnp.int32)
        offset = 1 + within // EPG % (EPG - 1)
        first_local = perms[group_of, within % EPG]
        second_local = perms[group_of, (within + offset) % EPG]
        pair = jnp.stack([group_of * EPG + first_local, group_of * EPG + second_local], axis=1).astype(jnp.int32)
        return jnp.zeros((ROWS, 2), jnp.int32).at[order].set(pair)
    block_keys = jax.vmap(lambda b: jax.random.fold_in(key, 100 + b))(jnp.arange(block_count, dtype=jnp.int32))
    return jax.vmap(one_block)(block_keys).reshape(TOKENS, 2)


def block_levels(own_key, extent, split, smallest, top_value):
    def one(axis_at, blocks):
        heights = jax.random.uniform(jax.random.fold_in(jax.random.fold_in(own_key, 6), axis_at), (blocks,), jnp.float32, smallest / len(split), top_value / len(split))
        return jnp.repeat(jnp.exp(heights), extent[axis_at] // blocks).reshape((-1,) + (1,) * (len(extent) - axis_at - 1))

    level = one(*split[0])
    for cut in split[1:]:
        level = level * one(*cut)
    return level


def normal_values(own_key, extent, scale, limit, shards=(), kind=jnp.bfloat16):
    entries = scale * jax.random.normal(own_key, extent, jnp.float32)
    if shards:
        entries = entries * block_levels(own_key, extent, shards, -0.22, 0.18)
    return jnp.clip(entries, -limit, limit).astype(kind)


def setup_inputs(seed: int = 0, part: int = 0) -> dict:
    keys = jax.random.split(jax.random.key(seed), 13)
    part_splits = jax.random.split(jax.random.fold_in(keys[12], part), 13)
    query_rows = draw_query_rows(jax.random.fold_in(jax.random.fold_in(keys[12], part), 71), part)
    key_rows = draw_key_rows(jax.random.fold_in(jax.random.fold_in(keys[12], part), 71), part)
    value_rows = normal_values(part_splits[2], (TOKENS, KV * HDIM), 1.0, 6.0, ((0, 32), (1, 4)))
    sink_logits = jnp.clip(3.0 + 4.0 * jax.random.uniform(keys[3], (HEADS,), jnp.float32) ** block_levels(keys[3], (HEADS,), ((0, 4),), -0.2, 0.2), 3.0, 7.0)
    residual = normal_values(part_splits[4], (TOKENS, D), 1.0, 6.0, ((0, 128),))
    out_weight = normal_values(keys[5], (HEADS * HDIM, D), (HEADS * HDIM) ** -0.5, 0.1875, ((0, 4),))
    norm_gain = jnp.clip(1.0 + 0.18 * jax.random.normal(keys[6], (D,), jnp.float32), 0.1, 1.9)
    gate_weight = normal_values(keys[7], (EXPERTS, D, FFE), D ** -0.5, 0.125, ((0, 128),))
    up_weight = normal_values(keys[8], (EXPERTS, D, FFE), D ** -0.5, 0.125, ((0, 128),))
    down_weight = normal_values(keys[9], (EXPERTS, FFE, D), FFE ** -0.5, 0.25, ((0, 128),))
    routes = draw_routes(jax.random.fold_in(jax.random.fold_in(keys[12], part), 71), part)
    route_weight = jnp.clip(jnp.exp(math.log(1.0) - 2.3025851 * jax.random.uniform(part_splits[11], (TOKENS, 2), jnp.float32) ** block_levels(part_splits[11], (TOKENS, 2), ((0, 128),), -0.2, 0.2)), 0.1, 1.0)
    return {"query_rows": query_rows, "key_rows": key_rows, "value_rows": value_rows, "sink_logits": sink_logits, "residual": residual, "out_weight": out_weight, "norm_gain": norm_gain, "gate_weight": gate_weight, "up_weight": up_weight, "down_weight": down_weight, "routes": routes, "route_weight": route_weight}


rope_base = 10000.0
norm_eps = 1e-06

def rotate(rows, positions, heads):
    half_dim = HDIM // 2
    values = rows.astype(jnp.float32).reshape(rows.shape[0], heads, HDIM)
    inverse = rope_base ** (-jnp.arange(half_dim, dtype=jnp.float32) / half_dim)
    angles = positions.astype(jnp.float32)[:, None] * inverse[None, :]
    cosines = jnp.cos(angles)[:, None, :]
    sines = jnp.sin(angles)[:, None, :]
    lower = values[..., :half_dim]
    upper = values[..., half_dim:]
    turned = jnp.concatenate([lower * cosines - upper * sines, upper * cosines + lower * sines], axis=-1)
    return turned.reshape(rows.shape[0], heads * HDIM).astype(jnp.bfloat16)

def reference(query_rows, key_rows, value_rows, sink_logits, residual, out_weight, norm_gain, gate_weight, up_weight, down_weight, routes, route_weight):
    positions = jnp.arange(TOKENS, dtype=jnp.int32)
    rot_q = rotate(query_rows, positions, HEADS)
    rot_k = rotate(key_rows, positions, KV)
    repeat = HEADS // KV
    blocks = TOKENS // WINDOW
    q_blocks = rot_q.reshape(blocks, WINDOW, KV, repeat, HDIM)
    k_blocks = rot_k.reshape(blocks, WINDOW, KV, HDIM)
    v_blocks = value_rows.reshape(blocks, WINDOW, KV, HDIM)
    k_wide = jnp.concatenate([jnp.concatenate([jnp.zeros_like(k_blocks[:1]), k_blocks[:-1]], axis=0), k_blocks], axis=1)
    v_wide = jnp.concatenate([jnp.concatenate([jnp.zeros_like(v_blocks[:1]), v_blocks[:-1]], axis=0), v_blocks], axis=1)
    query_pos = jnp.arange(WINDOW) + WINDOW
    key_pos = jnp.arange(2 * WINDOW)
    distance = query_pos[:, None] - key_pos[None, :]
    in_band = (distance >= 0) & (distance < WINDOW)
    earliest = (jnp.arange(blocks)[:, None, None] > 0) | (key_pos[None, None, :] >= WINDOW)
    allowed = in_band[None] & earliest
    sinks_grouped = sink_logits.astype(jnp.float32).reshape(KV, repeat)

    def one_group(group):
        q_group = q_blocks[:, :, group].astype(jnp.float32)
        k_group = k_wide[:, :, group].astype(jnp.float32)
        v_group = v_wide[:, :, group].astype(jnp.float32)
        scores = jnp.einsum('nqrd,nkd->rnqk', q_group, k_group) * HDIM ** (-0.5)
        scores = jnp.where(allowed[None], scores, -jnp.inf)
        sink_here = sinks_grouped[group][:, None, None, None]
        largest = jnp.maximum(scores.max(axis=-1, keepdims=True), sink_here)
        exp_scores = jnp.exp(scores - largest)
        denominator = exp_scores.sum(axis=-1, keepdims=True) + jnp.exp(sink_here - largest)
        probs = (exp_scores / denominator).astype(jnp.bfloat16)
        mixed = jnp.einsum('rnqk,nkd->nqrd', probs.astype(jnp.float32), v_group)
        return mixed.astype(jnp.bfloat16)
    attended = lax.map(one_group, jnp.arange(KV, dtype=jnp.int32))
    attended = attended.transpose(1, 2, 0, 3, 4).reshape(TOKENS, HEADS * HDIM)
    projected = jnp.dot(attended, out_weight, preferred_element_type=jnp.float32)
    stream = (residual.astype(jnp.float32) + projected).astype(jnp.bfloat16)
    stream_f = stream.astype(jnp.float32)
    normed = (stream_f * lax.rsqrt(lax.optimization_barrier(jnp.mean(stream_f * stream_f, axis=-1, keepdims=True)) + norm_eps) * norm_gain[None, :]).astype(jnp.bfloat16)
    flat_expert = routes.reshape(-1).astype(jnp.int32)
    token_of = (jnp.arange(2 * TOKENS, dtype=jnp.int32) // 2).astype(jnp.int32)
    one_hot = (flat_expert[:, None] == jnp.arange(EXPERTS, dtype=jnp.int32)[None, :]).astype(jnp.int32)
    slot_rank = lax.optimization_barrier(jnp.sum((jnp.cumsum(one_hot, axis=0) - one_hot) * one_hot, axis=1)).astype(jnp.int32)
    slots = EXPERTS * CAP
    index_table = jnp.full((EXPERTS, slots), TOKENS, jnp.int32).at[flat_expert, slot_rank].set(token_of)
    weight_table = jnp.zeros((EXPERTS, slots), jnp.float32).at[flat_expert, slot_rank].set(route_weight.reshape(-1).astype(jnp.float32))
    padded = jnp.concatenate([normed, jnp.zeros((1, D), jnp.bfloat16)], axis=0)

    def serve(total, expert):
        picked = index_table[expert]
        routed = padded[picked]
        gate_out = jnp.dot(routed, gate_weight[expert], preferred_element_type=jnp.float32)
        up_out = jnp.dot(routed, up_weight[expert], preferred_element_type=jnp.float32)
        hidden = (jax.nn.silu(gate_out) * up_out).astype(jnp.bfloat16)
        expert_out = jnp.dot(hidden, down_weight[expert], preferred_element_type=jnp.float32).astype(jnp.bfloat16)
        total = total.at[picked].add(weight_table[expert][:, None] * expert_out.astype(jnp.float32))
        return (total, None)
    summed, _ = lax.scan(serve, jnp.zeros((TOKENS + 1, D), jnp.float32), jnp.arange(EXPERTS, dtype=jnp.int32))
    return (stream_f + summed[:TOKENS]).astype(jnp.bfloat16)
```

```python
import functools

import jax
import jax.numpy as jnp
from jax import lax
from jax.experimental import pallas as pl
from jax.experimental.pallas import tpu as pltpu
from jax.sharding import PartitionSpec as P

MESH_ID = pl.DeviceIdType.MESH
CAP = 4
CORES = 2

HDIM = 64
WINDOW = 128


rope_base = 10000.0
norm_eps = 1e-06


def shifted(block, axis, distance):
    devices = range(lax.axis_size(axis))
    route = [(i - distance, i) for i in devices if i - distance in devices]
    return lax.ppermute(block, axis, route)


def cut_along(x, dim, size):
    lengths = x.shape
    tiles = x.reshape(*lengths[:dim], size, lengths[dim] // size, *lengths[dim + 1 :])
    return jnp.moveaxis(tiles, dim, 0)


def summed_on_arrival(x, axis, dim):
    size = lax.axis_size(axis)
    tiles = lax.all_to_all(cut_along(x, dim, size), axis, 0, 0, tiled=True)
    return jnp.sum(tiles.astype(jnp.float32), axis=0)


def rotate(rows, positions, heads):
    half_dim = HDIM // 2
    values = rows.astype(jnp.float32).reshape(rows.shape[0], heads, HDIM)
    inverse = rope_base ** (-jnp.arange(half_dim, dtype=jnp.float32) / half_dim)
    angles = positions.astype(jnp.float32)[:, None] * inverse[None, :]
    cosines = jnp.cos(angles)[:, None, :]
    sines = jnp.sin(angles)[:, None, :]
    lower = values[..., :half_dim]
    upper = values[..., half_dim:]
    turned = jnp.concatenate(
        [lower * cosines - upper * sines, upper * cosines + lower * sines], axis=-1
    )
    return turned.reshape(rows.shape[0], heads * HDIM).astype(jnp.bfloat16)


def expert_kernel(
    ring,
    xs,
    tile,
    normed_ref,
    stream_ref,
    meta_ref,
    gate_hbm,
    up_hbm,
    down_hbm,
    out_ref,
    pool,
    pool_meta,
    picked,
    routed,
    made,
    back,
    left_sum,
    right_sum,
    left_own,
    right_own,
    gate_w,
    up_w,
    down_w,
    weight_sem,
    pool_send,
    pool_recv,
    meta_send,
    meta_recv,
    pick_send,
    pick_recv,
    back_send,
    back_recv,
    sum_send,
    sum_recv,
):
    f32, bf16 = jnp.float32, jnp.bfloat16
    rows, width = normed_ref.shape
    half = rows // 2
    far = ring // 2
    peers = xs * CORES
    sp, tp = lax.axis_index("sp"), lax.axis_index("tp")
    core = lax.rem(sp, CORES)
    z = sp // CORES
    mine = core * xs + tp
    nxt = {"sp": lax.rem(sp + CORES, ring * CORES)}
    prv = {"sp": lax.rem(sp + (ring - 1) * CORES, ring * CORES)}

    def peer(offset):
        u = lax.rem(mine + offset, peers)
        return u, {"sp": z * CORES + u // xs, "tp": lax.rem(u, xs)}

    loads = [
        pltpu.make_async_copy(src, dst, weight_sem.at[i])
        for i, (src, dst) in enumerate(((gate_hbm, gate_w), (up_hbm, up_w), (down_hbm, down_w)))
    ]
    for load in loads:
        load.start()

    barrier = pltpu.get_barrier_semaphore()
    pl.semaphore_signal(barrier, inc=1, device_id=nxt, device_id_type=MESH_ID)
    pl.semaphore_signal(barrier, inc=1, device_id=prv, device_id_type=MESH_ID)
    for o in range(1, peers):
        pl.semaphore_signal(barrier, inc=1, device_id=peer(o)[1], device_id_type=MESH_ID)
    pl.semaphore_wait(barrier, peers + 1)

    def part(h):
        return pl.ds(h * half, half)

    def send_pool(way, slot, h, src=None):
        to = slot + 1 if way == 0 else lax.rem(slot + ring - 1, ring)
        step = slot if way == 0 else lax.rem(ring - slot, ring)
        src = pool.at[slot, part(h)] if src is None else src
        return pltpu.make_async_remote_copy(
            src_ref=src,
            dst_ref=pool.at[to, part(h)],
            send_sem=pool_send.at[way, step, h],
            recv_sem=pool_recv.at[way, step, h],
            device_id=nxt if way == 0 else prv,
            device_id_type=MESH_ID,
        )

    def send_meta(way, slot, src=None):
        to = slot + 1 if way == 0 else lax.rem(slot + ring - 1, ring)
        step = slot if way == 0 else lax.rem(ring - slot, ring)
        return pltpu.make_async_remote_copy(
            src_ref=pool_meta.at[slot] if src is None else src,
            dst_ref=pool_meta.at[to],
            send_sem=meta_send.at[way, step],
            recv_sem=meta_recv.at[way, step],
            device_id=nxt if way == 0 else prv,
            device_id_type=MESH_ID,
        )

    for way in range(2):
        send_meta(way, 0, meta_ref).start()
        for h in range(2):
            send_pool(way, 0, h, normed_ref.at[part(h)]).start()
    pool[0] = normed_ref[...]
    pool_meta[0] = meta_ref[...]

    row_id = lax.broadcasted_iota(jnp.int32, (peers * 2 * CAP, rows), 0)
    local_code = (row_id // (2 * CAP)) * CAP + lax.rem(row_id, CAP)
    in_second = lax.rem(row_id, 2 * CAP) >= CAP
    base = z * (peers * CAP)

    def matches(slot, second):
        here = jnp.where(in_second == second, local_code + base, -1).astype(f32)
        m = pool_meta[slot]
        return here == m[0:1, :], here == m[1:2, :], m

    def pick_of(slot, second):
        first_hit, second_hit, _ = matches(slot, second)
        return (first_hit | second_hit).astype(f32).astype(bf16)

    def weights_of(slot, second):
        first_hit, second_hit, m = matches(slot, second)
        w = jnp.where(first_hit, m[2:3, :], 0.0) + jnp.where(second_hit, m[3:4, :], 0.0)
        high = w.astype(bf16)
        return high, (w - high.astype(f32)).astype(bf16)

    def exchange(src, dst, sends, recvs, step, offset):
        u, where = peer(offset)
        return pltpu.make_async_remote_copy(
            src_ref=src.at[step, u],
            dst_ref=dst.at[step, mine],
            send_sem=sends.at[step, offset],
            recv_sem=recvs.at[step, offset],
            device_id=where,
            device_id_type=MESH_ID,
        )

    def pick(step):
        a, b = step, ring - 1 - step
        one_a, one_b = pick_of(a, False), pick_of(b, True)
        for c in range(width // tile):
            cols = pl.ds(c * tile, tile)
            got = jnp.dot(one_a, pool[a, :, cols], preferred_element_type=f32)
            got += jnp.dot(one_b, pool[b, :, cols], preferred_element_type=f32)
            got = got.astype(bf16).reshape(peers, 2 * CAP, tile)
            picked[step, :, :, cols] = got
        for o in range(1, peers):
            exchange(picked, routed, pick_send, pick_recv, step, o).start()
        routed[step, mine] = picked[step, mine]

    def serve(step):
        for o in range(1, peers):
            exchange(picked, routed, pick_send, pick_recv, step, o).wait_recv()
        x = routed[step].reshape(peers * 2 * CAP, width)
        g = jnp.dot(x, gate_w[...], preferred_element_type=f32)
        u = jnp.dot(x, up_w[...], preferred_element_type=f32)
        hidden = (g * (1.0 / (1.0 + jnp.exp(-g))) * u).astype(bf16)
        for c in range(width // tile):
            cols = pl.ds(c * tile, tile)
            y = jnp.dot(hidden, down_w[:, cols], preferred_element_type=f32)
            made[step, :, :, cols] = y.astype(bf16).reshape(peers, 2 * CAP, tile)
        for o in range(1, peers):
            exchange(made, back, back_send, back_recv, step, o).start()
        back[step, mine] = made[step, mine]

    def ring_step(n, _):
        for h in range(2):
            send_pool(0, n - 1, h).wait_recv()

            @pl.when((n < far - 1) | (h == 0))
            def _():
                send_pool(0, n, h).start()

            send_pool(1, lax.rem(ring - n + 1, ring), h).wait_recv()

            @pl.when((n < far - 1) | (h == 1))
            def _():
                send_pool(1, ring - n, h).start()

            if h == 0:
                send_meta(0, n - 1).wait_recv()
                send_meta(0, n).start()
                send_meta(1, lax.rem(ring - n + 1, ring)).wait_recv()

                @pl.when(n < far - 1)
                def _():
                    send_meta(1, ring - n).start()

                @pl.when(n >= 2)
                def _():
                    serve(n - 2)
            else:
                pick(n - 1)
        return 0

    for load in loads:
        load.wait()
    lax.fori_loop(1, far, ring_step, 0)
    serve(far - 2)
    send_meta(0, far - 1).wait_recv()
    send_pool(0, far - 1, 0).wait_recv()
    send_pool(1, ring - far + 1, 1).wait_recv()
    pick(far - 1)
    serve(far - 1)

    contract = (((0,), (0,)), ((), ()))

    def wait_back(step):
        for o in range(1, peers):
            exchange(made, back, back_send, back_recv, step, o).wait_recv()

    def own_share(slot, step, second, dst):
        high, low = weights_of(slot, second)
        w = jnp.concatenate([high, low], axis=0)
        for c in range(width // tile):
            cols = pl.ds(c * tile, tile)
            y = back[step, :, :, cols].reshape(peers * 2 * CAP, tile)
            y = jnp.concatenate([y, y], axis=0)
            dst[:, cols] = lax.dot_general(w, y, contract, preferred_element_type=f32)

    def send_sum(way, d, h):
        buf = left_sum if way == 0 else right_sum
        return pltpu.make_async_remote_copy(
            src_ref=buf.at[d, part(h)],
            dst_ref=buf.at[d - 1, part(h)],
            send_sem=sum_send.at[way, d - 1, h],
            recv_sem=sum_recv.at[way, d - 1, h],
            device_id=prv if way == 0 else nxt,
            device_id_type=MESH_ID,
        )

    wait_back(far - 1)
    own_share(far, far - 1, True, left_own)
    left_sum[far, part(0)] = left_own[part(0)].astype(bf16)
    send_sum(0, far, 0).start()
    right_sum[far, part(1)] = left_own[part(1)].astype(bf16)
    send_sum(1, far, 1).start()

    def sum_step(i, _):
        d = far - 1 - i
        wait_back(d - 1)
        own_share(d, d, False, left_own)
        own_share(ring - d, d - 1, True, right_own)
        for way, own, buf, order in ((0, left_own, left_sum, (1, 0)), (1, right_own, right_sum, (0, 1))):
            h = order[0]

            @pl.when(d < far - 1)
            def _():
                send_sum(way, d + 1, h).wait_recv()
                buf[d, part(h)] = (buf[d, part(h)].astype(f32) + own[part(h)]).astype(bf16)

            @pl.when(d == far - 1)
            def _():
                buf[d, part(h)] = own[part(h)].astype(bf16)

            send_sum(way, d, h).start()
        for way, own, buf, order in ((0, left_own, left_sum, (1, 0)), (1, right_own, right_sum, (0, 1))):
            h = order[1]
            send_sum(way, d + 1, h).wait_recv()
            buf[d, part(h)] = (buf[d, part(h)].astype(f32) + own[part(h)]).astype(bf16)
            send_sum(way, d, h).start()
        return 0

    lax.fori_loop(0, far - 1, sum_step, 0)
    own_share(0, 0, False, left_own)
    left_own[...] += stream_ref[...].astype(f32)
    for h in (1, 0):
        send_sum(0, 1, h).wait_recv()
        send_sum(1, 1, h).wait_recv()
        total = left_own[part(h)] + left_sum[0, part(h)].astype(f32)
        out_ref[part(h)] = (total + right_sum[0, part(h)].astype(f32)).astype(bf16)

    def drain(n, _):
        for way in range(2):
            slot = n if way == 0 else lax.rem(ring - n, ring)
            for h in range(2):

                @pl.when((n < far - 1) | (h == way))
                def _():
                    send_pool(way, slot, h).wait_send()

                @pl.when((n < far - 1) | (h == way))
                def _():
                    send_sum(way, n + 1, h).wait_send()

            @pl.when((n < far - 1) | (way == 0))
            def _():
                send_meta(way, slot).wait_send()

        for o in range(1, peers):
            exchange(picked, routed, pick_send, pick_recv, n, o).wait_send()
            exchange(made, back, back_send, back_recv, n, o).wait_send()
        return 0

    lax.fori_loop(0, far, drain, 0)


def routed_experts(normed, stream, meta, gate, up, down):
    rows, width = normed.shape
    ring = lax.axis_size("sp") // CORES
    xs = lax.axis_size("tp")
    far = ring // 2
    peers = xs * CORES
    hidden = gate.shape[1]
    tile = min(512, width)
    bf16 = jnp.bfloat16
    vmem = pl.BlockSpec(memory_space=pltpu.VMEM)
    hbm = pl.BlockSpec(memory_space=pl.ANY)
    slab = (far, peers, 2 * CAP, width)
    dma = pltpu.SemaphoreType.DMA
    return pl.pallas_call(
        functools.partial(expert_kernel, ring, xs, tile),
        out_shape=jax.ShapeDtypeStruct((rows, width), bf16),
        in_specs=[vmem, vmem, vmem, hbm, hbm, hbm],
        out_specs=vmem,
        scratch_shapes=[
            pltpu.VMEM((ring, rows, width), bf16),
            pltpu.VMEM((ring, 8, rows), jnp.float32),
            pltpu.VMEM(slab, bf16),
            pltpu.VMEM(slab, bf16),
            pltpu.VMEM(slab, bf16),
            pltpu.VMEM(slab, bf16),
            pltpu.VMEM((far + 1, rows, width), bf16),
            pltpu.VMEM((far + 1, rows, width), bf16),
            pltpu.VMEM((rows, width), jnp.float32),
            pltpu.VMEM((rows, width), jnp.float32),
            pltpu.VMEM((width, hidden), bf16),
            pltpu.VMEM((width, hidden), bf16),
            pltpu.VMEM((hidden, width), bf16),
            dma((3,)),
            dma((2, far, 2)),
            dma((2, far, 2)),
            dma((2, far)),
            dma((2, far)),
            dma((far, peers)),
            dma((far, peers)),
            dma((far, peers)),
            dma((far, peers)),
            dma((2, far, 2)),
            dma((2, far, 2)),
        ],
        compiler_params=pltpu.CompilerParams(
            collective_id=1, has_side_effects=True, vmem_limit_bytes=60 * 1024 * 1024
        ),
    )(normed, stream, meta, gate, up, down)


def per_device(
    query_rows,
    key_rows,
    value_rows,
    sink_logits,
    residual,
    out_weight,
    norm_gain,
    gate_weight,
    up_weight,
    down_weight,
    routes,
    route_weight,
):
    tok_count = query_rows.shape[0]
    head_local = query_rows.shape[1] // HDIM
    group_local = key_rows.shape[1] // HDIM
    repeat = head_local // group_local
    first_pos = lax.axis_index("sp") * tok_count
    positions = first_pos + jnp.arange(tok_count, dtype=jnp.int32)
    rot_q = rotate(query_rows, positions, head_local)
    rot_k = rotate(key_rows, positions, group_local)
    tails = jnp.stack([rot_k[tok_count - WINDOW :], value_rows[tok_count - WINDOW :]])
    earlier = shifted(tails, "sp", 1)
    blocks = tok_count // WINDOW
    q_blocks = rot_q.reshape(blocks, WINDOW, group_local, repeat, HDIM)
    k_blocks = rot_k.reshape(blocks, WINDOW, group_local, HDIM)
    v_blocks = value_rows.reshape(blocks, WINDOW, group_local, HDIM)
    k_prev = jnp.concatenate(
        [earlier[0].reshape(1, WINDOW, group_local, HDIM), k_blocks[:-1]], axis=0
    )
    v_prev = jnp.concatenate(
        [earlier[1].reshape(1, WINDOW, group_local, HDIM), v_blocks[:-1]], axis=0
    )
    k_wide = jnp.concatenate([k_prev, k_blocks], axis=1)
    v_wide = jnp.concatenate([v_prev, v_blocks], axis=1)
    query_pos = jnp.arange(WINDOW) + WINDOW
    key_pos = jnp.arange(2 * WINDOW)
    distance = query_pos[:, None] - key_pos[None, :]
    in_band = (distance >= 0) & (distance < WINDOW)
    key_global = (
        first_pos + jnp.arange(blocks)[:, None, None] * WINDOW + key_pos[None, None, :] - WINDOW
    )
    allowed = in_band[None] & (key_global >= 0)
    scores = jnp.einsum(
        "nqgrd,nkgd->grnqk", q_blocks, k_wide, preferred_element_type=jnp.float32
    ) * HDIM ** (-0.5)
    scores = jnp.where(allowed[None, None], scores, -jnp.inf)
    sink_here = sink_logits.reshape(group_local, repeat)[:, :, None, None, None]
    largest = jnp.maximum(scores.max(axis=-1, keepdims=True), sink_here)
    exp_scores = jnp.exp(scores - largest)
    denominator = exp_scores.sum(axis=-1, keepdims=True) + jnp.exp(sink_here - largest)
    probs = (exp_scores / denominator).astype(jnp.bfloat16)
    attended = jnp.einsum("grnqk,nkgd->nqgrd", probs, v_wide, preferred_element_type=jnp.float32)
    attended = attended.astype(jnp.bfloat16).reshape(tok_count, head_local * HDIM)
    row_count = residual.shape[0]
    projected = summed_on_arrival(
        jnp.dot(attended, out_weight, preferred_element_type=jnp.float32).astype(jnp.bfloat16),
        "tp",
        0,
    )
    stream_f = (residual.astype(jnp.float32) + projected).astype(jnp.bfloat16).astype(jnp.float32)
    normed = (
        stream_f
        * lax.rsqrt(jnp.mean(stream_f * stream_f, axis=-1, keepdims=True) + norm_eps)
        * norm_gain[None, :]
    ).astype(jnp.bfloat16)
    width = normed.shape[1]
    expert_count = lax.axis_size("sp") * lax.axis_size("tp")
    flat_expert = routes.reshape(-1)
    one_hot = (flat_expert[:, None] == jnp.arange(expert_count, dtype=jnp.int32)[None, :]).astype(
        jnp.int32
    )
    slot_rank = jnp.sum((jnp.cumsum(one_hot, axis=0) - one_hot) * one_hot, axis=1)
    codes = (flat_expert * CAP + slot_rank).astype(jnp.float32).reshape(row_count, 2)
    meta = jnp.concatenate(
        [codes.T, route_weight.T, jnp.zeros((4, row_count), jnp.float32)], axis=0
    )
    return routed_experts(
        normed, stream_f.astype(jnp.bfloat16), meta, gate_weight[0], up_weight[0], down_weight[0]
    )


def solution(mesh):
    in_specs = (
        P(("grp", "sp"), "tp"),
        P(("grp", "sp"), "tp"),
        P(("grp", "sp"), "tp"),
        P("tp"),
        P(("grp", "sp", "tp"), None),
        P("tp", None),
        P(),
        P(("sp", "tp"), None, None),
        P(("sp", "tp"), None, None),
        P(("sp", "tp"), None, None),
        P(("grp", "sp", "tp"), None),
        P(("grp", "sp", "tp"), None),
    )
    out_specs = P(("grp", "sp", "tp"), None)
    return jax.shard_map(
        per_device, mesh=mesh, in_specs=in_specs, out_specs=out_specs, check_vma=False
    )
```

```python
import functools

import jax
import jax.numpy as jnp
from jax import lax
from jax.experimental import pallas as pl
from jax.experimental.pallas import tpu as pltpu
from jax.sharding import PartitionSpec as P

MESH_ID = pl.DeviceIdType.MESH
HDIM = 64
WINDOW = 128
CAP = 4
CORES = 2


rope_base = 10000.0
norm_eps = 1e-06


def expert_kernel(
    ring,
    xs,
    tile,
    query_ref,
    key_ref,
    value_ref,
    cos_ref,
    sin_ref,
    sink_ref,
    gain_ref,
    meta_ref,
    residual_hbm,
    proj_hbm,
    gate_hbm,
    up_hbm,
    down_hbm,
    out_ref,
    rot_q,
    keys_values,
    residual,
    proj_w,
    shares,
    far_in,
    near_in,
    own_share_sum,
    stream,
    pool,
    pool_meta,
    picked,
    routed,
    made,
    back,
    left_sum,
    right_sum,
    left_own,
    right_own,
    gate_w,
    up_w,
    down_w,
    weight_sem,
    pool_send,
    pool_recv,
    meta_send,
    meta_recv,
    pick_send,
    pick_recv,
    back_send,
    back_recv,
    sum_send,
    sum_recv,
    halo_send,
    halo_recv,
    far_send,
    far_recv,
    near_send,
    near_recv,
):
    f32, bf16 = jnp.float32, jnp.bfloat16
    rows, width = residual.shape
    half = rows // 2
    far = ring // 2
    peers = xs * CORES
    sp, tp = lax.axis_index("sp"), lax.axis_index("tp")
    core = lax.rem(sp, CORES)
    z = sp // CORES
    mine = core * xs + tp
    nxt = {"sp": lax.rem(sp + CORES, ring * CORES)}
    prv = {"sp": lax.rem(sp + (ring - 1) * CORES, ring * CORES)}

    def peer(offset):
        u = lax.rem(mine + offset, peers)
        return u, {"sp": z * CORES + u // xs, "tp": lax.rem(u, xs)}

    loads = [
        pltpu.make_async_copy(src, dst, weight_sem.at[i])
        for i, (src, dst) in enumerate(
            (
                (proj_hbm, proj_w),
                (residual_hbm, residual),
                (gate_hbm, gate_w),
                (up_hbm, up_w),
                (down_hbm, down_w),
            )
        )
    ]
    for load in loads:
        load.start()

    barrier = pltpu.get_barrier_semaphore()
    pl.semaphore_signal(barrier, inc=1, device_id=nxt, device_id_type=MESH_ID)
    pl.semaphore_signal(barrier, inc=1, device_id=prv, device_id_type=MESH_ID)
    total_sp = ring * CORES
    after = {"sp": lax.rem(sp + 1, total_sp)}
    across = {"sp": lax.rem(sp + jnp.where(core == 1, 1, total_sp - 1), total_sp)}
    pl.semaphore_signal(barrier, inc=1, device_id=across, device_id_type=MESH_ID)
    for o in range(1, peers):
        pl.semaphore_signal(barrier, inc=1, device_id=peer(o)[1], device_id_type=MESH_ID)

    lane = lax.broadcasted_iota(jnp.int32, (query_ref.shape[1],) * 2, 1)
    line = lax.broadcasted_iota(jnp.int32, (query_ref.shape[1],) * 2, 0)
    low = lax.rem(lane, HDIM) < HDIM // 2
    turn = jnp.where(low & (line == lane + HDIM // 2), -1.0, 0.0)
    turn = (turn + jnp.where((~low) & (line == lane - HDIM // 2), 1.0, 0.0)).astype(bf16)

    def rotated(x, cosines, sines):
        n = x.shape[1]
        swapped = jnp.dot(x, turn[:n, :n], preferred_element_type=f32)
        return (x.astype(f32) * cosines + swapped * sines).astype(bf16)

    tok = query_ref.shape[0]
    keys_values[WINDOW:, 0:HDIM] = rotated(key_ref[...], cos_ref[:, 0:HDIM], sin_ref[:, 0:HDIM])
    keys_values[WINDOW:, HDIM:] = value_ref[...]
    pl.semaphore_wait(barrier, peers + 2)
    halo = pltpu.make_async_remote_copy(
        src_ref=keys_values.at[pl.ds(tok, WINDOW)],
        dst_ref=keys_values.at[pl.ds(0, WINDOW)],
        send_sem=halo_send,
        recv_sem=halo_recv,
        device_id=after,
        device_id_type=MESH_ID,
    )
    halo.start()
    for c in range(query_ref.shape[1] // 128):
        cols = pl.ds(c * 128, 128)
        rot_q[:, cols] = rotated(query_ref[:, cols], cos_ref[...], sin_ref[...])
    halo.wait_recv()

    def part(h):
        return pl.ds(h * half, half)

    def send_pool(way, slot, h):
        to = slot + 1 if way == 0 else lax.rem(slot + ring - 1, ring)
        step = slot if way == 0 else lax.rem(ring - slot, ring)
        return pltpu.make_async_remote_copy(
            src_ref=pool.at[slot, part(h)],
            dst_ref=pool.at[to, part(h)],
            send_sem=pool_send.at[way, step, h],
            recv_sem=pool_recv.at[way, step, h],
            device_id=nxt if way == 0 else prv,
            device_id_type=MESH_ID,
        )

    def send_meta(way, slot, src=None):
        to = slot + 1 if way == 0 else lax.rem(slot + ring - 1, ring)
        step = slot if way == 0 else lax.rem(ring - slot, ring)
        return pltpu.make_async_remote_copy(
            src_ref=pool_meta.at[slot] if src is None else src,
            dst_ref=pool_meta.at[to],
            send_sem=meta_send.at[way, step],
            recv_sem=meta_recv.at[way, step],
            device_id=nxt if way == 0 else prv,
            device_id_type=MESH_ID,
        )

    for way in range(2):
        send_meta(way, 0, meta_ref).start()
    pool_meta[0] = meta_ref[...]

    q_at = lax.broadcasted_iota(jnp.int32, (WINDOW, 2 * WINDOW), 0)
    k_at = lax.broadcasted_iota(jnp.int32, (WINDOW, 2 * WINDOW), 1)
    reach = q_at + WINDOW - k_at

    def projected(block):
        start = pl.multiple_of(block * WINDOW, WINDOW)
        first = start + sp * tok
        allowed = (reach >= 0) & (reach < WINDOW) & (k_at + first >= WINDOW)
        kv = keys_values[pl.ds(start, 2 * WINDOW), :]
        k, v = kv[:, 0:HDIM], kv[:, HDIM:]
        q = rot_q[pl.ds(start, WINDOW), :]
        heads = []
        for h in range(q.shape[1] // HDIM):
            qh = q[:, h * HDIM : (h + 1) * HDIM]
            s = lax.dot_general(qh, k, (((1,), (1,)), ((), ())), preferred_element_type=f32)
            s = jnp.where(allowed, s * HDIM ** (-0.5), -jnp.inf)
            sink = sink_ref[h]
            top = jnp.maximum(jnp.max(s, axis=1, keepdims=True), sink)
            e = jnp.exp(s - top)
            below = jnp.sum(e, axis=1, keepdims=True) + jnp.exp(sink - top)
            p = (e / below).astype(bf16)
            heads.append(jnp.dot(p, v, preferred_element_type=f32).astype(bf16))
        att = jnp.concatenate(heads, axis=1)
        for c in range(width // tile):
            cols = pl.ds(c * tile, tile)
            yield cols, jnp.dot(att, proj_w[:, cols], preferred_element_type=f32)

    def beside(step):
        return {"tp": lax.rem(tp + step + xs, xs)}

    quarter = half // 2

    def send_far(way, h):
        at = h * half + way * quarter
        return pltpu.make_async_remote_copy(
            src_ref=shares.at[2, pl.ds(at, quarter)],
            dst_ref=far_in.at[way, h],
            send_sem=far_send.at[way, h],
            recv_sem=far_recv.at[way, h],
            device_id=beside(1 - 2 * way),
            device_id_type=MESH_ID,
        )

    def send_near(way, h):
        return pltpu.make_async_remote_copy(
            src_ref=shares.at[way, part(h)],
            dst_ref=near_in.at[way, h],
            send_sem=near_send.at[way, h],
            recv_sem=near_recv.at[way, h],
            device_id=beside(1 - 2 * way),
            device_id_type=MESH_ID,
        )

    loads[0].wait()
    for cols, y in projected(lax.rem(tp + 2, xs)):
        shares[2, :, cols] = y.astype(bf16)
    for h in range(2):
        for way in range(2):
            send_far(way, h).start()
    for way in range(2):
        for cols, y in projected(lax.rem(tp + 1 - 2 * way + xs, xs)):
            own_share_sum[:, cols] = y
        for h in range(2):
            send_far(way, h).wait_recv()
            joint = pl.ds(h * half + way * quarter, quarter)
            alone = pl.ds(h * half + (1 - way) * quarter, quarter)
            shares[way, alone] = own_share_sum[alone].astype(bf16)
            joined = own_share_sum[joint] + far_in[way, h].astype(f32)
            shares[way, joint] = joined.astype(bf16)
            send_near(way, h).start()
    for cols, y in projected(tp):
        own_share_sum[:, cols] = y
    loads[1].wait()

    def own_rows(h):
        for way in range(2):
            send_near(way, h).wait_recv()
        got = near_in[0, h].astype(f32) + near_in[1, h].astype(f32)
        x = residual[part(h)].astype(f32) + (own_share_sum[part(h)] + got)
        x = x.astype(bf16)
        stream[part(h)] = x
        x = x.astype(f32)
        scale = lax.rsqrt(jnp.mean(x * x, axis=1, keepdims=True) + norm_eps)
        pool[0, part(h)] = (x * scale * gain_ref[...]).astype(bf16)
        for way in range(2):
            send_pool(way, 0, h).start()

    own_rows(0)

    row_id = lax.broadcasted_iota(jnp.int32, (peers * 2 * CAP, rows), 0)
    local_code = (row_id // (2 * CAP)) * CAP + lax.rem(row_id, CAP)
    in_second = lax.rem(row_id, 2 * CAP) >= CAP
    base = z * (peers * CAP)

    def matches(slot, second):
        here = jnp.where(in_second == second, local_code + base, -1).astype(f32)
        m = pool_meta[slot]
        return here == m[0:1, :], here == m[1:2, :], m

    def pick_of(slot, second):
        first_hit, second_hit, _ = matches(slot, second)
        return (first_hit | second_hit).astype(f32).astype(bf16)

    def weights_of(slot, second):
        first_hit, second_hit, m = matches(slot, second)
        w = jnp.where(first_hit, m[2:3, :], 0.0) + jnp.where(second_hit, m[3:4, :], 0.0)
        high = w.astype(bf16)
        return high, (w - high.astype(f32)).astype(bf16)

    def exchange(src, dst, sends, recvs, step, offset):
        u, where = peer(offset)
        return pltpu.make_async_remote_copy(
            src_ref=src.at[step, u],
            dst_ref=dst.at[step, mine],
            send_sem=sends.at[step, offset],
            recv_sem=recvs.at[step, offset],
            device_id=where,
            device_id_type=MESH_ID,
        )

    def pick(step):
        a, b = step, ring - 1 - step
        one_a, one_b = pick_of(a, False), pick_of(b, True)
        for c in range(width // tile):
            cols = pl.ds(c * tile, tile)
            got = jnp.dot(one_a, pool[a, :, cols], preferred_element_type=f32)
            got += jnp.dot(one_b, pool[b, :, cols], preferred_element_type=f32)
            got = got.astype(bf16).reshape(peers, 2 * CAP, tile)
            picked[step, :, :, cols] = got
        for o in range(1, peers):
            exchange(picked, routed, pick_send, pick_recv, step, o).start()
        routed[step, mine] = picked[step, mine]

    def serve(step):
        for o in range(1, peers):
            exchange(picked, routed, pick_send, pick_recv, step, o).wait_recv()
        x = routed[step].reshape(peers * 2 * CAP, width)
        g = jnp.dot(x, gate_w[...], preferred_element_type=f32)
        u = jnp.dot(x, up_w[...], preferred_element_type=f32)
        hidden = (g * (1.0 / (1.0 + jnp.exp(-g))) * u).astype(bf16)
        for c in range(width // tile):
            cols = pl.ds(c * tile, tile)
            y = jnp.dot(hidden, down_w[:, cols], preferred_element_type=f32)
            made[step, :, :, cols] = y.astype(bf16).reshape(peers, 2 * CAP, tile)
        for o in range(1, peers):
            exchange(made, back, back_send, back_recv, step, o).start()
        back[step, mine] = made[step, mine]

    def ring_step(n, _):
        for h in range(2):
            send_pool(0, n - 1, h).wait_recv()

            @pl.when((n < far - 1) | (h == 0))
            def _():
                send_pool(0, n, h).start()

            send_pool(1, lax.rem(ring - n + 1, ring), h).wait_recv()

            @pl.when((n < far - 1) | (h == 1))
            def _():
                send_pool(1, ring - n, h).start()

            if h == 0:
                send_meta(0, n - 1).wait_recv()
                send_meta(0, n).start()
                send_meta(1, lax.rem(ring - n + 1, ring)).wait_recv()

                @pl.when(n < far - 1)
                def _():
                    send_meta(1, ring - n).start()

                @pl.when(n == 1)
                def _():
                    own_rows(1)

                @pl.when(n >= 2)
                def _():
                    serve(n - 2)
            else:
                pick(n - 1)
        return 0

    for load in loads[2:]:
        load.wait()
    lax.fori_loop(1, far, ring_step, 0)
    serve(far - 2)
    send_meta(0, far - 1).wait_recv()
    send_pool(0, far - 1, 0).wait_recv()
    send_pool(1, ring - far + 1, 1).wait_recv()
    pick(far - 1)
    serve(far - 1)

    contract = (((0,), (0,)), ((), ()))

    def wait_back(step):
        for o in range(1, peers):
            exchange(made, back, back_send, back_recv, step, o).wait_recv()

    def own_share(slot, step, second, dst):
        high, low = weights_of(slot, second)
        w = jnp.concatenate([high, low], axis=0)
        for c in range(width // tile):
            cols = pl.ds(c * tile, tile)
            y = back[step, :, :, cols].reshape(peers * 2 * CAP, tile)
            y = jnp.concatenate([y, y], axis=0)
            dst[:, cols] = lax.dot_general(w, y, contract, preferred_element_type=f32)

    def send_sum(way, d, h):
        buf = left_sum if way == 0 else right_sum
        return pltpu.make_async_remote_copy(
            src_ref=buf.at[d, part(h)],
            dst_ref=buf.at[d - 1, part(h)],
            send_sem=sum_send.at[way, d - 1, h],
            recv_sem=sum_recv.at[way, d - 1, h],
            device_id=prv if way == 0 else nxt,
            device_id_type=MESH_ID,
        )

    wait_back(far - 1)
    own_share(far, far - 1, True, left_own)
    left_sum[far, part(0)] = left_own[part(0)].astype(bf16)
    send_sum(0, far, 0).start()
    right_sum[far, part(1)] = left_own[part(1)].astype(bf16)
    send_sum(1, far, 1).start()

    def sum_step(i, _):
        d = far - 1 - i
        wait_back(d - 1)
        own_share(d, d, False, left_own)
        own_share(ring - d, d - 1, True, right_own)
        for way, own, buf, order in ((0, left_own, left_sum, (1, 0)), (1, right_own, right_sum, (0, 1))):
            h = order[0]

            @pl.when(d < far - 1)
            def _():
                send_sum(way, d + 1, h).wait_recv()
                buf[d, part(h)] = (buf[d, part(h)].astype(f32) + own[part(h)]).astype(bf16)

            @pl.when(d == far - 1)
            def _():
                buf[d, part(h)] = own[part(h)].astype(bf16)

            send_sum(way, d, h).start()
        for way, own, buf, order in ((0, left_own, left_sum, (1, 0)), (1, right_own, right_sum, (0, 1))):
            h = order[1]
            send_sum(way, d + 1, h).wait_recv()
            buf[d, part(h)] = (buf[d, part(h)].astype(f32) + own[part(h)]).astype(bf16)
            send_sum(way, d, h).start()
        return 0

    lax.fori_loop(0, far - 1, sum_step, 0)
    own_share(0, 0, False, left_own)
    left_own[...] += stream[...].astype(f32)
    for h in (1, 0):
        send_sum(0, 1, h).wait_recv()
        send_sum(1, 1, h).wait_recv()
        total = left_own[part(h)] + left_sum[0, part(h)].astype(f32)
        out_ref[part(h)] = (total + right_sum[0, part(h)].astype(f32)).astype(bf16)

    def drain(n, _):
        for way in range(2):
            slot = n if way == 0 else lax.rem(ring - n, ring)
            for h in range(2):

                @pl.when((n < far - 1) | (h == way))
                def _():
                    send_pool(way, slot, h).wait_send()

                @pl.when((n < far - 1) | (h == way))
                def _():
                    send_sum(way, n + 1, h).wait_send()

            @pl.when((n < far - 1) | (way == 0))
            def _():
                send_meta(way, slot).wait_send()

        for o in range(1, peers):
            exchange(picked, routed, pick_send, pick_recv, n, o).wait_send()
            exchange(made, back, back_send, back_recv, n, o).wait_send()
        return 0

    lax.fori_loop(0, far, drain, 0)
    halo.wait_send()
    for h in range(2):
        for way in range(2):
            send_far(way, h).wait_send()
            send_near(way, h).wait_send()


def layer(query, key, value, cosines, sines, sinks, gain, meta, residual, proj, gate, up, down):
    rows, width = residual.shape
    ring = lax.axis_size("sp") // CORES
    xs = lax.axis_size("tp")
    far = ring // 2
    peers = xs * CORES
    hidden = gate.shape[1]
    tile = min(512, width)
    bf16, f32 = jnp.bfloat16, jnp.float32
    vmem = pl.BlockSpec(memory_space=pltpu.VMEM)
    smem = pl.BlockSpec(memory_space=pltpu.SMEM)
    hbm = pl.BlockSpec(memory_space=pl.ANY)
    slab = (far, peers, 2 * CAP, width)
    dma = pltpu.SemaphoreType.DMA
    return pl.pallas_call(
        functools.partial(expert_kernel, ring, xs, tile),
        out_shape=jax.ShapeDtypeStruct((rows, width), bf16),
        in_specs=[vmem] * 5 + [smem] + [vmem] * 2 + [hbm] * 5,
        out_specs=vmem,
        scratch_shapes=[
            pltpu.VMEM(query.shape, bf16),
            pltpu.VMEM((query.shape[0] + WINDOW, 2 * HDIM), bf16),
            pltpu.VMEM((rows, width), bf16),
            pltpu.VMEM(proj.shape, bf16),
            pltpu.VMEM((3, rows, width), bf16),
            pltpu.VMEM((2, 2, rows // 4, width), bf16),
            pltpu.VMEM((2, 2, rows // 2, width), bf16),
            pltpu.VMEM((rows, width), f32),
            pltpu.VMEM((rows, width), bf16),
            pltpu.VMEM((ring, rows, width), bf16),
            pltpu.VMEM((ring, 8, rows), f32),
            pltpu.VMEM(slab, bf16),
            pltpu.VMEM(slab, bf16),
            pltpu.VMEM(slab, bf16),
            pltpu.VMEM(slab, bf16),
            pltpu.VMEM((far + 1, rows, width), bf16),
            pltpu.VMEM((far + 1, rows, width), bf16),
            pltpu.VMEM((rows, width), f32),
            pltpu.VMEM((rows, width), f32),
            pltpu.VMEM((width, hidden), bf16),
            pltpu.VMEM((width, hidden), bf16),
            pltpu.VMEM((hidden, width), bf16),
            dma((5,)),
            dma((2, far, 2)),
            dma((2, far, 2)),
            dma((2, far)),
            dma((2, far)),
            dma((far, peers)),
            dma((far, peers)),
            dma((far, peers)),
            dma((far, peers)),
            dma((2, far, 2)),
            dma((2, far, 2)),
            dma,
            dma,
            dma((2, 2)),
            dma((2, 2)),
            dma((2, 2)),
            dma((2, 2)),
        ],
        compiler_params=pltpu.CompilerParams(
            collective_id=1, has_side_effects=True, vmem_limit_bytes=60 * 1024 * 1024
        ),
    )(query, key, value, cosines, sines, sinks, gain, meta, residual, proj, gate, up, down)


def per_device(
    query_rows,
    key_rows,
    value_rows,
    sink_logits,
    residual,
    out_weight,
    norm_gain,
    gate_weight,
    up_weight,
    down_weight,
    routes,
    route_weight,
):
    tok_count = query_rows.shape[0]
    row_count = residual.shape[0]
    positions = lax.axis_index("sp") * tok_count + jnp.arange(tok_count, dtype=jnp.int32)
    half_dim = HDIM // 2
    inverse = rope_base ** (-jnp.arange(half_dim, dtype=jnp.float32) / half_dim)
    angles = positions.astype(jnp.float32)[:, None] * inverse[None, :]
    cosines = jnp.tile(jnp.cos(angles), (1, 128 // half_dim))
    sines = jnp.tile(jnp.sin(angles), (1, 128 // half_dim))
    expert_count = lax.axis_size("sp") * lax.axis_size("tp")
    flat_expert = routes.reshape(-1)
    one_hot = (flat_expert[:, None] == jnp.arange(expert_count, dtype=jnp.int32)[None, :]).astype(
        jnp.int32
    )
    slot_rank = jnp.sum((jnp.cumsum(one_hot, axis=0) - one_hot) * one_hot, axis=1)
    codes = (flat_expert * CAP + slot_rank).astype(jnp.float32).reshape(row_count, 2)
    meta = jnp.concatenate(
        [codes.T, route_weight.T, jnp.zeros((4, row_count), jnp.float32)], axis=0
    )
    return layer(
        query_rows,
        key_rows,
        value_rows,
        cosines,
        sines,
        sink_logits,
        norm_gain[None, :],
        meta,
        residual,
        out_weight,
        gate_weight[0],
        up_weight[0],
        down_weight[0],
    )


def solution(mesh):
    in_specs = (
        P(("grp", "sp"), "tp"),
        P(("grp", "sp"), "tp"),
        P(("grp", "sp"), "tp"),
        P("tp"),
        P(("grp", "sp", "tp"), None),
        P("tp", None),
        P(),
        P(("sp", "tp"), None, None),
        P(("sp", "tp"), None, None),
        P(("sp", "tp"), None, None),
        P(("grp", "sp", "tp"), None),
        P(("grp", "sp", "tp"), None),
    )
    out_specs = P(("grp", "sp", "tp"), None)
    return jax.shard_map(
        per_device, mesh=mesh, in_specs=in_specs, out_specs=out_specs, check_vma=False
    )
```

```python
import functools

import jax
import jax.numpy as jnp
from jax import lax
from jax.experimental import pallas as pl
from jax.experimental.pallas import tpu as pltpu
from jax.sharding import PartitionSpec as P

MESH_ID = pl.DeviceIdType.MESH
HDIM = 64
WINDOW = 128
CAP = 4
CORES = 2
EXPERTS_PER_GROUP = 32
SPAN = 4
FIRST = (0, 4, 12)
LAST = (3, 7, 9)
ENTRIES = 22
HOME = 22


rope_base = 10000.0
norm_eps = 1e-06


def expert_kernel(
    ring,
    xs,
    tile,
    query_ref,
    key_ref,
    value_ref,
    cos_ref,
    sin_ref,
    sink_ref,
    gain_ref,
    ids_ref,
    mix_ref,
    residual_hbm,
    proj_hbm,
    gate_hbm,
    up_hbm,
    down_hbm,
    out_ref,
    rot_q,
    keys_values,
    residual,
    proj_w,
    shares,
    far_in,
    near_in,
    own_share_sum,
    stream,
    normed,
    places,
    sums,
    total,
    pool,
    pool_meta,
    picked,
    routed,
    made,
    back,
    own_part,
    gate_w,
    up_w,
    down_w,
    weight_sem,
    pool_send,
    pool_recv,
    meta_send,
    meta_recv,
    pick_send,
    pick_recv,
    back_send,
    back_recv,
    sum_send,
    sum_recv,
    halo_send,
    halo_recv,
    far_send,
    far_recv,
    near_send,
    near_recv,
):
    f32, bf16 = jnp.float32, jnp.bfloat16
    rows, width = residual.shape
    half = rows // 2
    far = ring // 2
    peers = xs * CORES
    sp, tp = lax.axis_index("sp"), lax.axis_index("tp")
    core = lax.rem(sp, CORES)
    z = sp // CORES
    mine = core * xs + tp
    nxt = {"sp": lax.rem(sp + CORES, ring * CORES)}
    prv = {"sp": lax.rem(sp + (ring - 1) * CORES, ring * CORES)}

    def peer(offset):
        u = lax.rem(mine + offset, peers)
        return u, {"sp": z * CORES + u // xs, "tp": lax.rem(u, xs)}

    loads = [
        pltpu.make_async_copy(src, dst, weight_sem.at[i])
        for i, (src, dst) in enumerate(
            (
                (proj_hbm, proj_w),
                (residual_hbm, residual),
                (gate_hbm, gate_w),
                (up_hbm, up_w),
                (down_hbm, down_w),
            )
        )
    ]
    for load in loads:
        load.start()

    barrier = pltpu.get_barrier_semaphore()
    pl.semaphore_signal(barrier, inc=1, device_id=nxt, device_id_type=MESH_ID)
    pl.semaphore_signal(barrier, inc=1, device_id=prv, device_id_type=MESH_ID)
    total_sp = ring * CORES
    after = {"sp": lax.rem(sp + 1, total_sp)}
    across = {"sp": lax.rem(sp + jnp.where(core == 1, 1, total_sp - 1), total_sp)}
    pl.semaphore_signal(barrier, inc=1, device_id=across, device_id_type=MESH_ID)
    for o in range(1, peers):
        pl.semaphore_signal(barrier, inc=1, device_id=peer(o)[1], device_id_type=MESH_ID)

    lane = lax.broadcasted_iota(jnp.int32, (query_ref.shape[1],) * 2, 1)
    line = lax.broadcasted_iota(jnp.int32, (query_ref.shape[1],) * 2, 0)
    low = lax.rem(lane, HDIM) < HDIM // 2
    turn = jnp.where(low & (line == lane + HDIM // 2), -1.0, 0.0)
    turn = (turn + jnp.where((~low) & (line == lane - HDIM // 2), 1.0, 0.0)).astype(bf16)

    def rotated(x, cosines, sines):
        n = x.shape[1]
        swapped = jnp.dot(x, turn[:n, :n], preferred_element_type=f32)
        return (x.astype(f32) * cosines + swapped * sines).astype(bf16)

    tok = query_ref.shape[0]
    keys_values[WINDOW:, 0:HDIM] = rotated(key_ref[...], cos_ref[:, 0:HDIM], sin_ref[:, 0:HDIM])
    keys_values[WINDOW:, HDIM:] = value_ref[...]
    pl.semaphore_wait(barrier, peers + 2)
    halo = pltpu.make_async_remote_copy(
        src_ref=keys_values.at[pl.ds(tok, WINDOW)],
        dst_ref=keys_values.at[pl.ds(0, WINDOW)],
        send_sem=halo_send,
        recv_sem=halo_recv,
        device_id=after,
        device_id_type=MESH_ID,
    )
    halo.start()
    for c in range(query_ref.shape[1] // 128):
        cols = pl.ds(c * 128, 128)
        rot_q[:, cols] = rotated(query_ref[:, cols], cos_ref[...], sin_ref[...])
    halo.wait_recv()

    def part(h):
        return pl.ds(h * half, half)

    block, at = z // SPAN, lax.rem(z, SPAN)
    opposite_way = jnp.where(at >= SPAN // 2, 0, 1)
    ends = (at, SPAN - 1 - at)
    onward = (nxt, prv)
    room = 2 * peers * CAP

    def origin(way, d):
        i = lax.rem(ends[way] - d + 3 * SPAN, SPAN)
        return i, (d + i - ends[way]) // SPAN

    def passes(way, kind, d):
        i, crossed = origin(way, d)
        there = (d <= LAST[kind]) & (kind >= crossed)
        return there & (i >= SPAN // 2) if kind == 2 else there

    def is_mine(way, kind, d):
        return origin(way, d)[1] == kind

    def send_chunk(way, kind, d, count):
        entry = FIRST[kind] + d
        return pltpu.make_async_remote_copy(
            src_ref=pool.at[way, entry, pl.ds(0, count)],
            dst_ref=pool.at[way, entry + 1, pl.ds(0, count)],
            send_sem=pool_send.at[way, entry],
            recv_sem=pool_recv.at[way, entry + 1],
            device_id=onward[way],
            device_id_type=MESH_ID,
        )

    def send_meta(way, kind, d):
        entry = FIRST[kind] + d
        return pltpu.make_async_remote_copy(
            src_ref=pool_meta.at[way, entry],
            dst_ref=pool_meta.at[way, entry + 1],
            send_sem=meta_send.at[way, entry],
            recv_sem=meta_recv.at[way, entry + 1],
            device_id=onward[way],
            device_id_type=MESH_ID,
        )

    def forwards(way, kind, d):
        goes = passes(way, kind, d)
        mine_here = is_mine(way, kind, d)
        whole = goes & jnp.where(mine_here, ends[way] < SPAN - 2, True)
        return whole, goes & mine_here & (ends[way] == SPAN - 2)

    def forward(way, kind, d, act):
        whole, first = forwards(way, kind, d)

        @pl.when(whole)
        def _():
            act(send_chunk(way, kind, d, room), send_meta(way, kind, d))

        @pl.when(first)
        def _():
            act(send_chunk(way, kind, d, room // 2), send_meta(way, kind, d))

    def start_both(chunk, about):
        about.start()
        chunk.start()

    def wait_sent(chunk, about):
        about.wait_send()
        chunk.wait_send()

    def receive(way, kind, d):
        goes = passes(way, kind, d)
        short = is_mine(way, kind, d) & (ends[way] == SPAN - 1)

        @pl.when(goes)
        def _():
            send_meta(way, kind, d - 1).wait_recv()

        @pl.when(goes & ~short)
        def _():
            send_chunk(way, kind, d - 1, room).wait_recv()

        @pl.when(goes & short)
        def _():
            send_chunk(way, kind, d - 1, room // 2).wait_recv()
            pool[way, FIRST[kind] + d, pl.ds(room // 2, room // 2)] = jnp.zeros(
                (room // 2, width), bf16
            )

    q_at = lax.broadcasted_iota(jnp.int32, (WINDOW, 2 * WINDOW), 0)
    k_at = lax.broadcasted_iota(jnp.int32, (WINDOW, 2 * WINDOW), 1)
    reach = q_at + WINDOW - k_at

    def projected(block):
        start = pl.multiple_of(block * WINDOW, WINDOW)
        first = start + sp * tok
        allowed = (reach >= 0) & (reach < WINDOW) & (k_at + first >= WINDOW)
        kv = keys_values[pl.ds(start, 2 * WINDOW), :]
        k, v = kv[:, 0:HDIM], kv[:, HDIM:]
        q = rot_q[pl.ds(start, WINDOW), :]
        heads = []
        for h in range(q.shape[1] // HDIM):
            qh = q[:, h * HDIM : (h + 1) * HDIM]
            s = lax.dot_general(qh, k, (((1,), (1,)), ((), ())), preferred_element_type=f32)
            s = jnp.where(allowed, s * HDIM ** (-0.5), -jnp.inf)
            sink = sink_ref[h]
            top = jnp.maximum(jnp.max(s, axis=1, keepdims=True), sink)
            e = jnp.exp(s - top)
            below = jnp.sum(e, axis=1, keepdims=True) + jnp.exp(sink - top)
            p = (e / below).astype(bf16)
            heads.append(jnp.dot(p, v, preferred_element_type=f32).astype(bf16))
        att = jnp.concatenate(heads, axis=1)
        for c in range(width // tile):
            cols = pl.ds(c * tile, tile)
            yield cols, jnp.dot(att, proj_w[:, cols], preferred_element_type=f32)

    def beside(step):
        return {"tp": lax.rem(tp + step + xs, xs)}

    quarter = half // 2

    def send_far(way, h):
        at = h * half + way * quarter
        return pltpu.make_async_remote_copy(
            src_ref=shares.at[2, pl.ds(at, quarter)],
            dst_ref=far_in.at[way, h],
            send_sem=far_send.at[way, h],
            recv_sem=far_recv.at[way, h],
            device_id=beside(1 - 2 * way),
            device_id_type=MESH_ID,
        )

    def send_near(way, h):
        return pltpu.make_async_remote_copy(
            src_ref=shares.at[way, part(h)],
            dst_ref=near_in.at[way, h],
            send_sem=near_send.at[way, h],
            recv_sem=near_recv.at[way, h],
            device_id=beside(1 - 2 * way),
            device_id_type=MESH_ID,
        )

    loads[0].wait()
    for cols, y in projected(lax.rem(tp + 2, xs)):
        shares[2, :, cols] = y.astype(bf16)
    for h in range(2):
        for way in range(2):
            send_far(way, h).start()
    for way in range(2):
        for cols, y in projected(lax.rem(tp + 1 - 2 * way + xs, xs)):
            own_share_sum[:, cols] = y
        for h in range(2):
            send_far(way, h).wait_recv()
            joint = pl.ds(h * half + way * quarter, quarter)
            alone = pl.ds(h * half + (1 - way) * quarter, quarter)
            shares[way, alone] = own_share_sum[alone].astype(bf16)
            joined = own_share_sum[joint] + far_in[way, h].astype(f32)
            shares[way, joint] = joined.astype(bf16)
            send_near(way, h).start()
    for cols, y in projected(tp):
        own_share_sum[:, cols] = y
    loads[1].wait()

    def own_rows(h):
        for way in range(2):
            send_near(way, h).wait_recv()
        got = near_in[0, h].astype(f32) + near_in[1, h].astype(f32)
        x = residual[part(h)].astype(f32) + (own_share_sum[part(h)] + got)
        x = x.astype(bf16)
        stream[part(h)] = x
        x = x.astype(f32)
        scale = lax.rsqrt(jnp.mean(x * x, axis=1, keepdims=True) + norm_eps)
        normed[part(h)] = (x * scale * gain_ref[...]).astype(bf16)

    ids = ids_ref[...]
    expert_at = lax.broadcasted_iota(jnp.int32, (ring * peers, rows), 0)
    token_row = lax.broadcasted_iota(jnp.int32, (rows, rows), 0)
    token_col = lax.broadcasted_iota(jnp.int32, (rows, rows), 1)
    ahead = (token_row < token_col).astype(f32).astype(bf16)
    named = [(expert_at == ids[c : c + 1]).astype(f32) for c in range(2)]
    earlier = jnp.dot((named[0] + named[1]).astype(bf16), ahead, preferred_element_type=f32)
    ranks = [jnp.sum(n * earlier, axis=0, keepdims=True) for n in named]
    group = ids[0:1] // EXPERTS_PER_GROUP
    chip = [ids[c : c + 1] // peers for c in range(2)]
    spot = [lax.rem(c, SPAN) for c in chip]
    blocks = ring // SPAN
    apart = lax.rem(group - block + blocks, blocks)
    top = [(spot[0] == SPAN - 1) | (spot[1] == SPAN - 1), (spot[0] == 0) | (spot[1] == 0)]
    beyond = [(spot[0] > at) | (spot[1] > at), (spot[0] < at) | (spot[1] < at)]
    here = (chip[0] == z) | (chip[1] == z)
    joins = [
        (apart == 0) & beyond[0],
        apart == 1,
        (apart == 0) & beyond[1],
        apart == blocks - 1,
        apart == 2,
        here,
    ]
    joins = [x.astype(f32) for x in joins]
    top = [x.astype(f32) for x in top]
    leads = [top[0], top[0], top[1], top[1], jnp.where(at >= SPAN // 2, top[0], top[1]), top[0]]
    pack_row = lax.broadcasted_iota(jnp.int32, (8, rows), 0)
    lead, rest = jnp.zeros((8, rows), f32), jnp.zeros((8, rows), f32)
    for n in range(6):
        lead = jnp.where(pack_row == n, joins[n] * leads[n], lead)
        rest = jnp.where(pack_row == n, joins[n] * (1.0 - leads[n]), rest)
    lead_rank = jnp.dot(lead.astype(bf16), ahead, preferred_element_type=f32)
    rest_rank = jnp.dot(rest.astype(bf16), ahead, preferred_element_type=f32)
    rest_rank += jnp.sum(lead, axis=1, keepdims=True)
    places[...] = jnp.where(lead > 0, lead_rank, jnp.where(rest > 0, rest_rank, -1.0))
    mix = mix_ref[...]
    mix_high = mix.astype(bf16).astype(f32)
    mix_low = mix - mix_high
    facts_row = lax.broadcasted_iota(jnp.int32, (16, rows), 0)
    facts = jnp.where(facts_row == 8, 1.0, 0.0)
    known = [ids[0:1].astype(f32), ids[1:2].astype(f32), ranks[0], ranks[1]]
    known += [mix_high[0:1], mix_high[1:2], mix_low[0:1], mix_low[1:2]]
    for n in range(8):
        facts = jnp.where(facts_row == n, known[n], facts)
    facts = facts.astype(bf16)
    chunk_row = lax.broadcasted_iota(jnp.int32, (room, rows), 0).astype(f32)

    def packing(n):
        return (chunk_row == places[n : n + 1, :]).astype(f32).astype(bf16)

    def pack(n, way, entry):
        choose = packing(n)
        for c in range(width // tile):
            cols = pl.ds(c * tile, tile)
            got = jnp.dot(choose, normed[:, cols], preferred_element_type=f32)
            pool[way, entry, :, cols] = got.astype(bf16)

    def pack_meta(n, way, entry):
        got = lax.dot_general(
            facts, packing(n), (((1,), (1,)), ((), ())), preferred_element_type=f32
        )
        out_row = lax.broadcasted_iota(jnp.int32, (8, room), 0)
        found = got[8:9] > 0
        out = jnp.where(out_row == 0, jnp.where(found, got[0:1] * CAP + got[2:3], -1.0), 0.0)
        out = jnp.where(out_row == 1, jnp.where(found, got[1:2] * CAP + got[3:4], -1.0), out)
        out = jnp.where(out_row == 2, got[4:5] + got[6:7], out)
        out = jnp.where(out_row == 3, got[5:6] + got[7:8], out)
        pool_meta[way, entry] = jnp.concatenate([out, jnp.zeros_like(out)], axis=1)

    packs = ((4, opposite_way, 2), (1, 0, 1), (3, 1, 1), (0, 0, 0), (2, 1, 0))
    for n, way, kind in packs:
        pack_meta(n, way, FIRST[kind])
    pack_meta(5, 0, HOME)

    own_rows(0)
    own_rows(1)
    for n, way, kind in packs:
        pack(n, way, FIRST[kind])
        if kind == 2:
            for w in range(2):
                forward(w, 2, 0, start_both)
        else:
            forward(way, kind, 0, start_both)
    pack(5, 0, HOME)

    row_id = lax.broadcasted_iota(jnp.int32, (room, room), 0)
    local_code = (row_id // (2 * CAP)) * CAP + lax.rem(row_id, CAP)
    which_half = lax.rem(row_id, 2 * CAP) // CAP
    base = z * (peers * CAP)

    def locate(back):
        other = back > at + SPAN + SPAN // 2
        d = jnp.where(other, ring - back, back)
        end = jnp.where(other, ends[1], ends[0])
        i = lax.rem(end - d + 3 * SPAN, SPAN)
        crossed = (d + i - end) // SPAN
        first = jnp.where(crossed == 0, FIRST[0], jnp.where(crossed == 1, FIRST[1], FIRST[2]))
        entry = jnp.where(back == 0, HOME, first + d)
        return jnp.where(other, 1, 0), entry

    def matches(way, entry, side):
        code = jnp.where(which_half == side, local_code + base, -2).astype(f32)
        m = pool_meta[way, entry][:, 0:room]
        return code == m[0:1, :], code == m[1:2, :], m

    def pick_of(way, entry, side):
        first_hit, second_hit, _ = matches(way, entry, side)
        return (first_hit | second_hit).astype(f32).astype(bf16)

    def weights_of(way, entry, side):
        first_hit, second_hit, m = matches(way, entry, side)
        w = jnp.where(first_hit, m[2:3, :], 0.0) + jnp.where(second_hit, m[3:4, :], 0.0)
        high = w.astype(bf16)
        return high, (w - high.astype(f32)).astype(bf16)

    def exchange(src, dst, sends, recvs, step, offset):
        u, where = peer(offset)
        return pltpu.make_async_remote_copy(
            src_ref=src.at[step, u],
            dst_ref=dst.at[step, mine],
            send_sem=sends.at[step, offset],
            recv_sem=recvs.at[step, offset],
            device_id=where,
            device_id_type=MESH_ID,
        )

    def pick(step):
        a, b = locate(step), locate(ring - 1 - step)
        one_a, one_b = pick_of(*a, 0), pick_of(*b, 1)
        for c in range(width // tile):
            cols = pl.ds(c * tile, tile)
            got = jnp.dot(one_a, pool[a[0], a[1], :, cols], preferred_element_type=f32)
            got += jnp.dot(one_b, pool[b[0], b[1], :, cols], preferred_element_type=f32)
            got = got.astype(bf16).reshape(peers, 2 * CAP, tile)
            picked[step, :, :, cols] = got
        for o in range(1, peers):
            exchange(picked, routed, pick_send, pick_recv, step, o).start()
        routed[step, mine] = picked[step, mine]

    def serve(step):
        for o in range(1, peers):
            exchange(picked, routed, pick_send, pick_recv, step, o).wait_recv()
        x = routed[step].reshape(peers * 2 * CAP, width)
        g = jnp.dot(x, gate_w[...], preferred_element_type=f32)
        u = jnp.dot(x, up_w[...], preferred_element_type=f32)
        hidden = (g * (1.0 / (1.0 + jnp.exp(-g))) * u).astype(bf16)
        for c in range(width // tile):
            cols = pl.ds(c * tile, tile)
            y = jnp.dot(hidden, down_w[:, cols], preferred_element_type=f32)
            made[step, :, :, cols] = y.astype(bf16).reshape(peers, 2 * CAP, tile)
        for o in range(1, peers):
            exchange(made, back, back_send, back_recv, step, o).start()
        back[step, mine] = made[step, mine]

    def ring_step(d, _):
        for kind in (2, 1, 0):
            for way in range(2):
                receive(way, kind, d)
                forward(way, kind, d, start_both)

        @pl.when(d <= far - 2)
        def _():
            pick(d - 1)

        @pl.when((d >= 2) & (d <= far - 1))
        def _():
            serve(d - 2)

        return 0

    for load in loads[2:]:
        load.wait()
    lax.fori_loop(1, LAST[2] + 1, ring_step, 0)
    pick(far - 2)
    pick(far - 1)
    serve(far - 2)
    serve(far - 1)

    contract = (((0,), (0,)), ((), ()))

    def wait_back(step):
        for o in range(1, peers):
            exchange(made, back, back_send, back_recv, step, o).wait_recv()

    def own_share(way, entry, behind, dst):
        side = jnp.where(behind >= far, 1, 0)
        step = jnp.where(behind >= far, ring - 1 - behind, behind)
        high, low = weights_of(way, entry, side)
        w = jnp.concatenate([high, low], axis=0)
        for c in range(width // tile):
            cols = pl.ds(c * tile, tile)
            y = back[step, :, :, cols].reshape(room, tile)
            y = jnp.concatenate([y, y], axis=0)
            dst[:, cols] = lax.dot_general(w, y, contract, preferred_element_type=f32)

    def send_sum(way, kind, d, count):
        entry = FIRST[kind] + d
        return pltpu.make_async_remote_copy(
            src_ref=sums.at[way, entry, pl.ds(0, count)],
            dst_ref=sums.at[way, entry - 1, pl.ds(0, count)],
            send_sem=sum_send.at[way, entry],
            recv_sem=sum_recv.at[way, entry - 1],
            device_id=onward[1 - way],
            device_id_type=MESH_ID,
        )

    def give_back(way, kind, d, act):
        goes = passes(way, kind, d)
        short = is_mine(way, kind, d) & (ends[way] == SPAN - 1)

        @pl.when(goes & ~short)
        def _():
            act(send_sum(way, kind, d, room))

        @pl.when(goes & short)
        def _():
            act(send_sum(way, kind, d, room // 2))

    first_rows, last_rows = pl.ds(0, room // 2), pl.ds(room // 2, room // 2)

    def sum_entry(way, kind, d):
        entry = FIRST[kind] + d
        goes = passes(way, kind, d)
        mine_here = is_mine(way, kind, d)
        end = ends[way]

        @pl.when(goes & (~mine_here | (end < SPAN - 2)))
        def _():
            send_sum(way, kind, d + 1, room).wait_recv()

        @pl.when(goes & mine_here & (end < SPAN - 2))
        def _():
            sums[way, entry] = (sums[way, entry].astype(f32) + own_part[way]).astype(bf16)

        @pl.when(goes & mine_here & (end == SPAN - 2))
        def _():
            sums[way, entry, last_rows] = own_part[way, last_rows].astype(bf16)
            send_sum(way, kind, d + 1, room // 2).wait_recv()
            got = sums[way, entry, first_rows].astype(f32) + own_part[way, first_rows]
            sums[way, entry, first_rows] = got.astype(bf16)

        @pl.when(goes & mine_here & (end == SPAN - 1))
        def _():
            sums[way, entry, first_rows] = own_part[way, first_rows].astype(bf16)

        give_back(way, kind, d, lambda copy: copy.start())

    wait_back(far - 1)
    wait_back(far - 2)

    def sum_step(i, _):
        d = LAST[2] - i

        @pl.when(d <= far - 2)
        def _():
            wait_back(d - 1)

        for kind in range(3):
            for way in range(2):

                @pl.when(passes(way, kind, d) & is_mine(way, kind, d))
                def _():
                    behind = d if way == 0 else ring - d
                    own_share(way, FIRST[kind] + d, behind, own_part.at[way])

        for kind in range(3):
            for way in range(2):
                sum_entry(way, kind, d)
        return 0

    lax.fori_loop(0, LAST[2], sum_step, 0)
    own_share(0, HOME, 0, own_part.at[0])

    def place(n, value):
        choose = packing(n)
        for c in range(width // tile):
            cols = pl.ds(c * tile, tile)
            got = lax.dot_general(choose, value(cols), contract, preferred_element_type=f32)
            total[:, cols] += got

    total[...] = stream[...].astype(f32)
    place(5, lambda cols: own_part[0, :, cols].astype(bf16))

    def land(n, way, kind):
        whole, first = forwards(way, kind, 0)

        @pl.when(whole)
        def _():
            send_sum(way, kind, 1, room).wait_recv()

        @pl.when(first)
        def _():
            send_sum(way, kind, 1, room // 2).wait_recv()
            sums[way, FIRST[kind], last_rows] = jnp.zeros((room // 2, width), bf16)

        @pl.when(whole | first)
        def _():
            place(n, lambda cols: sums[way, FIRST[kind], :, cols])

    for n, way, kind in ((0, 0, 0), (2, 1, 0), (1, 0, 1), (3, 1, 1)):
        land(n, way, kind)
    for way in range(2):
        land(4, way, 2)
    out_ref[...] = total[...].astype(bf16)

    def drain(d, _):
        for kind in range(3):
            for way in range(2):
                forward(way, kind, d, wait_sent)

                @pl.when(d >= 1)
                def _():
                    give_back(way, kind, d, lambda copy: copy.wait_send())

        return 0

    lax.fori_loop(0, LAST[2] + 1, drain, 0)

    def drain_steps(n, _):
        for o in range(1, peers):
            exchange(picked, routed, pick_send, pick_recv, n, o).wait_send()
            exchange(made, back, back_send, back_recv, n, o).wait_send()
        return 0

    lax.fori_loop(0, far, drain_steps, 0)
    halo.wait_send()
    for h in range(2):
        for way in range(2):
            send_far(way, h).wait_send()
            send_near(way, h).wait_send()


def layer(query, key, value, cosines, sines, sinks, gain, ids, mix, residual, proj, gate, up, down):
    rows, width = residual.shape
    ring = lax.axis_size("sp") // CORES
    xs = lax.axis_size("tp")
    far = ring // 2
    peers = xs * CORES
    hidden = gate.shape[1]
    room = 2 * peers * CAP
    tile = min(512, width)
    bf16, f32 = jnp.bfloat16, jnp.float32
    vmem = pl.BlockSpec(memory_space=pltpu.VMEM)
    smem = pl.BlockSpec(memory_space=pltpu.SMEM)
    hbm = pl.BlockSpec(memory_space=pl.ANY)
    slab = (far, peers, 2 * CAP, width)
    dma = pltpu.SemaphoreType.DMA
    return pl.pallas_call(
        functools.partial(expert_kernel, ring, xs, tile),
        out_shape=jax.ShapeDtypeStruct((rows, width), bf16),
        in_specs=[vmem] * 5 + [smem] + [vmem] * 3 + [hbm] * 5,
        out_specs=vmem,
        scratch_shapes=[
            pltpu.VMEM(query.shape, bf16),
            pltpu.VMEM((query.shape[0] + WINDOW, 2 * HDIM), bf16),
            pltpu.VMEM((rows, width), bf16),
            pltpu.VMEM(proj.shape, bf16),
            pltpu.VMEM((3, rows, width), bf16),
            pltpu.VMEM((2, 2, rows // 4, width), bf16),
            pltpu.VMEM((2, 2, rows // 2, width), bf16),
            pltpu.VMEM((rows, width), f32),
            pltpu.VMEM((rows, width), bf16),
            pltpu.VMEM((rows, width), bf16),
            pltpu.VMEM((8, rows), f32),
            pltpu.VMEM((2, ENTRIES, room, width), bf16),
            pltpu.VMEM((rows, width), f32),
            pltpu.VMEM((2, ENTRIES + 1, room, width), bf16),
            pltpu.VMEM((2, ENTRIES + 1, 8, rows), f32),
            pltpu.VMEM(slab, bf16),
            pltpu.VMEM(slab, bf16),
            pltpu.VMEM(slab, bf16),
            pltpu.VMEM(slab, bf16),
            pltpu.VMEM((2, room, width), f32),
            pltpu.VMEM((width, hidden), bf16),
            pltpu.VMEM((width, hidden), bf16),
            pltpu.VMEM((hidden, width), bf16),
            dma((5,)),
            dma((2, ENTRIES)),
            dma((2, ENTRIES)),
            dma((2, ENTRIES)),
            dma((2, ENTRIES)),
            dma((far, peers)),
            dma((far, peers)),
            dma((far, peers)),
            dma((far, peers)),
            dma((2, ENTRIES)),
            dma((2, ENTRIES)),
            dma,
            dma,
            dma((2, 2)),
            dma((2, 2)),
            dma((2, 2)),
            dma((2, 2)),
        ],
        compiler_params=pltpu.CompilerParams(
            collective_id=1, has_side_effects=True, vmem_limit_bytes=60 * 1024 * 1024
        ),
    )(query, key, value, cosines, sines, sinks, gain, ids, mix, residual, proj, gate, up, down)


def per_device(
    query_rows,
    key_rows,
    value_rows,
    sink_logits,
    residual,
    out_weight,
    norm_gain,
    gate_weight,
    up_weight,
    down_weight,
    routes,
    route_weight,
):
    tok_count = query_rows.shape[0]
    positions = lax.axis_index("sp") * tok_count + jnp.arange(tok_count, dtype=jnp.int32)
    half_dim = HDIM // 2
    inverse = rope_base ** (-jnp.arange(half_dim, dtype=jnp.float32) / half_dim)
    angles = positions.astype(jnp.float32)[:, None] * inverse[None, :]
    cosines = jnp.tile(jnp.cos(angles), (1, 128 // half_dim))
    sines = jnp.tile(jnp.sin(angles), (1, 128 // half_dim))
    return layer(
        query_rows,
        key_rows,
        value_rows,
        cosines,
        sines,
        sink_logits,
        norm_gain[None, :],
        routes.T,
        route_weight.T,
        residual,
        out_weight,
        gate_weight[0],
        up_weight[0],
        down_weight[0],
    )


def solution(mesh):
    in_specs = (
        P(("grp", "sp"), "tp"),
        P(("grp", "sp"), "tp"),
        P(("grp", "sp"), "tp"),
        P("tp"),
        P(("grp", "sp", "tp"), None),
        P("tp", None),
        P(),
        P(("sp", "tp"), None, None),
        P(("sp", "tp"), None, None),
        P(("sp", "tp"), None, None),
        P(("grp", "sp", "tp"), None),
        P(("grp", "sp", "tp"), None),
    )
    out_specs = P(("grp", "sp", "tp"), None)
    return jax.shard_map(
        per_device, mesh=mesh, in_specs=in_specs, out_specs=out_specs, check_vma=False
    )
```

```python
import functools

import jax
import jax.numpy as jnp
from jax import lax
from jax.experimental import pallas as pl
from jax.experimental.pallas import tpu as pltpu
from jax.sharding import PartitionSpec as P

MESH_ID = pl.DeviceIdType.MESH
HDIM = 64
WINDOW = 128
CAP = 4
CORES = 2
EXPERTS_PER_GROUP = 32
SPAN = 4
FIRST = (0, 4, 12)
LAST = (3, 7, 9)
ENTRIES = 22
HOME = 22


rope_base = 10000.0
norm_eps = 1e-06


def expert_kernel(
    ring,
    xs,
    tile,
    query_ref,
    key_ref,
    value_ref,
    cos_ref,
    sin_ref,
    sink_ref,
    gain_ref,
    ids_ref,
    mix_ref,
    residual_hbm,
    proj_hbm,
    gate_hbm,
    up_hbm,
    down_hbm,
    out_ref,
    rot_q,
    keys_values,
    residual,
    proj_w,
    shares,
    far_in,
    near_in,
    own_share_sum,
    stream,
    normed,
    places,
    sums,
    total,
    pool,
    pool_meta,
    picked,
    routed,
    made,
    back,
    own_part,
    gate_w,
    up_w,
    down_w,
    weight_sem,
    pool_send,
    pool_recv,
    meta_send,
    meta_recv,
    pick_send,
    pick_recv,
    back_send,
    back_recv,
    sum_send,
    sum_recv,
    halo_send,
    halo_recv,
    far_send,
    far_recv,
    near_send,
    near_recv,
):
    f32, bf16 = jnp.float32, jnp.bfloat16
    rows, width = residual.shape
    half = rows // 2
    far = ring // 2
    peers = xs * CORES
    sp, tp = lax.axis_index("sp"), lax.axis_index("tp")
    core = lax.rem(sp, CORES)
    z = sp // CORES
    mine = core * xs + tp
    nxt = {"sp": lax.rem(sp + CORES, ring * CORES)}
    prv = {"sp": lax.rem(sp + (ring - 1) * CORES, ring * CORES)}

    def peer(offset):
        u = lax.rem(mine + offset, peers)
        return u, {"sp": z * CORES + u // xs, "tp": lax.rem(u, xs)}

    loads = [
        pltpu.make_async_copy(src, dst, weight_sem.at[i])
        for i, (src, dst) in enumerate(
            (
                (proj_hbm, proj_w),
                (residual_hbm, residual),
                (gate_hbm, gate_w),
                (up_hbm, up_w),
                (down_hbm, down_w),
            )
        )
    ]
    for load in loads:
        load.start()

    barrier = pltpu.get_barrier_semaphore()
    pl.semaphore_signal(barrier, inc=1, device_id=nxt, device_id_type=MESH_ID)
    pl.semaphore_signal(barrier, inc=1, device_id=prv, device_id_type=MESH_ID)
    total_sp = ring * CORES
    after = {"sp": lax.rem(sp + 1, total_sp)}
    across = {"sp": lax.rem(sp + jnp.where(core == 1, 1, total_sp - 1), total_sp)}
    pl.semaphore_signal(barrier, inc=1, device_id=across, device_id_type=MESH_ID)
    for o in range(1, peers):
        pl.semaphore_signal(barrier, inc=1, device_id=peer(o)[1], device_id_type=MESH_ID)

    lane = lax.broadcasted_iota(jnp.int32, (query_ref.shape[1],) * 2, 1)
    line = lax.broadcasted_iota(jnp.int32, (query_ref.shape[1],) * 2, 0)
    low = lax.rem(lane, HDIM) < HDIM // 2
    turn = jnp.where(low & (line == lane + HDIM // 2), -1.0, 0.0)
    turn = (turn + jnp.where((~low) & (line == lane - HDIM // 2), 1.0, 0.0)).astype(bf16)

    def rotated(x, cosines, sines):
        n = x.shape[1]
        swapped = jnp.dot(x, turn[:n, :n], preferred_element_type=f32)
        return (x.astype(f32) * cosines + swapped * sines).astype(bf16)

    tok = query_ref.shape[0]
    k_low = key_ref[0 : HDIM // 2].astype(f32)
    k_high = key_ref[HDIM // 2 :].astype(f32)
    turned_low = k_low * cos_ref[...] - k_high * sin_ref[...]
    turned_high = k_high * cos_ref[...] + k_low * sin_ref[...]
    turned_k = jnp.concatenate([turned_low, turned_high], axis=0)
    keys_values[0:HDIM, WINDOW:] = turned_k.astype(bf16)
    keys_values[HDIM:, WINDOW:] = value_ref[...]
    pl.semaphore_wait(barrier, peers + 2)
    halo = pltpu.make_async_remote_copy(
        src_ref=keys_values.at[:, pl.ds(tok, WINDOW)],
        dst_ref=keys_values.at[:, pl.ds(0, WINDOW)],
        send_sem=halo_send,
        recv_sem=halo_recv,
        device_id=after,
        device_id_type=MESH_ID,
    )
    halo.start()
    repeats = 128 // (HDIM // 2)
    cosines = jnp.concatenate([cos_ref[...]] * repeats, axis=0).T
    sines = jnp.concatenate([sin_ref[...]] * repeats, axis=0).T
    for c in range(query_ref.shape[1] // 128):
        cols = pl.ds(c * 128, 128)
        rot_q[:, cols] = rotated(query_ref[:, cols], cosines, sines)
    halo.wait_recv()

    def part(h):
        return pl.ds(h * half, half)

    block, at = z // SPAN, lax.rem(z, SPAN)
    opposite_way = jnp.where(at >= SPAN // 2, 0, 1)
    ends = (at, SPAN - 1 - at)
    onward = (nxt, prv)
    room = 2 * peers * CAP

    def origin(way, d):
        i = lax.rem(ends[way] - d + 3 * SPAN, SPAN)
        return i, (d + i - ends[way]) // SPAN

    def passes(way, kind, d):
        i, crossed = origin(way, d)
        there = (d <= LAST[kind]) & (kind >= crossed)
        return there & (i >= SPAN // 2) if kind == 2 else there

    def is_mine(way, kind, d):
        return origin(way, d)[1] == kind

    def send_chunk(way, kind, d, count):
        entry = FIRST[kind] + d
        return pltpu.make_async_remote_copy(
            src_ref=pool.at[way, entry, pl.ds(0, count)],
            dst_ref=pool.at[way, entry + 1, pl.ds(0, count)],
            send_sem=pool_send.at[way, entry],
            recv_sem=pool_recv.at[way, entry + 1],
            device_id=onward[way],
            device_id_type=MESH_ID,
        )

    def send_meta(way, kind, d):
        entry = FIRST[kind] + d
        return pltpu.make_async_remote_copy(
            src_ref=pool_meta.at[way, entry],
            dst_ref=pool_meta.at[way, entry + 1],
            send_sem=meta_send.at[way, entry],
            recv_sem=meta_recv.at[way, entry + 1],
            device_id=onward[way],
            device_id_type=MESH_ID,
        )

    def forwards(way, kind, d):
        goes = passes(way, kind, d)
        mine_here = is_mine(way, kind, d)
        whole = goes & jnp.where(mine_here, ends[way] < SPAN - 2, True)
        return whole, goes & mine_here & (ends[way] == SPAN - 2)

    def forward(way, kind, d, act):
        whole, first = forwards(way, kind, d)

        @pl.when(whole)
        def _():
            act(send_chunk(way, kind, d, room), send_meta(way, kind, d))

        @pl.when(first)
        def _():
            act(send_chunk(way, kind, d, room // 2), send_meta(way, kind, d))

    def start_both(chunk, about):
        about.start()
        chunk.start()

    def wait_sent(chunk, about):
        about.wait_send()
        chunk.wait_send()

    def receive(way, kind, d):
        goes = passes(way, kind, d)
        short = is_mine(way, kind, d) & (ends[way] == SPAN - 1)

        @pl.when(goes)
        def _():
            send_meta(way, kind, d - 1).wait_recv()

        @pl.when(goes & ~short)
        def _():
            send_chunk(way, kind, d - 1, room).wait_recv()

        @pl.when(goes & short)
        def _():
            send_chunk(way, kind, d - 1, room // 2).wait_recv()
            pool[way, FIRST[kind] + d, pl.ds(room // 2, room // 2)] = jnp.zeros(
                (room // 2, width), bf16
            )

    q_at = lax.broadcasted_iota(jnp.int32, (WINDOW, 2 * WINDOW), 0)
    k_at = lax.broadcasted_iota(jnp.int32, (WINDOW, 2 * WINDOW), 1)
    reach = q_at + WINDOW - k_at

    def projected(block):
        start = pl.multiple_of(block * WINDOW, WINDOW)
        first = start + sp * tok
        allowed = (reach >= 0) & (reach < WINDOW) & (k_at + first >= WINDOW)
        k = keys_values[0:HDIM, pl.ds(start, 2 * WINDOW)]
        v = keys_values[HDIM:, pl.ds(start, 2 * WINDOW)]
        q = rot_q[pl.ds(start, WINDOW), :]
        heads = []
        for h in range(q.shape[1] // HDIM):
            qh = q[:, h * HDIM : (h + 1) * HDIM]
            s = jnp.dot(qh, k, preferred_element_type=f32)
            s = jnp.where(allowed, s * HDIM ** (-0.5), -jnp.inf)
            sink = sink_ref[h]
            top = jnp.maximum(jnp.max(s, axis=1, keepdims=True), sink)
            e = jnp.exp(s - top)
            below = jnp.sum(e, axis=1, keepdims=True) + jnp.exp(sink - top)
            p = (e / below).astype(bf16)
            seen = lax.dot_general(p, v, (((1,), (1,)), ((), ())), preferred_element_type=f32)
            heads.append(seen.astype(bf16))
        att = jnp.concatenate(heads, axis=1)
        for c in range(width // tile):
            cols = pl.ds(c * tile, tile)
            yield cols, jnp.dot(att, proj_w[:, cols], preferred_element_type=f32)

    def beside(step):
        return {"tp": lax.rem(tp + step + xs, xs)}

    quarter = half // 2

    def send_far(way, h):
        at = h * half + way * quarter
        return pltpu.make_async_remote_copy(
            src_ref=shares.at[2, pl.ds(at, quarter)],
            dst_ref=far_in.at[way, h],
            send_sem=far_send.at[way, h],
            recv_sem=far_recv.at[way, h],
            device_id=beside(1 - 2 * way),
            device_id_type=MESH_ID,
        )

    def send_near(way, h):
        return pltpu.make_async_remote_copy(
            src_ref=shares.at[way, part(h)],
            dst_ref=near_in.at[way, h],
            send_sem=near_send.at[way, h],
            recv_sem=near_recv.at[way, h],
            device_id=beside(1 - 2 * way),
            device_id_type=MESH_ID,
        )

    loads[0].wait()
    for cols, y in projected(lax.rem(tp + 2, xs)):
        shares[2, :, cols] = y.astype(bf16)
    for h in range(2):
        for way in range(2):
            send_far(way, h).start()
    for way in range(2):
        for cols, y in projected(lax.rem(tp + 1 - 2 * way + xs, xs)):
            own_share_sum[:, cols] = y
        for h in range(2):
            send_far(way, h).wait_recv()
            joint = pl.ds(h * half + way * quarter, quarter)
            alone = pl.ds(h * half + (1 - way) * quarter, quarter)
            shares[way, alone] = own_share_sum[alone].astype(bf16)
            joined = own_share_sum[joint] + far_in[way, h].astype(f32)
            shares[way, joint] = joined.astype(bf16)
            send_near(way, h).start()
    for cols, y in projected(tp):
        own_share_sum[:, cols] = y
    loads[1].wait()

    def own_rows(h):
        for way in range(2):
            send_near(way, h).wait_recv()
        got = near_in[0, h].astype(f32) + near_in[1, h].astype(f32)
        x = residual[part(h)].astype(f32) + (own_share_sum[part(h)] + got)
        x = x.astype(bf16)
        stream[part(h)] = x
        x = x.astype(f32)
        scale = lax.rsqrt(jnp.mean(x * x, axis=1, keepdims=True) + norm_eps)
        normed[part(h)] = (x * scale * gain_ref[...]).astype(bf16)

    ids = ids_ref[...]
    expert_at = lax.broadcasted_iota(jnp.int32, (ring * peers, rows), 0)
    token_row = lax.broadcasted_iota(jnp.int32, (rows, rows), 0)
    token_col = lax.broadcasted_iota(jnp.int32, (rows, rows), 1)
    ahead = (token_row < token_col).astype(f32).astype(bf16)
    named = [(expert_at == ids[c : c + 1]).astype(f32) for c in range(2)]
    earlier = jnp.dot((named[0] + named[1]).astype(bf16), ahead, preferred_element_type=f32)
    ranks = [jnp.sum(n * earlier, axis=0, keepdims=True) for n in named]
    group = ids[0:1] // EXPERTS_PER_GROUP
    chip = [ids[c : c + 1] // peers for c in range(2)]
    spot = [lax.rem(c, SPAN) for c in chip]
    blocks = ring // SPAN
    apart = lax.rem(group - block + blocks, blocks)
    top = [(spot[0] == SPAN - 1) | (spot[1] == SPAN - 1), (spot[0] == 0) | (spot[1] == 0)]
    beyond = [(spot[0] > at) | (spot[1] > at), (spot[0] < at) | (spot[1] < at)]
    here = (chip[0] == z) | (chip[1] == z)
    joins = [
        (apart == 0) & beyond[0],
        apart == 1,
        (apart == 0) & beyond[1],
        apart == blocks - 1,
        apart == 2,
        here,
    ]
    joins = [x.astype(f32) for x in joins]
    top = [x.astype(f32) for x in top]
    leads = [top[0], top[0], top[1], top[1], jnp.where(at >= SPAN // 2, top[0], top[1]), top[0]]
    pack_row = lax.broadcasted_iota(jnp.int32, (8, rows), 0)
    lead, rest = jnp.zeros((8, rows), f32), jnp.zeros((8, rows), f32)
    for n in range(6):
        lead = jnp.where(pack_row == n, joins[n] * leads[n], lead)
        rest = jnp.where(pack_row == n, joins[n] * (1.0 - leads[n]), rest)
    lead_rank = jnp.dot(lead.astype(bf16), ahead, preferred_element_type=f32)
    rest_rank = jnp.dot(rest.astype(bf16), ahead, preferred_element_type=f32)
    rest_rank += jnp.sum(lead, axis=1, keepdims=True)
    places[...] = jnp.where(lead > 0, lead_rank, jnp.where(rest > 0, rest_rank, -1.0))
    mix = mix_ref[...]
    mix_high = mix.astype(bf16).astype(f32)
    mix_low = mix - mix_high
    facts_row = lax.broadcasted_iota(jnp.int32, (16, rows), 0)
    facts = jnp.where(facts_row == 8, 1.0, 0.0)
    known = [ids[0:1].astype(f32), ids[1:2].astype(f32), ranks[0], ranks[1]]
    known += [mix_high[0:1], mix_high[1:2], mix_low[0:1], mix_low[1:2]]
    for n in range(8):
        facts = jnp.where(facts_row == n, known[n], facts)
    facts = facts.astype(bf16)
    chunk_row = lax.broadcasted_iota(jnp.int32, (room, rows), 0).astype(f32)

    def packing(n):
        return (chunk_row == places[n : n + 1, :]).astype(f32).astype(bf16)

    def pack(n, way, entry):
        choose = packing(n)
        for c in range(width // tile):
            cols = pl.ds(c * tile, tile)
            got = jnp.dot(choose, normed[:, cols], preferred_element_type=f32)
            pool[way, entry, :, cols] = got.astype(bf16)

    def pack_meta(n, way, entry):
        got = lax.dot_general(
            facts, packing(n), (((1,), (1,)), ((), ())), preferred_element_type=f32
        )
        out_row = lax.broadcasted_iota(jnp.int32, (8, room), 0)
        found = got[8:9] > 0
        out = jnp.where(out_row == 0, jnp.where(found, got[0:1] * CAP + got[2:3], -1.0), 0.0)
        out = jnp.where(out_row == 1, jnp.where(found, got[1:2] * CAP + got[3:4], -1.0), out)
        out = jnp.where(out_row == 2, got[4:5] + got[6:7], out)
        out = jnp.where(out_row == 3, got[5:6] + got[7:8], out)
        pool_meta[way, entry] = jnp.concatenate([out, jnp.zeros_like(out)], axis=1)

    packs = ((4, opposite_way, 2), (1, 0, 1), (3, 1, 1), (0, 0, 0), (2, 1, 0))
    for n, way, kind in packs:
        pack_meta(n, way, FIRST[kind])
    pack_meta(5, 0, HOME)

    own_rows(0)
    own_rows(1)
    for n, way, kind in packs:
        pack(n, way, FIRST[kind])
        if kind == 2:
            for w in range(2):
                forward(w, 2, 0, start_both)
        else:
            forward(way, kind, 0, start_both)
    pack(5, 0, HOME)

    row_id = lax.broadcasted_iota(jnp.int32, (room, room), 0)
    local_code = (row_id // (2 * CAP)) * CAP + lax.rem(row_id, CAP)
    which_half = lax.rem(row_id, 2 * CAP) // CAP
    base = z * (peers * CAP)

    def locate(back):
        other = back > at + SPAN + SPAN // 2
        d = jnp.where(other, ring - back, back)
        end = jnp.where(other, ends[1], ends[0])
        i = lax.rem(end - d + 3 * SPAN, SPAN)
        crossed = (d + i - end) // SPAN
        first = jnp.where(crossed == 0, FIRST[0], jnp.where(crossed == 1, FIRST[1], FIRST[2]))
        entry = jnp.where(back == 0, HOME, first + d)
        return jnp.where(other, 1, 0), entry

    def matches(way, entry, side):
        code = jnp.where(which_half == side, local_code + base, -2).astype(f32)
        m = pool_meta[way, entry][:, 0:room]
        return code == m[0:1, :], code == m[1:2, :], m

    def pick_of(way, entry, side):
        first_hit, second_hit, _ = matches(way, entry, side)
        return (first_hit | second_hit).astype(f32).astype(bf16)

    def weights_of(way, entry, side):
        first_hit, second_hit, m = matches(way, entry, side)
        w = jnp.where(first_hit, m[2:3, :], 0.0) + jnp.where(second_hit, m[3:4, :], 0.0)
        high = w.astype(bf16)
        return high, (w - high.astype(f32)).astype(bf16)

    def exchange(src, dst, sends, recvs, step, offset):
        u, where = peer(offset)
        return pltpu.make_async_remote_copy(
            src_ref=src.at[step, u],
            dst_ref=dst.at[step, mine],
            send_sem=sends.at[step, offset],
            recv_sem=recvs.at[step, offset],
            device_id=where,
            device_id_type=MESH_ID,
        )

    def pick(step):
        a, b = locate(step), locate(ring - 1 - step)
        one_a, one_b = pick_of(*a, 0), pick_of(*b, 1)
        for c in range(width // tile):
            cols = pl.ds(c * tile, tile)
            got = jnp.dot(one_a, pool[a[0], a[1], :, cols], preferred_element_type=f32)
            got += jnp.dot(one_b, pool[b[0], b[1], :, cols], preferred_element_type=f32)
            got = got.astype(bf16).reshape(peers, 2 * CAP, tile)
            picked[step, :, :, cols] = got
        for o in range(1, peers):
            exchange(picked, routed, pick_send, pick_recv, step, o).start()
        routed[step, mine] = picked[step, mine]

    def serve(step):
        for o in range(1, peers):
            exchange(picked, routed, pick_send, pick_recv, step, o).wait_recv()
        x = routed[step].reshape(peers * 2 * CAP, width)
        g = jnp.dot(x, gate_w[...], preferred_element_type=f32)
        u = jnp.dot(x, up_w[...], preferred_element_type=f32)
        hidden = (g * (1.0 / (1.0 + jnp.exp(-g))) * u).astype(bf16)
        for c in range(width // tile):
            cols = pl.ds(c * tile, tile)
            y = jnp.dot(hidden, down_w[:, cols], preferred_element_type=f32)
            made[step, :, :, cols] = y.astype(bf16).reshape(peers, 2 * CAP, tile)
        for o in range(1, peers):
            exchange(made, back, back_send, back_recv, step, o).start()
        back[step, mine] = made[step, mine]

    def ring_step(d, _):
        for kind in (2, 1, 0):
            for way in range(2):
                receive(way, kind, d)
                forward(way, kind, d, start_both)

        @pl.when(d <= far - 2)
        def _():
            pick(d - 1)

        @pl.when((d >= 2) & (d <= far - 1))
        def _():
            serve(d - 2)

        return 0

    for load in loads[2:]:
        load.wait()
    lax.fori_loop(1, LAST[2] + 1, ring_step, 0)
    contract = (((0,), (0,)), ((), ()))

    def wait_back(step):
        for o in range(1, peers):
            exchange(made, back, back_send, back_recv, step, o).wait_recv()

    def own_share(way, entry, behind, dst):
        side = jnp.where(behind >= far, 1, 0)
        step = jnp.where(behind >= far, ring - 1 - behind, behind)
        high, low = weights_of(way, entry, side)
        w = jnp.concatenate([high, low], axis=0)
        for c in range(width // tile):
            cols = pl.ds(c * tile, tile)
            y = back[step, :, :, cols].reshape(room, tile)
            y = jnp.concatenate([y, y], axis=0)
            dst[:, cols] = lax.dot_general(w, y, contract, preferred_element_type=f32)

    def send_sum(way, kind, d, count):
        entry = FIRST[kind] + d
        return pltpu.make_async_remote_copy(
            src_ref=sums.at[way, entry, pl.ds(0, count)],
            dst_ref=sums.at[way, entry - 1, pl.ds(0, count)],
            send_sem=sum_send.at[way, entry],
            recv_sem=sum_recv.at[way, entry - 1],
            device_id=onward[1 - way],
            device_id_type=MESH_ID,
        )

    def give_back(way, kind, d, act):
        goes = passes(way, kind, d)
        short = is_mine(way, kind, d) & (ends[way] == SPAN - 1)

        @pl.when(goes & ~short)
        def _():
            act(send_sum(way, kind, d, room))

        @pl.when(goes & short)
        def _():
            act(send_sum(way, kind, d, room // 2))

    first_rows, last_rows = pl.ds(0, room // 2), pl.ds(room // 2, room // 2)

    def sum_entry(way, kind, d):
        entry = FIRST[kind] + d
        goes = passes(way, kind, d)
        mine_here = is_mine(way, kind, d)
        end = ends[way]

        @pl.when(goes & (~mine_here | (end < SPAN - 2)))
        def _():
            send_sum(way, kind, d + 1, room).wait_recv()

        @pl.when(goes & mine_here & (end < SPAN - 2))
        def _():
            sums[way, entry] = (sums[way, entry].astype(f32) + own_part[way]).astype(bf16)

        @pl.when(goes & mine_here & (end == SPAN - 2))
        def _():
            sums[way, entry, last_rows] = own_part[way, last_rows].astype(bf16)
            send_sum(way, kind, d + 1, room // 2).wait_recv()
            got = sums[way, entry, first_rows].astype(f32) + own_part[way, first_rows]
            sums[way, entry, first_rows] = got.astype(bf16)

        @pl.when(goes & mine_here & (end == SPAN - 1))
        def _():
            sums[way, entry, first_rows] = own_part[way, first_rows].astype(bf16)

        give_back(way, kind, d, lambda copy: copy.start())

    def return_kinds(kinds, d):
        for kind in kinds:
            for way in range(2):

                @pl.when(passes(way, kind, d) & is_mine(way, kind, d))
                def _():
                    behind = d if way == 0 else ring - d
                    own_share(way, FIRST[kind] + d, behind, own_part.at[way])

        for kind in kinds:
            for way in range(2):
                sum_entry(way, kind, d)

    def place(n, value):
        choose = packing(n)
        for c in range(width // tile):
            cols = pl.ds(c * tile, tile)
            got = lax.dot_general(choose, value(cols), contract, preferred_element_type=f32)
            total[:, cols] += got

    def land(n, way, kind):
        whole, first = forwards(way, kind, 0)

        @pl.when(whole)
        def _():
            send_sum(way, kind, 1, room).wait_recv()

        @pl.when(first)
        def _():
            send_sum(way, kind, 1, room // 2).wait_recv()
            sums[way, FIRST[kind], last_rows] = jnp.zeros((room // 2, width), bf16)

        @pl.when(whole | first)
        def _():
            place(n, lambda cols: sums[way, FIRST[kind], :, cols])

    pick(far - 2)
    pick(far - 1)
    wait_back(3)
    wait_back(2)
    return_kinds((0,), 3)
    serve(far - 2)
    wait_back(1)
    return_kinds((0,), 2)
    serve(far - 1)
    wait_back(0)
    return_kinds((0,), 1)
    own_share(0, HOME, 0, own_part.at[0])
    total[...] = stream[...].astype(f32)
    place(5, lambda cols: own_part[0, :, cols].astype(bf16))
    wait_back(far - 1)
    wait_back(far - 2)

    def sum_step(i, _):
        d = LAST[2] - i

        @pl.when((d <= far - 2) & (d >= 5))
        def _():
            wait_back(d - 1)

        return_kinds((1, 2), d)

        @pl.when(d == 4)
        def _():
            land(0, 0, 0)

        @pl.when(d == 3)
        def _():
            land(2, 1, 0)

        return 0

    lax.fori_loop(0, LAST[2], sum_step, 0)
    for n, way, kind in ((1, 0, 1), (3, 1, 1)):
        land(n, way, kind)
    for way in range(2):
        land(4, way, 2)
    out_ref[...] = total[...].astype(bf16)

    def drain(d, _):
        for kind in range(3):
            for way in range(2):
                forward(way, kind, d, wait_sent)

                @pl.when(d >= 1)
                def _():
                    give_back(way, kind, d, lambda copy: copy.wait_send())

        return 0

    lax.fori_loop(0, LAST[2] + 1, drain, 0)

    def drain_steps(n, _):
        for o in range(1, peers):
            exchange(picked, routed, pick_send, pick_recv, n, o).wait_send()
            exchange(made, back, back_send, back_recv, n, o).wait_send()
        return 0

    lax.fori_loop(0, far, drain_steps, 0)
    halo.wait_send()
    for h in range(2):
        for way in range(2):
            send_far(way, h).wait_send()
            send_near(way, h).wait_send()


def layer(query, key, value, cosines, sines, sinks, gain, ids, mix, residual, proj, gate, up, down):
    rows, width = residual.shape
    ring = lax.axis_size("sp") // CORES
    xs = lax.axis_size("tp")
    far = ring // 2
    peers = xs * CORES
    hidden = gate.shape[1]
    room = 2 * peers * CAP
    tile = min(512, width)
    bf16, f32 = jnp.bfloat16, jnp.float32
    vmem = pl.BlockSpec(memory_space=pltpu.VMEM)
    smem = pl.BlockSpec(memory_space=pltpu.SMEM)
    hbm = pl.BlockSpec(memory_space=pl.ANY)
    slab = (far, peers, 2 * CAP, width)
    dma = pltpu.SemaphoreType.DMA
    return pl.pallas_call(
        functools.partial(expert_kernel, ring, xs, tile),
        out_shape=jax.ShapeDtypeStruct((rows, width), bf16),
        in_specs=[vmem] * 5 + [smem] + [vmem] * 3 + [hbm] * 5,
        out_specs=vmem,
        scratch_shapes=[
            pltpu.VMEM(query.shape, bf16),
            pltpu.VMEM((2 * HDIM, query.shape[0] + WINDOW), bf16),
            pltpu.VMEM((rows, width), bf16),
            pltpu.VMEM(proj.shape, bf16),
            pltpu.VMEM((3, rows, width), bf16),
            pltpu.VMEM((2, 2, rows // 4, width), bf16),
            pltpu.VMEM((2, 2, rows // 2, width), bf16),
            pltpu.VMEM((rows, width), f32),
            pltpu.VMEM((rows, width), bf16),
            pltpu.VMEM((rows, width), bf16),
            pltpu.VMEM((8, rows), f32),
            pltpu.VMEM((2, ENTRIES, room, width), bf16),
            pltpu.VMEM((rows, width), f32),
            pltpu.VMEM((2, ENTRIES + 1, room, width), bf16),
            pltpu.VMEM((2, ENTRIES + 1, 8, rows), f32),
            pltpu.VMEM(slab, bf16),
            pltpu.VMEM(slab, bf16),
            pltpu.VMEM(slab, bf16),
            pltpu.VMEM(slab, bf16),
            pltpu.VMEM((2, room, width), f32),
            pltpu.VMEM((width, hidden), bf16),
            pltpu.VMEM((width, hidden), bf16),
            pltpu.VMEM((hidden, width), bf16),
            dma((5,)),
            dma((2, ENTRIES)),
            dma((2, ENTRIES)),
            dma((2, ENTRIES)),
            dma((2, ENTRIES)),
            dma((far, peers)),
            dma((far, peers)),
            dma((far, peers)),
            dma((far, peers)),
            dma((2, ENTRIES)),
            dma((2, ENTRIES)),
            dma,
            dma,
            dma((2, 2)),
            dma((2, 2)),
            dma((2, 2)),
            dma((2, 2)),
        ],
        compiler_params=pltpu.CompilerParams(
            collective_id=1, has_side_effects=True, vmem_limit_bytes=60 * 1024 * 1024
        ),
    )(query, key, value, cosines, sines, sinks, gain, ids, mix, residual, proj, gate, up, down)


def per_device(
    query_rows,
    key_rows,
    value_rows,
    sink_logits,
    residual,
    out_weight,
    norm_gain,
    gate_weight,
    up_weight,
    down_weight,
    routes,
    route_weight,
):
    tok_count = query_rows.shape[0]
    positions = lax.axis_index("sp") * tok_count + jnp.arange(tok_count, dtype=jnp.int32)
    half_dim = HDIM // 2
    inverse = rope_base ** (-jnp.arange(half_dim, dtype=jnp.float32) / half_dim)
    angles = positions.astype(jnp.float32)[None, :] * inverse[:, None]
    cosines = jnp.cos(angles)
    sines = jnp.sin(angles)
    return layer(
        query_rows,
        key_rows.T,
        value_rows.T,
        cosines,
        sines,
        sink_logits,
        norm_gain[None, :],
        routes.T,
        route_weight.T,
        residual,
        out_weight,
        gate_weight[0],
        up_weight[0],
        down_weight[0],
    )


def solution(mesh):
    in_specs = (
        P(("grp", "sp"), "tp"),
        P(("grp", "sp"), "tp"),
        P(("grp", "sp"), "tp"),
        P("tp"),
        P(("grp", "sp", "tp"), None),
        P("tp", None),
        P(),
        P(("sp", "tp"), None, None),
        P(("sp", "tp"), None, None),
        P(("sp", "tp"), None, None),
        P(("grp", "sp", "tp"), None),
        P(("grp", "sp", "tp"), None),
    )
    out_specs = P(("grp", "sp", "tp"), None)
    return jax.shard_map(
        per_device, mesh=mesh, in_specs=in_specs, out_specs=out_specs, check_vma=False
    )
```

```python
import functools

import jax
import jax.numpy as jnp
from jax import lax
from jax.experimental import pallas as pl
from jax.experimental.pallas import tpu as pltpu
from jax.sharding import PartitionSpec as P

MESH_ID = pl.DeviceIdType.MESH
HDIM = 64
WINDOW = 128
CAP = 4
CORES = 2
EXPERTS_PER_GROUP = 32
SPAN = 4
FIRST = (0, 4, 12)
LAST = (3, 7, 9)
ENTRIES = 22
HOME = 22


rope_base = 10000.0
norm_eps = 1e-06


def expert_kernel(
    ring,
    xs,
    tile,
    query_ref,
    key_ref,
    value_ref,
    cos_ref,
    sin_ref,
    sink_ref,
    gain_ref,
    ids_ref,
    mix_ref,
    residual_hbm,
    proj_hbm,
    gate_hbm,
    up_hbm,
    down_hbm,
    out_ref,
    rot_q,
    keys_values,
    residual,
    proj_w,
    shares,
    far_in,
    near_in,
    own_share_sum,
    stream,
    normed,
    places,
    sums,
    total,
    pool,
    pool_meta,
    picked,
    routed,
    made,
    back,
    own_part,
    gate_w,
    up_w,
    down_w,
    weight_sem,
    pool_send,
    pool_recv,
    meta_send,
    meta_recv,
    pick_send,
    pick_recv,
    back_send,
    back_recv,
    sum_send,
    sum_recv,
    halo_send,
    halo_recv,
    far_send,
    far_recv,
    near_send,
    near_recv,
):
    f32, bf16 = jnp.float32, jnp.bfloat16
    rows, width = residual.shape
    half = rows // 2
    far = ring // 2
    peers = xs * CORES
    sp, tp = lax.axis_index("sp"), lax.axis_index("tp")
    core = lax.rem(sp, CORES)
    z = sp // CORES
    mine = core * xs + tp
    nxt = {"sp": lax.rem(sp + CORES, ring * CORES)}
    prv = {"sp": lax.rem(sp + (ring - 1) * CORES, ring * CORES)}

    def peer(offset):
        u = lax.rem(mine + offset, peers)
        return u, {"sp": z * CORES + u // xs, "tp": lax.rem(u, xs)}

    loads = [
        pltpu.make_async_copy(src, dst, weight_sem.at[i])
        for i, (src, dst) in enumerate(
            (
                (proj_hbm, proj_w),
                (residual_hbm, residual),
                (gate_hbm, gate_w),
                (up_hbm, up_w),
                (down_hbm, down_w),
            )
        )
    ]
    for load in loads:
        load.start()

    barrier = pltpu.get_barrier_semaphore()
    pl.semaphore_signal(barrier, inc=1, device_id=nxt, device_id_type=MESH_ID)
    pl.semaphore_signal(barrier, inc=1, device_id=prv, device_id_type=MESH_ID)
    total_sp = ring * CORES
    after = {"sp": lax.rem(sp + 1, total_sp)}
    across = {"sp": lax.rem(sp + jnp.where(core == 1, 1, total_sp - 1), total_sp)}
    pl.semaphore_signal(barrier, inc=1, device_id=across, device_id_type=MESH_ID)
    block, at = z // SPAN, lax.rem(z, SPAN)
    opposite_way = jnp.where(at >= SPAN // 2, 0, 1)
    ends = (at, SPAN - 1 - at)

    def chips_on(count):
        return {"sp": lax.rem(sp + (count + ring) * CORES, total_sp)}

    def greet(count):
        pl.semaphore_signal(barrier, inc=1, device_id=chips_on(count), device_id_type=MESH_ID)

    greet(SPAN - ends[0])
    greet(ends[1] - SPAN)
    greet(jnp.where(opposite_way == 0, 2 * SPAN - ends[0], ends[1] - 2 * SPAN))
    for way in range(2):

        @pl.when(ends[way] == 0)
        def _():
            for d in range(1, SPAN + SPAN // 2 + 1):
                greet(d if way else -d)

    edge = (ends[0] == 0) | (ends[1] == 0)
    greetings = peers + 2 + 3 + jnp.where(edge, SPAN + SPAN // 2, 0)
    for o in range(1, peers):
        pl.semaphore_signal(barrier, inc=1, device_id=peer(o)[1], device_id_type=MESH_ID)

    lane = lax.broadcasted_iota(jnp.int32, (query_ref.shape[1],) * 2, 1)
    line = lax.broadcasted_iota(jnp.int32, (query_ref.shape[1],) * 2, 0)
    low = lax.rem(lane, HDIM) < HDIM // 2
    turn = jnp.where(low & (line == lane + HDIM // 2), -1.0, 0.0)
    turn = (turn + jnp.where((~low) & (line == lane - HDIM // 2), 1.0, 0.0)).astype(bf16)

    def rotated(x, cosines, sines):
        n = x.shape[1]
        swapped = jnp.dot(x, turn[:n, :n], preferred_element_type=f32)
        return (x.astype(f32) * cosines + swapped * sines).astype(bf16)

    tok = query_ref.shape[0]
    k_low = key_ref[0 : HDIM // 2].astype(f32)
    k_high = key_ref[HDIM // 2 :].astype(f32)
    turned_low = k_low * cos_ref[...] - k_high * sin_ref[...]
    turned_high = k_high * cos_ref[...] + k_low * sin_ref[...]
    turned_k = jnp.concatenate([turned_low, turned_high], axis=0)
    keys_values[0:HDIM, WINDOW:] = turned_k.astype(bf16)
    keys_values[HDIM:, WINDOW:] = value_ref[...]
    pl.semaphore_wait(barrier, greetings)
    halo = pltpu.make_async_remote_copy(
        src_ref=keys_values.at[:, pl.ds(tok, WINDOW)],
        dst_ref=keys_values.at[:, pl.ds(0, WINDOW)],
        send_sem=halo_send,
        recv_sem=halo_recv,
        device_id=after,
        device_id_type=MESH_ID,
    )
    halo.start()
    repeats = 128 // (HDIM // 2)
    cosines = jnp.concatenate([cos_ref[...]] * repeats, axis=0).T
    sines = jnp.concatenate([sin_ref[...]] * repeats, axis=0).T
    for c in range(query_ref.shape[1] // 128):
        cols = pl.ds(c * 128, 128)
        rot_q[:, cols] = rotated(query_ref[:, cols], cosines, sines)
    halo.wait_recv()

    def part(h):
        return pl.ds(h * half, half)

    onward = (nxt, prv)
    room = 2 * peers * CAP

    def origin(way, d):
        i = lax.rem(ends[way] - d + 3 * SPAN, SPAN)
        return i, (d + i - ends[way]) // SPAN

    def passes(way, kind, d):
        i, crossed = origin(way, d)
        there = (d <= LAST[kind]) & (kind >= crossed)
        return there & (i >= SPAN // 2) if kind == 2 else there

    def is_mine(way, kind, d):
        return origin(way, d)[1] == kind

    def send_chunk(way, kind, d, count):
        entry = FIRST[kind] + d
        return pltpu.make_async_remote_copy(
            src_ref=pool.at[way, entry, pl.ds(0, count)],
            dst_ref=pool.at[way, entry + 1, pl.ds(0, count)],
            send_sem=pool_send.at[way, entry],
            recv_sem=pool_recv.at[way, entry + 1],
            device_id=onward[way],
            device_id_type=MESH_ID,
        )

    def send_meta(way, kind, d):
        entry = FIRST[kind] + d
        return pltpu.make_async_remote_copy(
            src_ref=pool_meta.at[way, entry],
            dst_ref=pool_meta.at[way, entry + 1],
            send_sem=meta_send.at[way, entry],
            recv_sem=meta_recv.at[way, entry + 1],
            device_id=onward[way],
            device_id_type=MESH_ID,
        )

    def forwards(way, kind, d):
        goes = passes(way, kind, d)
        mine_here = is_mine(way, kind, d)
        whole = goes & jnp.where(mine_here, ends[way] < SPAN - 2, True)
        return whole, goes & mine_here & (ends[way] == SPAN - 2)

    def forward(way, kind, d, act):
        whole, first = forwards(way, kind, d)

        @pl.when(whole)
        def _():
            act(send_chunk(way, kind, d, room), send_meta(way, kind, d))

        @pl.when(first)
        def _():
            act(send_chunk(way, kind, d, room // 2), send_meta(way, kind, d))

    def start_both(chunk, about):
        about.start()
        chunk.start()

    def wait_sent(chunk, about):
        about.wait_send()
        chunk.wait_send()

    def receive(way, kind, d):
        goes = passes(way, kind, d)
        short = is_mine(way, kind, d) & (ends[way] == SPAN - 1)

        @pl.when(goes)
        def _():
            send_meta(way, kind, d - 1).wait_recv()

        @pl.when(goes & ~short)
        def _():
            send_chunk(way, kind, d - 1, room).wait_recv()

        @pl.when(goes & short)
        def _():
            send_chunk(way, kind, d - 1, room // 2).wait_recv()
            pool[way, FIRST[kind] + d, pl.ds(room // 2, room // 2)] = jnp.zeros(
                (room // 2, width), bf16
            )

    q_at = lax.broadcasted_iota(jnp.int32, (WINDOW, 2 * WINDOW), 0)
    k_at = lax.broadcasted_iota(jnp.int32, (WINDOW, 2 * WINDOW), 1)
    reach = q_at + WINDOW - k_at

    def projected(block):
        start = pl.multiple_of(block * WINDOW, WINDOW)
        first = start + sp * tok
        allowed = (reach >= 0) & (reach < WINDOW) & (k_at + first >= WINDOW)
        k = keys_values[0:HDIM, pl.ds(start, 2 * WINDOW)]
        v = keys_values[HDIM:, pl.ds(start, 2 * WINDOW)]
        q = rot_q[pl.ds(start, WINDOW), :]
        heads = []
        for h in range(q.shape[1] // HDIM):
            qh = q[:, h * HDIM : (h + 1) * HDIM]
            s = jnp.dot(qh, k, preferred_element_type=f32)
            s = jnp.where(allowed, s * HDIM ** (-0.5), -jnp.inf)
            sink = sink_ref[h]
            top = jnp.maximum(jnp.max(s, axis=1, keepdims=True), sink)
            e = jnp.exp(s - top)
            below = jnp.sum(e, axis=1, keepdims=True) + jnp.exp(sink - top)
            p = (e / below).astype(bf16)
            seen = lax.dot_general(p, v, (((1,), (1,)), ((), ())), preferred_element_type=f32)
            heads.append(seen.astype(bf16))
        att = jnp.concatenate(heads, axis=1)
        for c in range(width // tile):
            cols = pl.ds(c * tile, tile)
            yield cols, jnp.dot(att, proj_w[:, cols], preferred_element_type=f32)

    def beside(step):
        return {"tp": lax.rem(tp + step + xs, xs)}

    quarter = half // 2

    def send_far(way, h):
        at = h * half + way * quarter
        return pltpu.make_async_remote_copy(
            src_ref=shares.at[2, pl.ds(at, quarter)],
            dst_ref=far_in.at[way, h],
            send_sem=far_send.at[way, h],
            recv_sem=far_recv.at[way, h],
            device_id=beside(1 - 2 * way),
            device_id_type=MESH_ID,
        )

    def send_near(way, h):
        return pltpu.make_async_remote_copy(
            src_ref=shares.at[way, part(h)],
            dst_ref=near_in.at[way, h],
            send_sem=near_send.at[way, h],
            recv_sem=near_recv.at[way, h],
            device_id=beside(1 - 2 * way),
            device_id_type=MESH_ID,
        )

    loads[0].wait()
    for cols, y in projected(lax.rem(tp + 2, xs)):
        shares[2, :, cols] = y.astype(bf16)
    for h in range(2):
        for way in range(2):
            send_far(way, h).start()
    for way in range(2):
        for cols, y in projected(lax.rem(tp + 1 - 2 * way + xs, xs)):
            own_share_sum[:, cols] = y
        for h in range(2):
            send_far(way, h).wait_recv()
            joint = pl.ds(h * half + way * quarter, quarter)
            alone = pl.ds(h * half + (1 - way) * quarter, quarter)
            shares[way, alone] = own_share_sum[alone].astype(bf16)
            joined = own_share_sum[joint] + far_in[way, h].astype(f32)
            shares[way, joint] = joined.astype(bf16)
            send_near(way, h).start()
    for cols, y in projected(tp):
        own_share_sum[:, cols] = y
    loads[1].wait()

    def own_rows(h):
        for way in range(2):
            send_near(way, h).wait_recv()
        got = near_in[0, h].astype(f32) + near_in[1, h].astype(f32)
        x = residual[part(h)].astype(f32) + (own_share_sum[part(h)] + got)
        x = x.astype(bf16)
        stream[part(h)] = x
        x = x.astype(f32)
        scale = lax.rsqrt(jnp.mean(x * x, axis=1, keepdims=True) + norm_eps)
        normed[part(h)] = (x * scale * gain_ref[...]).astype(bf16)

    ids = ids_ref[...]
    expert_at = lax.broadcasted_iota(jnp.int32, (ring * peers, rows), 0)
    token_row = lax.broadcasted_iota(jnp.int32, (rows, rows), 0)
    token_col = lax.broadcasted_iota(jnp.int32, (rows, rows), 1)
    ahead = (token_row < token_col).astype(f32).astype(bf16)
    named = [(expert_at == ids[c : c + 1]).astype(f32) for c in range(2)]
    earlier = jnp.dot((named[0] + named[1]).astype(bf16), ahead, preferred_element_type=f32)
    ranks = [jnp.sum(n * earlier, axis=0, keepdims=True) for n in named]
    group = ids[0:1] // EXPERTS_PER_GROUP
    chip = [ids[c : c + 1] // peers for c in range(2)]
    spot = [lax.rem(c, SPAN) for c in chip]
    blocks = ring // SPAN
    apart = lax.rem(group - block + blocks, blocks)
    top = [(spot[0] == SPAN - 1) | (spot[1] == SPAN - 1), (spot[0] == 0) | (spot[1] == 0)]
    beyond = [(spot[0] > at) | (spot[1] > at), (spot[0] < at) | (spot[1] < at)]
    here = (chip[0] == z) | (chip[1] == z)
    joins = [
        (apart == 0) & beyond[0],
        apart == 1,
        (apart == 0) & beyond[1],
        apart == blocks - 1,
        apart == 2,
        here,
    ]
    joins = [x.astype(f32) for x in joins]
    top = [x.astype(f32) for x in top]
    leads = [top[0], top[0], top[1], top[1], jnp.where(at >= SPAN // 2, top[0], top[1]), top[0]]
    pack_row = lax.broadcasted_iota(jnp.int32, (8, rows), 0)
    lead, rest = jnp.zeros((8, rows), f32), jnp.zeros((8, rows), f32)
    for n in range(6):
        lead = jnp.where(pack_row == n, joins[n] * leads[n], lead)
        rest = jnp.where(pack_row == n, joins[n] * (1.0 - leads[n]), rest)
    lead_rank = jnp.dot(lead.astype(bf16), ahead, preferred_element_type=f32)
    rest_rank = jnp.dot(rest.astype(bf16), ahead, preferred_element_type=f32)
    rest_rank += jnp.sum(lead, axis=1, keepdims=True)
    places[...] = jnp.where(lead > 0, lead_rank, jnp.where(rest > 0, rest_rank, -1.0))
    mix = mix_ref[...]
    mix_high = mix.astype(bf16).astype(f32)
    mix_low = mix - mix_high
    facts_row = lax.broadcasted_iota(jnp.int32, (16, rows), 0)
    facts = jnp.where(facts_row == 8, 1.0, 0.0)
    known = [ids[0:1].astype(f32), ids[1:2].astype(f32), ranks[0], ranks[1]]
    known += [mix_high[0:1], mix_high[1:2], mix_low[0:1], mix_low[1:2]]
    for n in range(8):
        facts = jnp.where(facts_row == n, known[n], facts)
    facts = facts.astype(bf16)
    chunk_row = lax.broadcasted_iota(jnp.int32, (room, rows), 0).astype(f32)

    def packing(n):
        return (chunk_row == places[n : n + 1, :]).astype(f32).astype(bf16)

    def pack(n, way, entry):
        choose = packing(n)
        for c in range(width // tile):
            cols = pl.ds(c * tile, tile)
            got = jnp.dot(choose, normed[:, cols], preferred_element_type=f32)
            pool[way, entry, :, cols] = got.astype(bf16)

    def pack_meta(n, way, entry):
        got = lax.dot_general(
            facts, packing(n), (((1,), (1,)), ((), ())), preferred_element_type=f32
        )
        out_row = lax.broadcasted_iota(jnp.int32, (8, room), 0)
        found = got[8:9] > 0
        out = jnp.where(out_row == 0, jnp.where(found, got[0:1] * CAP + got[2:3], -1.0), 0.0)
        out = jnp.where(out_row == 1, jnp.where(found, got[1:2] * CAP + got[3:4], -1.0), out)
        out = jnp.where(out_row == 2, got[4:5] + got[6:7], out)
        out = jnp.where(out_row == 3, got[5:6] + got[7:8], out)
        pool_meta[way, entry] = jnp.concatenate([out, jnp.zeros_like(out)], axis=1)

    packs = ((4, opposite_way, 2), (1, 0, 1), (3, 1, 1), (0, 0, 0), (2, 1, 0))
    for n, way, kind in packs:
        pack_meta(n, way, FIRST[kind])
    pack_meta(5, 0, HOME)

    own_rows(0)
    own_rows(1)
    for n, way, kind in packs:
        pack(n, way, FIRST[kind])
        if kind == 2:
            for w in range(2):
                forward(w, 2, 0, start_both)
        else:
            forward(way, kind, 0, start_both)
    pack(5, 0, HOME)

    row_id = lax.broadcasted_iota(jnp.int32, (room, room), 0)
    local_code = (row_id // (2 * CAP)) * CAP + lax.rem(row_id, CAP)
    which_half = lax.rem(row_id, 2 * CAP) // CAP
    base = z * (peers * CAP)

    def locate(back):
        other = back > at + SPAN + SPAN // 2
        d = jnp.where(other, ring - back, back)
        end = jnp.where(other, ends[1], ends[0])
        i = lax.rem(end - d + 3 * SPAN, SPAN)
        crossed = (d + i - end) // SPAN
        first = jnp.where(crossed == 0, FIRST[0], jnp.where(crossed == 1, FIRST[1], FIRST[2]))
        entry = jnp.where(back == 0, HOME, first + d)
        return jnp.where(other, 1, 0), entry

    def matches(way, entry, side):
        code = jnp.where(which_half == side, local_code + base, -2).astype(f32)
        m = pool_meta[way, entry][:, 0:room]
        return code == m[0:1, :], code == m[1:2, :], m

    def pick_of(way, entry, side):
        first_hit, second_hit, _ = matches(way, entry, side)
        return (first_hit | second_hit).astype(f32).astype(bf16)

    def weights_of(way, entry, side):
        first_hit, second_hit, m = matches(way, entry, side)
        w = jnp.where(first_hit, m[2:3, :], 0.0) + jnp.where(second_hit, m[3:4, :], 0.0)
        high = w.astype(bf16)
        return high, (w - high.astype(f32)).astype(bf16)

    def exchange(src, dst, sends, recvs, step, offset):
        u, where = peer(offset)
        return pltpu.make_async_remote_copy(
            src_ref=src.at[step, u],
            dst_ref=dst.at[step, mine],
            send_sem=sends.at[step, offset],
            recv_sem=recvs.at[step, offset],
            device_id=where,
            device_id_type=MESH_ID,
        )

    def pick(step):
        a, b = locate(step), locate(ring - 1 - step)
        one_a, one_b = pick_of(*a, 0), pick_of(*b, 1)
        for c in range(width // tile):
            cols = pl.ds(c * tile, tile)
            got = jnp.dot(one_a, pool[a[0], a[1], :, cols], preferred_element_type=f32)
            got += jnp.dot(one_b, pool[b[0], b[1], :, cols], preferred_element_type=f32)
            got = got.astype(bf16).reshape(peers, 2 * CAP, tile)
            picked[step, :, :, cols] = got
        for o in range(1, peers):
            exchange(picked, routed, pick_send, pick_recv, step, o).start()
        routed[step, mine] = picked[step, mine]

    def serve(step):
        for o in range(1, peers):
            exchange(picked, routed, pick_send, pick_recv, step, o).wait_recv()
        x = routed[step].reshape(peers * 2 * CAP, width)
        g = jnp.dot(x, gate_w[...], preferred_element_type=f32)
        u = jnp.dot(x, up_w[...], preferred_element_type=f32)
        hidden = (g * (1.0 / (1.0 + jnp.exp(-g))) * u).astype(bf16)
        for c in range(width // tile):
            cols = pl.ds(c * tile, tile)
            y = jnp.dot(hidden, down_w[:, cols], preferred_element_type=f32)
            made[step, :, :, cols] = y.astype(bf16).reshape(peers, 2 * CAP, tile)
        for o in range(1, peers):
            exchange(made, back, back_send, back_recv, step, o).start()
        back[step, mine] = made[step, mine]

    def ring_step(d, _):
        for kind in (2, 1, 0):
            for way in range(2):
                receive(way, kind, d)
                forward(way, kind, d, start_both)

        @pl.when(d <= far - 2)
        def _():
            pick(d - 1)

        @pl.when((d >= 2) & (d <= far - 1))
        def _():
            serve(d - 2)

        return 0

    for load in loads[2:]:
        load.wait()
    lax.fori_loop(1, LAST[2] + 1, ring_step, 0)
    contract = (((0,), (0,)), ((), ()))

    def wait_back(step):
        for o in range(1, peers):
            exchange(made, back, back_send, back_recv, step, o).wait_recv()

    def own_share(way, entry, behind, dst):
        side = jnp.where(behind >= far, 1, 0)
        step = jnp.where(behind >= far, ring - 1 - behind, behind)
        high, low = weights_of(way, entry, side)
        w = jnp.concatenate([high, low], axis=0)
        for c in range(width // tile):
            cols = pl.ds(c * tile, tile)
            y = back[step, :, :, cols].reshape(room, tile)
            y = jnp.concatenate([y, y], axis=0)
            dst[:, cols] = lax.dot_general(w, y, contract, preferred_element_type=f32)

    def send_sum(way, kind, d, count, home=False):
        entry = FIRST[kind] + d
        return pltpu.make_async_remote_copy(
            src_ref=sums.at[way, entry, pl.ds(0, count)],
            dst_ref=sums.at[way, FIRST[kind] if home else entry - 1, pl.ds(0, count)],
            send_sem=sum_send.at[way, entry],
            recv_sem=sum_recv.at[way, FIRST[kind] if home else entry - 1],
            device_id=chips_on(d if way else -d) if home else onward[1 - way],
            device_id_type=MESH_ID,
        )

    def give_back(way, kind, d, act):
        goes = passes(way, kind, d) & is_mine(way, kind, d)
        end = ends[way]

        @pl.when(goes & (end == SPAN - 1))
        def _():
            act(send_sum(way, kind, d, room // 2))

        @pl.when(goes & (end < SPAN - 1) & (end > 0))
        def _():
            act(send_sum(way, kind, d, room))

        if kind > 0:

            @pl.when(goes & (end == 0))
            def _():
                act(send_sum(way, kind, d, room, home=True))

    first_rows, last_rows = pl.ds(0, room // 2), pl.ds(room // 2, room // 2)

    def sum_entry(way, kind, d):
        entry = FIRST[kind] + d
        goes = passes(way, kind, d) & is_mine(way, kind, d)
        end = ends[way]

        @pl.when(goes & (end < SPAN - 2))
        def _():
            send_sum(way, kind, d + 1, room).wait_recv()
            sums[way, entry] = (sums[way, entry].astype(f32) + own_part[way]).astype(bf16)

        @pl.when(goes & (end == SPAN - 2))
        def _():
            sums[way, entry, last_rows] = own_part[way, last_rows].astype(bf16)
            send_sum(way, kind, d + 1, room // 2).wait_recv()
            got = sums[way, entry, first_rows].astype(f32) + own_part[way, first_rows]
            sums[way, entry, first_rows] = got.astype(bf16)

        @pl.when(goes & (end == SPAN - 1))
        def _():
            sums[way, entry, first_rows] = own_part[way, first_rows].astype(bf16)

        give_back(way, kind, d, lambda copy: copy.start())

    def return_kinds(kinds, d):
        for kind in kinds:
            for way in range(2):

                @pl.when(passes(way, kind, d) & is_mine(way, kind, d))
                def _():
                    behind = d if way == 0 else ring - d
                    own_share(way, FIRST[kind] + d, behind, own_part.at[way])

        for kind in kinds:
            for way in range(2):
                sum_entry(way, kind, d)

    def place(n, value):
        choose = packing(n)
        for c in range(width // tile):
            cols = pl.ds(c * tile, tile)
            got = lax.dot_general(choose, value(cols), contract, preferred_element_type=f32)
            total[:, cols] += got

    def land(n, way, kind):
        whole, first = forwards(way, kind, 0)

        @pl.when(whole)
        def _():
            send_sum(way, kind, 1, room).wait_recv()

        @pl.when(first)
        def _():
            send_sum(way, kind, 1, room // 2).wait_recv()
            sums[way, FIRST[kind], last_rows] = jnp.zeros((room // 2, width), bf16)

        @pl.when(whole | first)
        def _():
            place(n, lambda cols: sums[way, FIRST[kind], :, cols])

    pick(far - 2)
    pick(far - 1)
    wait_back(3)
    wait_back(2)
    return_kinds((0,), 3)
    serve(far - 2)
    wait_back(1)
    return_kinds((0,), 2)
    serve(far - 1)
    wait_back(0)
    return_kinds((0,), 1)
    own_share(0, HOME, 0, own_part.at[0])
    total[...] = stream[...].astype(f32)
    place(5, lambda cols: own_part[0, :, cols].astype(bf16))
    wait_back(far - 1)
    wait_back(far - 2)

    def sum_step(i, _):
        d = LAST[2] - i

        @pl.when((d <= far - 2) & (d >= 5))
        def _():
            wait_back(d - 1)

        return_kinds((1, 2), d)

        @pl.when(d == 4)
        def _():
            land(0, 0, 0)

        @pl.when(d == 3)
        def _():
            land(2, 1, 0)

        return 0

    lax.fori_loop(0, LAST[2], sum_step, 0)
    for n, way, kind in ((1, 0, 1), (3, 1, 1)):
        land(n, way, kind)
    for way in range(2):
        land(4, way, 2)
    out_ref[...] = total[...].astype(bf16)

    def drain(d, _):
        for kind in range(3):
            for way in range(2):
                forward(way, kind, d, wait_sent)

                @pl.when(d >= 1)
                def _():
                    give_back(way, kind, d, lambda copy: copy.wait_send())

        return 0

    lax.fori_loop(0, LAST[2] + 1, drain, 0)

    def drain_steps(n, _):
        for o in range(1, peers):
            exchange(picked, routed, pick_send, pick_recv, n, o).wait_send()
            exchange(made, back, back_send, back_recv, n, o).wait_send()
        return 0

    lax.fori_loop(0, far, drain_steps, 0)
    halo.wait_send()
    for h in range(2):
        for way in range(2):
            send_far(way, h).wait_send()
            send_near(way, h).wait_send()


def layer(query, key, value, cosines, sines, sinks, gain, ids, mix, residual, proj, gate, up, down):
    rows, width = residual.shape
    ring = lax.axis_size("sp") // CORES
    xs = lax.axis_size("tp")
    far = ring // 2
    peers = xs * CORES
    hidden = gate.shape[1]
    room = 2 * peers * CAP
    tile = min(512, width)
    bf16, f32 = jnp.bfloat16, jnp.float32
    vmem = pl.BlockSpec(memory_space=pltpu.VMEM)
    smem = pl.BlockSpec(memory_space=pltpu.SMEM)
    hbm = pl.BlockSpec(memory_space=pl.ANY)
    slab = (far, peers, 2 * CAP, width)
    dma = pltpu.SemaphoreType.DMA
    return pl.pallas_call(
        functools.partial(expert_kernel, ring, xs, tile),
        out_shape=jax.ShapeDtypeStruct((rows, width), bf16),
        in_specs=[vmem] * 5 + [smem] + [vmem] * 3 + [hbm] * 5,
        out_specs=vmem,
        scratch_shapes=[
            pltpu.VMEM(query.shape, bf16),
            pltpu.VMEM((2 * HDIM, query.shape[0] + WINDOW), bf16),
            pltpu.VMEM((rows, width), bf16),
            pltpu.VMEM(proj.shape, bf16),
            pltpu.VMEM((3, rows, width), bf16),
            pltpu.VMEM((2, 2, rows // 4, width), bf16),
            pltpu.VMEM((2, 2, rows // 2, width), bf16),
            pltpu.VMEM((rows, width), f32),
            pltpu.VMEM((rows, width), bf16),
            pltpu.VMEM((rows, width), bf16),
            pltpu.VMEM((8, rows), f32),
            pltpu.VMEM((2, ENTRIES, room, width), bf16),
            pltpu.VMEM((rows, width), f32),
            pltpu.VMEM((2, ENTRIES + 1, room, width), bf16),
            pltpu.VMEM((2, ENTRIES + 1, 8, rows), f32),
            pltpu.VMEM(slab, bf16),
            pltpu.VMEM(slab, bf16),
            pltpu.VMEM(slab, bf16),
            pltpu.VMEM(slab, bf16),
            pltpu.VMEM((2, room, width), f32),
            pltpu.VMEM((width, hidden), bf16),
            pltpu.VMEM((width, hidden), bf16),
            pltpu.VMEM((hidden, width), bf16),
            dma((5,)),
            dma((2, ENTRIES)),
            dma((2, ENTRIES)),
            dma((2, ENTRIES)),
            dma((2, ENTRIES)),
            dma((far, peers)),
            dma((far, peers)),
            dma((far, peers)),
            dma((far, peers)),
            dma((2, ENTRIES)),
            dma((2, ENTRIES)),
            dma,
            dma,
            dma((2, 2)),
            dma((2, 2)),
            dma((2, 2)),
            dma((2, 2)),
        ],
        compiler_params=pltpu.CompilerParams(
            collective_id=1, has_side_effects=True, vmem_limit_bytes=60 * 1024 * 1024
        ),
    )(query, key, value, cosines, sines, sinks, gain, ids, mix, residual, proj, gate, up, down)


def per_device(
    query_rows,
    key_rows,
    value_rows,
    sink_logits,
    residual,
    out_weight,
    norm_gain,
    gate_weight,
    up_weight,
    down_weight,
    routes,
    route_weight,
):
    tok_count = query_rows.shape[0]
    positions = lax.axis_index("sp") * tok_count + jnp.arange(tok_count, dtype=jnp.int32)
    half_dim = HDIM // 2
    inverse = rope_base ** (-jnp.arange(half_dim, dtype=jnp.float32) / half_dim)
    angles = positions.astype(jnp.float32)[None, :] * inverse[:, None]
    cosines = jnp.cos(angles)
    sines = jnp.sin(angles)
    return layer(
        query_rows,
        key_rows.T,
        value_rows.T,
        cosines,
        sines,
        sink_logits,
        norm_gain[None, :],
        routes.T,
        route_weight.T,
        residual,
        out_weight,
        gate_weight[0],
        up_weight[0],
        down_weight[0],
    )


def solution(mesh):
    in_specs = (
        P(("grp", "sp"), "tp"),
        P(("grp", "sp"), "tp"),
        P(("grp", "sp"), "tp"),
        P("tp"),
        P(("grp", "sp", "tp"), None),
        P("tp", None),
        P(),
        P(("sp", "tp"), None, None),
        P(("sp", "tp"), None, None),
        P(("sp", "tp"), None, None),
        P(("grp", "sp", "tp"), None),
        P(("grp", "sp", "tp"), None),
    )
    out_specs = P(("grp", "sp", "tp"), None)
    return jax.shard_map(
        per_device, mesh=mesh, in_specs=in_specs, out_specs=out_specs, check_vma=False
    )
```

```python
import functools

import jax
import jax.numpy as jnp
from jax import lax
from jax.experimental import pallas as pl
from jax.experimental.pallas import tpu as pltpu
from jax.sharding import PartitionSpec as P

MESH_ID = pl.DeviceIdType.MESH
HDIM = 64
WINDOW = 128
CAP = 4
CORES = 2
EXPERTS_PER_GROUP = 32
SPAN = 4
FIRST = (0, 4, 12)
LAST = (3, 7, 9)
ENTRIES = 22
HOME = 22


rope_base = 10000.0
norm_eps = 1e-06


def expert_kernel(
    ring,
    xs,
    tile,
    query_ref,
    key_ref,
    value_ref,
    cos_ref,
    sin_ref,
    sink_ref,
    gain_ref,
    ids_ref,
    mix_ref,
    residual_hbm,
    proj_hbm,
    gate_hbm,
    up_hbm,
    down_hbm,
    out_ref,
    rot_q,
    keys_values,
    residual,
    proj_w,
    shares,
    far_in,
    near_in,
    own_share_sum,
    stream,
    normed,
    places,
    sums,
    total,
    pool,
    pool_meta,
    picked,
    routed,
    made,
    back,
    own_part,
    gate_w,
    up_w,
    down_w,
    weight_sem,
    pool_send,
    pool_recv,
    meta_send,
    meta_recv,
    pick_send,
    pick_recv,
    back_send,
    back_recv,
    sum_send,
    sum_recv,
    halo_send,
    halo_recv,
    far_send,
    far_recv,
    near_send,
    near_recv,
):
    f32, bf16 = jnp.float32, jnp.bfloat16
    rows, width = residual.shape
    half = rows // 2
    far = ring // 2
    peers = xs * CORES
    sp, tp = lax.axis_index("sp"), lax.axis_index("tp")
    core = lax.rem(sp, CORES)
    z = sp // CORES
    mine = core * xs + tp
    nxt = {"sp": lax.rem(sp + CORES, ring * CORES)}
    prv = {"sp": lax.rem(sp + (ring - 1) * CORES, ring * CORES)}

    def peer(offset):
        u = lax.rem(mine + offset, peers)
        return u, {"sp": z * CORES + u // xs, "tp": lax.rem(u, xs)}

    loads = [
        pltpu.make_async_copy(src, dst, weight_sem.at[i])
        for i, (src, dst) in enumerate(
            (
                (proj_hbm, proj_w),
                (residual_hbm, residual),
                (gate_hbm, gate_w),
                (up_hbm, up_w),
                (down_hbm, down_w),
            )
        )
    ]
    for load in loads:
        load.start()

    barrier = pltpu.get_barrier_semaphore()
    pl.semaphore_signal(barrier, inc=1, device_id=nxt, device_id_type=MESH_ID)
    pl.semaphore_signal(barrier, inc=1, device_id=prv, device_id_type=MESH_ID)
    total_sp = ring * CORES
    after = {"sp": lax.rem(sp + 1, total_sp)}
    across = {"sp": lax.rem(sp + jnp.where(core == 1, 1, total_sp - 1), total_sp)}
    pl.semaphore_signal(barrier, inc=1, device_id=across, device_id_type=MESH_ID)
    for o in range(1, peers):
        pl.semaphore_signal(barrier, inc=1, device_id=peer(o)[1], device_id_type=MESH_ID)

    lane = lax.broadcasted_iota(jnp.int32, (query_ref.shape[1],) * 2, 1)
    line = lax.broadcasted_iota(jnp.int32, (query_ref.shape[1],) * 2, 0)
    low = lax.rem(lane, HDIM) < HDIM // 2
    turn = jnp.where(low & (line == lane + HDIM // 2), -1.0, 0.0)
    turn = (turn + jnp.where((~low) & (line == lane - HDIM // 2), 1.0, 0.0)).astype(bf16)

    def rotated(x, cosines, sines):
        n = x.shape[1]
        swapped = jnp.dot(x, turn[:n, :n], preferred_element_type=f32)
        return (x.astype(f32) * cosines + swapped * sines).astype(bf16)

    tok = query_ref.shape[0]
    k_low = key_ref[0 : HDIM // 2].astype(f32)
    k_high = key_ref[HDIM // 2 :].astype(f32)
    turned_low = k_low * cos_ref[...] - k_high * sin_ref[...]
    turned_high = k_high * cos_ref[...] + k_low * sin_ref[...]
    turned_k = jnp.concatenate([turned_low, turned_high], axis=0)
    keys_values[0:HDIM, WINDOW:] = turned_k.astype(bf16)
    keys_values[HDIM:, WINDOW:] = value_ref[...]
    pl.semaphore_wait(barrier, peers + 2)
    halo = pltpu.make_async_remote_copy(
        src_ref=keys_values.at[:, pl.ds(tok, WINDOW)],
        dst_ref=keys_values.at[:, pl.ds(0, WINDOW)],
        send_sem=halo_send,
        recv_sem=halo_recv,
        device_id=after,
        device_id_type=MESH_ID,
    )
    halo.start()
    repeats = 128 // (HDIM // 2)
    cosines = jnp.concatenate([cos_ref[...]] * repeats, axis=0).T
    sines = jnp.concatenate([sin_ref[...]] * repeats, axis=0).T
    for c in range(query_ref.shape[1] // 128):
        cols = pl.ds(c * 128, 128)
        rot_q[:, cols] = rotated(query_ref[:, cols], cosines, sines)
    halo.wait_recv()

    def part(h):
        return pl.ds(h * half, half)

    block, at = z // SPAN, lax.rem(z, SPAN)
    opposite_way = jnp.where(at >= SPAN // 2, 0, 1)
    ends = (at, SPAN - 1 - at)
    onward = (nxt, prv)
    room = 2 * peers * CAP

    def origin(way, d):
        i = lax.rem(ends[way] - d + 3 * SPAN, SPAN)
        return i, (d + i - ends[way]) // SPAN

    def passes(way, kind, d):
        i, crossed = origin(way, d)
        there = (d <= LAST[kind]) & (kind >= crossed)
        return there & (i >= SPAN // 2) if kind == 2 else there

    def is_mine(way, kind, d):
        return origin(way, d)[1] == kind

    def send_chunk(way, kind, d, count):
        entry = FIRST[kind] + d
        return pltpu.make_async_remote_copy(
            src_ref=pool.at[way, entry, pl.ds(0, count)],
            dst_ref=pool.at[way, entry + 1, pl.ds(0, count)],
            send_sem=pool_send.at[way, entry],
            recv_sem=pool_recv.at[way, entry + 1],
            device_id=onward[way],
            device_id_type=MESH_ID,
        )

    def send_meta(way, kind, d):
        entry = FIRST[kind] + d
        return pltpu.make_async_remote_copy(
            src_ref=pool_meta.at[way, entry],
            dst_ref=pool_meta.at[way, entry + 1],
            send_sem=meta_send.at[way, entry],
            recv_sem=meta_recv.at[way, entry + 1],
            device_id=onward[way],
            device_id_type=MESH_ID,
        )

    def forwards(way, kind, d):
        goes = passes(way, kind, d)
        mine_here = is_mine(way, kind, d)
        whole = goes & jnp.where(mine_here, ends[way] < SPAN - 2, True)
        return whole, goes & mine_here & (ends[way] == SPAN - 2)

    def forward(way, kind, d, act):
        whole, first = forwards(way, kind, d)

        @pl.when(whole)
        def _():
            act(send_chunk(way, kind, d, room), send_meta(way, kind, d))

        @pl.when(first)
        def _():
            act(send_chunk(way, kind, d, room // 2), send_meta(way, kind, d))

    def start_both(chunk, about):
        about.start()
        chunk.start()

    def wait_sent(chunk, about):
        about.wait_send()
        chunk.wait_send()

    def receive(way, kind, d):
        goes = passes(way, kind, d)
        short = is_mine(way, kind, d) & (ends[way] == SPAN - 1)

        @pl.when(goes)
        def _():
            send_meta(way, kind, d - 1).wait_recv()

        @pl.when(goes & ~short)
        def _():
            send_chunk(way, kind, d - 1, room).wait_recv()

        @pl.when(goes & short)
        def _():
            send_chunk(way, kind, d - 1, room // 2).wait_recv()
            pool[way, FIRST[kind] + d, pl.ds(room // 2, room // 2)] = jnp.zeros(
                (room // 2, width), bf16
            )

    q_at = lax.broadcasted_iota(jnp.int32, (WINDOW, 2 * WINDOW), 0)
    k_at = lax.broadcasted_iota(jnp.int32, (WINDOW, 2 * WINDOW), 1)
    reach = q_at + WINDOW - k_at

    def projected(block):
        start = pl.multiple_of(block * WINDOW, WINDOW)
        first = start + sp * tok
        allowed = (reach >= 0) & (reach < WINDOW) & (k_at + first >= WINDOW)
        k = keys_values[0:HDIM, pl.ds(start, 2 * WINDOW)]
        v = keys_values[HDIM:, pl.ds(start, 2 * WINDOW)]
        q = rot_q[pl.ds(start, WINDOW), :]
        heads = []
        for h in range(q.shape[1] // HDIM):
            qh = q[:, h * HDIM : (h + 1) * HDIM]
            s = jnp.dot(qh, k, preferred_element_type=f32)
            s = jnp.where(allowed, s * HDIM ** (-0.5), -jnp.inf)
            sink = sink_ref[h]
            top = jnp.maximum(jnp.max(s, axis=1, keepdims=True), sink)
            e = jnp.exp(s - top)
            below = jnp.sum(e, axis=1, keepdims=True) + jnp.exp(sink - top)
            p = (e / below).astype(bf16)
            seen = lax.dot_general(p, v, (((1,), (1,)), ((), ())), preferred_element_type=f32)
            heads.append(seen.astype(bf16))
        att = jnp.concatenate(heads, axis=1)
        for c in range(width // tile):
            cols = pl.ds(c * tile, tile)
            yield cols, jnp.dot(att, proj_w[:, cols], preferred_element_type=f32)

    def beside(step):
        return {"tp": lax.rem(tp + step + xs, xs)}

    quarter = half // 2

    def send_far(way, h):
        at = h * half + way * quarter
        return pltpu.make_async_remote_copy(
            src_ref=shares.at[2, pl.ds(at, quarter)],
            dst_ref=far_in.at[way, h],
            send_sem=far_send.at[way, h],
            recv_sem=far_recv.at[way, h],
            device_id=beside(1 - 2 * way),
            device_id_type=MESH_ID,
        )

    def send_near(way, h):
        return pltpu.make_async_remote_copy(
            src_ref=shares.at[way, part(h)],
            dst_ref=near_in.at[way, h],
            send_sem=near_send.at[way, h],
            recv_sem=near_recv.at[way, h],
            device_id=beside(1 - 2 * way),
            device_id_type=MESH_ID,
        )

    loads[0].wait()
    for cols, y in projected(lax.rem(tp + 2, xs)):
        shares[2, :, cols] = y.astype(bf16)
    for h in range(2):
        for way in range(2):
            send_far(way, h).start()
    for way in range(2):
        for cols, y in projected(lax.rem(tp + 1 - 2 * way + xs, xs)):
            own_share_sum[:, cols] = y
        for h in range(2):
            send_far(way, h).wait_recv()
            joint = pl.ds(h * half + way * quarter, quarter)
            alone = pl.ds(h * half + (1 - way) * quarter, quarter)
            shares[way, alone] = own_share_sum[alone].astype(bf16)
            joined = own_share_sum[joint] + far_in[way, h].astype(f32)
            shares[way, joint] = joined.astype(bf16)
            send_near(way, h).start()
    for cols, y in projected(tp):
        own_share_sum[:, cols] = y
    loads[1].wait()

    def own_rows(h):
        for way in range(2):
            send_near(way, h).wait_recv()
        got = near_in[0, h].astype(f32) + near_in[1, h].astype(f32)
        x = residual[part(h)].astype(f32) + (own_share_sum[part(h)] + got)
        x = x.astype(bf16)
        stream[part(h)] = x
        x = x.astype(f32)
        scale = lax.rsqrt(jnp.mean(x * x, axis=1, keepdims=True) + norm_eps)
        normed[part(h)] = (x * scale * gain_ref[...]).astype(bf16)

    ids = ids_ref[...]
    expert_at = lax.broadcasted_iota(jnp.int32, (ring * peers, rows), 0)
    token_row = lax.broadcasted_iota(jnp.int32, (rows, rows), 0)
    token_col = lax.broadcasted_iota(jnp.int32, (rows, rows), 1)
    ahead = (token_row < token_col).astype(f32).astype(bf16)
    named = [(expert_at == ids[c : c + 1]).astype(f32) for c in range(2)]
    earlier = jnp.dot((named[0] + named[1]).astype(bf16), ahead, preferred_element_type=f32)
    ranks = [jnp.sum(n * earlier, axis=0, keepdims=True) for n in named]
    group = ids[0:1] // EXPERTS_PER_GROUP
    chip = [ids[c : c + 1] // peers for c in range(2)]
    spot = [lax.rem(c, SPAN) for c in chip]
    blocks = ring // SPAN
    apart = lax.rem(group - block + blocks, blocks)
    top = [(spot[0] == SPAN - 1) | (spot[1] == SPAN - 1), (spot[0] == 0) | (spot[1] == 0)]
    beyond = [(spot[0] > at) | (spot[1] > at), (spot[0] < at) | (spot[1] < at)]
    here = (chip[0] == z) | (chip[1] == z)
    joins = [
        (apart == 0) & beyond[0],
        apart == 1,
        (apart == 0) & beyond[1],
        apart == blocks - 1,
        apart == 2,
        here,
    ]
    joins = [x.astype(f32) for x in joins]
    top = [x.astype(f32) for x in top]
    leads = [top[0], top[0], top[1], top[1], jnp.where(at >= SPAN // 2, top[0], top[1]), top[0]]
    pack_row = lax.broadcasted_iota(jnp.int32, (8, rows), 0)
    lead, rest = jnp.zeros((8, rows), f32), jnp.zeros((8, rows), f32)
    for n in range(6):
        lead = jnp.where(pack_row == n, joins[n] * leads[n], lead)
        rest = jnp.where(pack_row == n, joins[n] * (1.0 - leads[n]), rest)
    lead_rank = jnp.dot(lead.astype(bf16), ahead, preferred_element_type=f32)
    rest_rank = jnp.dot(rest.astype(bf16), ahead, preferred_element_type=f32)
    rest_rank += jnp.sum(lead, axis=1, keepdims=True)
    places[...] = jnp.where(lead > 0, lead_rank, jnp.where(rest > 0, rest_rank, -1.0))
    mix = mix_ref[...]
    mix_high = mix.astype(bf16).astype(f32)
    mix_low = mix - mix_high
    facts_row = lax.broadcasted_iota(jnp.int32, (16, rows), 0)
    facts = jnp.where(facts_row == 8, 1.0, 0.0)
    known = [ids[0:1].astype(f32), ids[1:2].astype(f32), ranks[0], ranks[1]]
    known += [mix_high[0:1], mix_high[1:2], mix_low[0:1], mix_low[1:2]]
    for n in range(8):
        facts = jnp.where(facts_row == n, known[n], facts)
    facts = facts.astype(bf16)
    chunk_row = lax.broadcasted_iota(jnp.int32, (room, rows), 0).astype(f32)

    def packing(n):
        return (chunk_row == places[n : n + 1, :]).astype(f32).astype(bf16)

    def pack(n, way, entry):
        choose = packing(n)
        for c in range(width // tile):
            cols = pl.ds(c * tile, tile)
            got = jnp.dot(choose, normed[:, cols], preferred_element_type=f32)
            pool[way, entry, :, cols] = got.astype(bf16)

    def pack_meta(n, way, entry):
        got = lax.dot_general(
            facts, packing(n), (((1,), (1,)), ((), ())), preferred_element_type=f32
        )
        out_row = lax.broadcasted_iota(jnp.int32, (8, room), 0)
        found = got[8:9] > 0
        out = jnp.where(out_row == 0, jnp.where(found, got[0:1] * CAP + got[2:3], -1.0), 0.0)
        out = jnp.where(out_row == 1, jnp.where(found, got[1:2] * CAP + got[3:4], -1.0), out)
        out = jnp.where(out_row == 2, got[4:5] + got[6:7], out)
        out = jnp.where(out_row == 3, got[5:6] + got[7:8], out)
        pool_meta[way, entry] = jnp.concatenate([out, jnp.zeros_like(out)], axis=1)

    packs = ((4, opposite_way, 2), (1, 0, 1), (3, 1, 1), (0, 0, 0), (2, 1, 0))
    for n, way, kind in packs:
        pack_meta(n, way, FIRST[kind])
    pack_meta(5, 0, HOME)

    own_rows(0)
    own_rows(1)
    for n, way, kind in packs:
        pack(n, way, FIRST[kind])
        if kind == 2:
            for w in range(2):
                forward(w, 2, 0, start_both)
        else:
            forward(way, kind, 0, start_both)
    pack(5, 0, HOME)

    row_id = lax.broadcasted_iota(jnp.int32, (room, room), 0)
    local_code = (row_id // (2 * CAP)) * CAP + lax.rem(row_id, CAP)
    which_half = lax.rem(row_id, 2 * CAP) // CAP
    base = z * (peers * CAP)

    def paired(back):
        late = (at == SPAN - 1) & ((back == far - 1) | (back == far + 1))
        return jnp.where(late, ring - back, back)

    def locate(back):
        other = back > at + SPAN + SPAN // 2
        d = jnp.where(other, ring - back, back)
        end = jnp.where(other, ends[1], ends[0])
        i = lax.rem(end - d + 3 * SPAN, SPAN)
        crossed = (d + i - end) // SPAN
        first = jnp.where(crossed == 0, FIRST[0], jnp.where(crossed == 1, FIRST[1], FIRST[2]))
        entry = jnp.where(back == 0, HOME, first + d)
        return jnp.where(other, 1, 0), entry

    def matches(way, entry, side):
        code = jnp.where(which_half == side, local_code + base, -2).astype(f32)
        m = pool_meta[way, entry][:, 0:room]
        return code == m[0:1, :], code == m[1:2, :], m

    def pick_of(way, entry, side):
        first_hit, second_hit, _ = matches(way, entry, side)
        return (first_hit | second_hit).astype(f32).astype(bf16)

    def weights_of(way, entry, side):
        first_hit, second_hit, m = matches(way, entry, side)
        w = jnp.where(first_hit, m[2:3, :], 0.0) + jnp.where(second_hit, m[3:4, :], 0.0)
        high = w.astype(bf16)
        return high, (w - high.astype(f32)).astype(bf16)

    def exchange(src, dst, sends, recvs, step, offset):
        u, where = peer(offset)
        return pltpu.make_async_remote_copy(
            src_ref=src.at[step, u],
            dst_ref=dst.at[step, mine],
            send_sem=sends.at[step, offset],
            recv_sem=recvs.at[step, offset],
            device_id=where,
            device_id_type=MESH_ID,
        )

    def pick(step):
        a, b = locate(paired(step)), locate(paired(ring - 1 - step))
        one_a, one_b = pick_of(*a, 0), pick_of(*b, 1)
        for c in range(width // tile):
            cols = pl.ds(c * tile, tile)
            got = jnp.dot(one_a, pool[a[0], a[1], :, cols], preferred_element_type=f32)
            got += jnp.dot(one_b, pool[b[0], b[1], :, cols], preferred_element_type=f32)
            got = got.astype(bf16).reshape(peers, 2 * CAP, tile)
            picked[step, :, :, cols] = got
        for o in range(1, peers):
            exchange(picked, routed, pick_send, pick_recv, step, o).start()
        routed[step, mine] = picked[step, mine]

    def serve(step):
        for o in range(1, peers):
            exchange(picked, routed, pick_send, pick_recv, step, o).wait_recv()
        x = routed[step].reshape(peers * 2 * CAP, width)
        g = jnp.dot(x, gate_w[...], preferred_element_type=f32)
        u = jnp.dot(x, up_w[...], preferred_element_type=f32)
        hidden = (g * (1.0 / (1.0 + jnp.exp(-g))) * u).astype(bf16)
        for c in range(width // tile):
            cols = pl.ds(c * tile, tile)
            y = jnp.dot(hidden, down_w[:, cols], preferred_element_type=f32)
            made[step, :, :, cols] = y.astype(bf16).reshape(peers, 2 * CAP, tile)
        for o in range(1, peers):
            exchange(made, back, back_send, back_recv, step, o).start()
        back[step, mine] = made[step, mine]

    def ring_step(d, _):
        for kind in (2, 1, 0):
            for way in range(2):
                receive(way, kind, d)
                forward(way, kind, d, start_both)

        @pl.when(d <= far - 1)
        def _():
            pick(d - 1)

        @pl.when((d >= 2) & (d <= far))
        def _():
            serve(d - 2)

        return 0

    for load in loads[2:]:
        load.wait()
    lax.fori_loop(1, LAST[2] + 1, ring_step, 0)
    contract = (((0,), (0,)), ((), ()))

    def wait_back(step):
        for o in range(1, peers):
            exchange(made, back, back_send, back_recv, step, o).wait_recv()

    def own_share(way, entry, behind, dst):
        place_of = paired(behind)
        side = jnp.where(place_of >= far, 1, 0)
        step = jnp.where(place_of >= far, ring - 1 - place_of, place_of)
        high, low = weights_of(way, entry, side)
        w = jnp.concatenate([high, low], axis=0)
        for c in range(width // tile):
            cols = pl.ds(c * tile, tile)
            y = back[step, :, :, cols].reshape(room, tile)
            y = jnp.concatenate([y, y], axis=0)
            dst[:, cols] = lax.dot_general(w, y, contract, preferred_element_type=f32)

    def lines(h):
        return pl.ds(h * (room // 2), room // 2)

    def send_sum(way, kind, d, h):
        entry = FIRST[kind] + d
        return pltpu.make_async_remote_copy(
            src_ref=sums.at[way, entry, lines(h)],
            dst_ref=sums.at[way, entry - 1, lines(h)],
            send_sem=sum_send.at[way, entry, h],
            recv_sem=sum_recv.at[way, entry - 1, h],
            device_id=onward[1 - way],
            device_id_type=MESH_ID,
        )

    def gives(way, kind, d, h):
        goes = passes(way, kind, d)
        return goes if h == 0 else goes & ~(is_mine(way, kind, d) & (ends[way] == SPAN - 1))

    def give_back(way, kind, d, act):
        for h in range(2):

            @pl.when(gives(way, kind, d, h))
            def _():
                act(send_sum(way, kind, d, h))

    def sum_entry(way, kind, d, h):
        entry = FIRST[kind] + d
        goes = passes(way, kind, d)
        mine_here = is_mine(way, kind, d)
        comes = ends[way] < SPAN - 1 - h

        @pl.when(goes & (comes | ~mine_here))
        def _():
            send_sum(way, kind, d + 1, h).wait_recv()

        @pl.when(goes & comes & mine_here)
        def _():
            got = sums[way, entry, lines(h)].astype(f32) + own_part[way, lines(h)]
            sums[way, entry, lines(h)] = got.astype(bf16)

        @pl.when(goes & ~comes & mine_here)
        def _():
            sums[way, entry, lines(h)] = own_part[way, lines(h)].astype(bf16)

        @pl.when(gives(way, kind, d, h))
        def _():
            send_sum(way, kind, d, h).start()

    def return_kind(kind, d):
        for way in range(2):

            @pl.when(passes(way, kind, d) & is_mine(way, kind, d))
            def _():
                behind = d if way == 0 else ring - d
                own_share(way, FIRST[kind] + d, behind, own_part.at[way])

        for h in (1, 0):
            for way in range(2):
                sum_entry(way, kind, d, h)

    def place(n, value):
        choose = packing(n)
        for c in range(width // tile):
            cols = pl.ds(c * tile, tile)
            got = lax.dot_general(choose, value(cols), contract, preferred_element_type=f32)
            total[:, cols] += got

    def land(n, way, kind):
        whole, first = forwards(way, kind, 0)

        @pl.when(whole | first)
        def _():
            send_sum(way, kind, 1, 0).wait_recv()

        @pl.when(whole)
        def _():
            send_sum(way, kind, 1, 1).wait_recv()

        @pl.when(first)
        def _():
            sums[way, FIRST[kind], lines(1)] = jnp.zeros((room // 2, width), bf16)

        @pl.when(whole | first)
        def _():
            place(n, lambda cols: sums[way, FIRST[kind], :, cols])

    pick(far - 1)
    wait_back(0)
    own_share(0, HOME, 0, own_part.at[0])
    total[...] = stream[...].astype(f32)
    place(5, lambda cols: own_part[0, :, cols].astype(bf16))
    serve(far - 1)
    wait_back(far - 2)
    wait_back(far - 1)

    def sum_step(i, _):
        r = LAST[2] - 1 - i

        @pl.when((r <= far - 2) & (r >= 2))
        def _():
            wait_back(r - 1)

        @pl.when(r >= 1)
        def _():
            return_kind(1, r)

        return_kind(2, r + 1)

        @pl.when(r >= 1)
        def _():
            return_kind(0, r)

        return 0

    lax.fori_loop(0, LAST[2], sum_step, 0)
    for n, way, kind in ((1, 0, 1), (3, 1, 1), (0, 0, 0), (2, 1, 0), (4, 0, 2), (4, 1, 2)):
        land(n, way, kind)
    out_ref[...] = total[...].astype(bf16)

    def drain(d, _):
        for kind in range(3):
            for way in range(2):
                forward(way, kind, d, wait_sent)

                @pl.when(d >= 1)
                def _():
                    give_back(way, kind, d, lambda copy: copy.wait_send())

        return 0

    lax.fori_loop(0, LAST[2] + 1, drain, 0)

    def drain_steps(n, _):
        for o in range(1, peers):
            exchange(picked, routed, pick_send, pick_recv, n, o).wait_send()
            exchange(made, back, back_send, back_recv, n, o).wait_send()
        return 0

    lax.fori_loop(0, far, drain_steps, 0)
    halo.wait_send()
    for h in range(2):
        for way in range(2):
            send_far(way, h).wait_send()
            send_near(way, h).wait_send()


def layer(query, key, value, cosines, sines, sinks, gain, ids, mix, residual, proj, gate, up, down):
    rows, width = residual.shape
    ring = lax.axis_size("sp") // CORES
    xs = lax.axis_size("tp")
    far = ring // 2
    peers = xs * CORES
    hidden = gate.shape[1]
    room = 2 * peers * CAP
    tile = min(512, width)
    bf16, f32 = jnp.bfloat16, jnp.float32
    vmem = pl.BlockSpec(memory_space=pltpu.VMEM)
    smem = pl.BlockSpec(memory_space=pltpu.SMEM)
    hbm = pl.BlockSpec(memory_space=pl.ANY)
    slab = (far, peers, 2 * CAP, width)
    dma = pltpu.SemaphoreType.DMA
    return pl.pallas_call(
        functools.partial(expert_kernel, ring, xs, tile),
        out_shape=jax.ShapeDtypeStruct((rows, width), bf16),
        in_specs=[vmem] * 5 + [smem] + [vmem] * 3 + [hbm] * 5,
        out_specs=vmem,
        scratch_shapes=[
            pltpu.VMEM(query.shape, bf16),
            pltpu.VMEM((2 * HDIM, query.shape[0] + WINDOW), bf16),
            pltpu.VMEM((rows, width), bf16),
            pltpu.VMEM(proj.shape, bf16),
            pltpu.VMEM((3, rows, width), bf16),
            pltpu.VMEM((2, 2, rows // 4, width), bf16),
            pltpu.VMEM((2, 2, rows // 2, width), bf16),
            pltpu.VMEM((rows, width), f32),
            pltpu.VMEM((rows, width), bf16),
            pltpu.VMEM((rows, width), bf16),
            pltpu.VMEM((8, rows), f32),
            pltpu.VMEM((2, ENTRIES, room, width), bf16),
            pltpu.VMEM((rows, width), f32),
            pltpu.VMEM((2, ENTRIES + 1, room, width), bf16),
            pltpu.VMEM((2, ENTRIES + 1, 8, rows), f32),
            pltpu.VMEM(slab, bf16),
            pltpu.VMEM(slab, bf16),
            pltpu.VMEM(slab, bf16),
            pltpu.VMEM(slab, bf16),
            pltpu.VMEM((2, room, width), f32),
            pltpu.VMEM((width, hidden), bf16),
            pltpu.VMEM((width, hidden), bf16),
            pltpu.VMEM((hidden, width), bf16),
            dma((5,)),
            dma((2, ENTRIES)),
            dma((2, ENTRIES)),
            dma((2, ENTRIES)),
            dma((2, ENTRIES)),
            dma((far, peers)),
            dma((far, peers)),
            dma((far, peers)),
            dma((far, peers)),
            dma((2, ENTRIES, 2)),
            dma((2, ENTRIES, 2)),
            dma,
            dma,
            dma((2, 2)),
            dma((2, 2)),
            dma((2, 2)),
            dma((2, 2)),
        ],
        compiler_params=pltpu.CompilerParams(
            collective_id=1, has_side_effects=True, vmem_limit_bytes=60 * 1024 * 1024
        ),
    )(query, key, value, cosines, sines, sinks, gain, ids, mix, residual, proj, gate, up, down)


def per_device(
    query_rows,
    key_rows,
    value_rows,
    sink_logits,
    residual,
    out_weight,
    norm_gain,
    gate_weight,
    up_weight,
    down_weight,
    routes,
    route_weight,
):
    tok_count = query_rows.shape[0]
    positions = lax.axis_index("sp") * tok_count + jnp.arange(tok_count, dtype=jnp.int32)
    half_dim = HDIM // 2
    inverse = rope_base ** (-jnp.arange(half_dim, dtype=jnp.float32) / half_dim)
    angles = positions.astype(jnp.float32)[None, :] * inverse[:, None]
    cosines = jnp.cos(angles)
    sines = jnp.sin(angles)
    return layer(
        query_rows,
        key_rows.T,
        value_rows.T,
        cosines,
        sines,
        sink_logits,
        norm_gain[None, :],
        routes.T,
        route_weight.T,
        residual,
        out_weight,
        gate_weight[0],
        up_weight[0],
        down_weight[0],
    )


def solution(mesh):
    in_specs = (
        P(("grp", "sp"), "tp"),
        P(("grp", "sp"), "tp"),
        P(("grp", "sp"), "tp"),
        P("tp"),
        P(("grp", "sp", "tp"), None),
        P("tp", None),
        P(),
        P(("sp", "tp"), None, None),
        P(("sp", "tp"), None, None),
        P(("sp", "tp"), None, None),
        P(("grp", "sp", "tp"), None),
        P(("grp", "sp", "tp"), None),
    )
    out_specs = P(("grp", "sp", "tp"), None)
    return jax.shard_map(
        per_device, mesh=mesh, in_specs=in_specs, out_specs=out_specs, check_vma=False
    )
```

```python
import functools

import jax
import jax.numpy as jnp
from jax import lax
from jax.experimental import pallas as pl
from jax.experimental.pallas import tpu as pltpu
from jax.sharding import PartitionSpec as P

MESH_ID = pl.DeviceIdType.MESH
HDIM = 64
WINDOW = 128
CAP = 4
CORES = 2
EXPERTS_PER_GROUP = 32
SPAN = 4
FIRST = (0, 4, 12)
LAST = (3, 7, 9)
ENTRIES = 22
HOME = 22


rope_base = 10000.0
norm_eps = 1e-06


def expert_kernel(
    ring,
    xs,
    tile,
    query_ref,
    key_ref,
    value_ref,
    cos_ref,
    sin_ref,
    sink_ref,
    gain_ref,
    ids_ref,
    mix_ref,
    residual_hbm,
    proj_hbm,
    gate_hbm,
    up_hbm,
    down_hbm,
    out_ref,
    rot_q,
    keys_values,
    residual,
    proj_w,
    shares,
    far_in,
    near_in,
    own_share_sum,
    stream,
    normed,
    places,
    sums,
    total,
    pool,
    pool_meta,
    picked,
    routed,
    made,
    back,
    own_part,
    gate_w,
    up_w,
    down_w,
    weight_sem,
    pool_send,
    pool_recv,
    meta_send,
    meta_recv,
    pick_send,
    pick_recv,
    back_send,
    back_recv,
    sum_send,
    sum_recv,
    halo_send,
    halo_recv,
    far_send,
    far_recv,
    near_send,
    near_recv,
):
    f32, bf16 = jnp.float32, jnp.bfloat16
    rows, width = residual.shape
    half = rows // 2
    far = ring // 2
    peers = xs * CORES
    sp, tp = lax.axis_index("sp"), lax.axis_index("tp")
    core = lax.rem(sp, CORES)
    z = sp // CORES
    mine = core * xs + tp
    nxt = {"sp": lax.rem(sp + CORES, ring * CORES)}
    prv = {"sp": lax.rem(sp + (ring - 1) * CORES, ring * CORES)}

    def peer(offset):
        u = lax.rem(mine + offset, peers)
        return u, {"sp": z * CORES + u // xs, "tp": lax.rem(u, xs)}

    loads = [
        pltpu.make_async_copy(src, dst, weight_sem.at[i])
        for i, (src, dst) in enumerate(
            (
                (proj_hbm, proj_w),
                (residual_hbm, residual),
                (gate_hbm, gate_w),
                (up_hbm, up_w),
                (down_hbm, down_w),
            )
        )
    ]
    for load in loads:
        load.start()

    barrier = pltpu.get_barrier_semaphore()
    pl.semaphore_signal(barrier, inc=1, device_id=nxt, device_id_type=MESH_ID)
    pl.semaphore_signal(barrier, inc=1, device_id=prv, device_id_type=MESH_ID)
    total_sp = ring * CORES
    after = {"sp": lax.rem(sp + 1, total_sp)}
    across = {"sp": lax.rem(sp + jnp.where(core == 1, 1, total_sp - 1), total_sp)}
    pl.semaphore_signal(barrier, inc=1, device_id=across, device_id_type=MESH_ID)
    for o in range(1, peers):
        pl.semaphore_signal(barrier, inc=1, device_id=peer(o)[1], device_id_type=MESH_ID)

    lane = lax.broadcasted_iota(jnp.int32, (query_ref.shape[1],) * 2, 1)
    line = lax.broadcasted_iota(jnp.int32, (query_ref.shape[1],) * 2, 0)
    low = lax.rem(lane, HDIM) < HDIM // 2
    turn = jnp.where(low & (line == lane + HDIM // 2), -1.0, 0.0)
    turn = (turn + jnp.where((~low) & (line == lane - HDIM // 2), 1.0, 0.0)).astype(bf16)

    def rotated(x, cosines, sines):
        n = x.shape[1]
        swapped = jnp.dot(x, turn[:n, :n], preferred_element_type=f32)
        return (x.astype(f32) * cosines + swapped * sines).astype(bf16)

    tok = query_ref.shape[0]
    k_low = key_ref[0 : HDIM // 2].astype(f32)
    k_high = key_ref[HDIM // 2 :].astype(f32)
    turned_low = k_low * cos_ref[...] - k_high * sin_ref[...]
    turned_high = k_high * cos_ref[...] + k_low * sin_ref[...]
    turned_k = jnp.concatenate([turned_low, turned_high], axis=0)
    keys_values[0:HDIM, WINDOW:] = turned_k.astype(bf16)
    keys_values[HDIM:, WINDOW:] = value_ref[...]
    pl.semaphore_wait(barrier, peers + 2)
    halo = pltpu.make_async_remote_copy(
        src_ref=keys_values.at[:, pl.ds(tok, WINDOW)],
        dst_ref=keys_values.at[:, pl.ds(0, WINDOW)],
        send_sem=halo_send,
        recv_sem=halo_recv,
        device_id=after,
        device_id_type=MESH_ID,
    )
    halo.start()
    repeats = 128 // (HDIM // 2)
    cosines = jnp.concatenate([cos_ref[...]] * repeats, axis=0).T
    sines = jnp.concatenate([sin_ref[...]] * repeats, axis=0).T
    for c in range(query_ref.shape[1] // 128):
        cols = pl.ds(c * 128, 128)
        rot_q[:, cols] = rotated(query_ref[:, cols], cosines, sines)
    halo.wait_recv()

    def part(h):
        return pl.ds(h * half, half)

    block, at = z // SPAN, lax.rem(z, SPAN)
    opposite_way = jnp.where(at >= SPAN // 2, 0, 1)
    ends = (at, SPAN - 1 - at)
    onward = (nxt, prv)
    room = 2 * peers * CAP

    def origin(way, d):
        i = lax.rem(ends[way] - d + 3 * SPAN, SPAN)
        return i, (d + i - ends[way]) // SPAN

    def passes(way, kind, d):
        i, crossed = origin(way, d)
        there = (d <= LAST[kind]) & (kind >= crossed)
        return there & (i >= SPAN // 2) if kind == 2 else there

    def is_mine(way, kind, d):
        return origin(way, d)[1] == kind

    def send_chunk(way, kind, d, count):
        entry = FIRST[kind] + d
        return pltpu.make_async_remote_copy(
            src_ref=pool.at[way, entry, pl.ds(0, count)],
            dst_ref=pool.at[way, entry + 1, pl.ds(0, count)],
            send_sem=pool_send.at[way, entry],
            recv_sem=pool_recv.at[way, entry + 1],
            device_id=onward[way],
            device_id_type=MESH_ID,
        )

    def send_meta(way, kind, d):
        entry = FIRST[kind] + d
        return pltpu.make_async_remote_copy(
            src_ref=pool_meta.at[way, entry],
            dst_ref=pool_meta.at[way, entry + 1],
            send_sem=meta_send.at[way, entry],
            recv_sem=meta_recv.at[way, entry + 1],
            device_id=onward[way],
            device_id_type=MESH_ID,
        )

    def forwards(way, kind, d):
        goes = passes(way, kind, d)
        mine_here = is_mine(way, kind, d)
        whole = goes & jnp.where(mine_here, ends[way] < SPAN - 2, True)
        return whole, goes & mine_here & (ends[way] == SPAN - 2)

    def forward(way, kind, d, act):
        whole, first = forwards(way, kind, d)

        @pl.when(whole)
        def _():
            act(send_chunk(way, kind, d, room), send_meta(way, kind, d))

        @pl.when(first)
        def _():
            act(send_chunk(way, kind, d, room // 2), send_meta(way, kind, d))

    def start_both(chunk, about):
        about.start()
        chunk.start()

    def wait_sent(chunk, about):
        about.wait_send()
        chunk.wait_send()

    def receive(way, kind, d):
        goes = passes(way, kind, d)
        short = is_mine(way, kind, d) & (ends[way] == SPAN - 1)

        @pl.when(goes)
        def _():
            send_meta(way, kind, d - 1).wait_recv()

        @pl.when(goes & ~short)
        def _():
            send_chunk(way, kind, d - 1, room).wait_recv()

        @pl.when(goes & short)
        def _():
            send_chunk(way, kind, d - 1, room // 2).wait_recv()
            pool[way, FIRST[kind] + d, pl.ds(room // 2, room // 2)] = jnp.zeros(
                (room // 2, width), bf16
            )

    q_at = lax.broadcasted_iota(jnp.int32, (WINDOW, 2 * WINDOW), 0)
    k_at = lax.broadcasted_iota(jnp.int32, (WINDOW, 2 * WINDOW), 1)
    reach = q_at + WINDOW - k_at

    def projected(block):
        start = pl.multiple_of(block * WINDOW, WINDOW)
        first = start + sp * tok
        allowed = (reach >= 0) & (reach < WINDOW) & (k_at + first >= WINDOW)
        k = keys_values[0:HDIM, pl.ds(start, 2 * WINDOW)]
        v = keys_values[HDIM:, pl.ds(start, 2 * WINDOW)]
        q = rot_q[pl.ds(start, WINDOW), :]
        heads = []
        for h in range(q.shape[1] // HDIM):
            qh = q[:, h * HDIM : (h + 1) * HDIM]
            s = jnp.dot(qh, k, preferred_element_type=f32)
            s = jnp.where(allowed, s * HDIM ** (-0.5), -jnp.inf)
            sink = sink_ref[h]
            top = jnp.maximum(jnp.max(s, axis=1, keepdims=True), sink)
            e = jnp.exp(s - top)
            below = jnp.sum(e, axis=1, keepdims=True) + jnp.exp(sink - top)
            p = (e / below).astype(bf16)
            seen = lax.dot_general(p, v, (((1,), (1,)), ((), ())), preferred_element_type=f32)
            heads.append(seen.astype(bf16))
        att = jnp.concatenate(heads, axis=1)
        for c in range(width // tile):
            cols = pl.ds(c * tile, tile)
            yield cols, jnp.dot(att, proj_w[:, cols], preferred_element_type=f32)

    def beside(step):
        return {"tp": lax.rem(tp + step + xs, xs)}

    quarter = half // 2

    def send_far(way, h):
        at = h * half + way * quarter
        return pltpu.make_async_remote_copy(
            src_ref=shares.at[2, pl.ds(at, quarter)],
            dst_ref=far_in.at[way, h],
            send_sem=far_send.at[way, h],
            recv_sem=far_recv.at[way, h],
            device_id=beside(1 - 2 * way),
            device_id_type=MESH_ID,
        )

    def send_near(way, h):
        return pltpu.make_async_remote_copy(
            src_ref=shares.at[way, part(h)],
            dst_ref=near_in.at[way, h],
            send_sem=near_send.at[way, h],
            recv_sem=near_recv.at[way, h],
            device_id=beside(1 - 2 * way),
            device_id_type=MESH_ID,
        )

    loads[0].wait()
    for cols, y in projected(lax.rem(tp + 2, xs)):
        shares[2, :, cols] = y.astype(bf16)
    for h in range(2):
        for way in range(2):
            send_far(way, h).start()
    for way in range(2):
        for cols, y in projected(lax.rem(tp + 1 - 2 * way + xs, xs)):
            own_share_sum[:, cols] = y
        for h in range(2):
            send_far(way, h).wait_recv()
            joint = pl.ds(h * half + way * quarter, quarter)
            alone = pl.ds(h * half + (1 - way) * quarter, quarter)
            shares[way, alone] = own_share_sum[alone].astype(bf16)
            joined = own_share_sum[joint] + far_in[way, h].astype(f32)
            shares[way, joint] = joined.astype(bf16)
            send_near(way, h).start()
    for cols, y in projected(tp):
        own_share_sum[:, cols] = y
    loads[1].wait()

    def own_rows(h):
        for way in range(2):
            send_near(way, h).wait_recv()
        got = near_in[0, h].astype(f32) + near_in[1, h].astype(f32)
        x = residual[part(h)].astype(f32) + (own_share_sum[part(h)] + got)
        x = x.astype(bf16)
        stream[part(h)] = x
        x = x.astype(f32)
        scale = lax.rsqrt(jnp.mean(x * x, axis=1, keepdims=True) + norm_eps)
        normed[part(h)] = (x * scale * gain_ref[...]).astype(bf16)

    ids = ids_ref[...]
    expert_at = lax.broadcasted_iota(jnp.int32, (ring * peers, rows), 0)
    token_row = lax.broadcasted_iota(jnp.int32, (rows, rows), 0)
    token_col = lax.broadcasted_iota(jnp.int32, (rows, rows), 1)
    ahead = (token_row < token_col).astype(f32).astype(bf16)
    named = [(expert_at == ids[c : c + 1]).astype(f32) for c in range(2)]
    earlier = jnp.dot((named[0] + named[1]).astype(bf16), ahead, preferred_element_type=f32)
    ranks = [jnp.sum(n * earlier, axis=0, keepdims=True) for n in named]
    group = ids[0:1] // EXPERTS_PER_GROUP
    chip = [ids[c : c + 1] // peers for c in range(2)]
    spot = [lax.rem(c, SPAN) for c in chip]
    blocks = ring // SPAN
    apart = lax.rem(group - block + blocks, blocks)
    top = [(spot[0] == SPAN - 1) | (spot[1] == SPAN - 1), (spot[0] == 0) | (spot[1] == 0)]
    beyond = [(spot[0] > at) | (spot[1] > at), (spot[0] < at) | (spot[1] < at)]
    here = (chip[0] == z) | (chip[1] == z)
    joins = [
        (apart == 0) & beyond[0],
        apart == 1,
        (apart == 0) & beyond[1],
        apart == blocks - 1,
        apart == 2,
        here,
    ]
    joins = [x.astype(f32) for x in joins]
    top = [x.astype(f32) for x in top]
    leads = [top[0], top[0], top[1], top[1], jnp.where(at >= SPAN // 2, top[0], top[1]), top[0]]
    pack_row = lax.broadcasted_iota(jnp.int32, (8, rows), 0)
    lead, rest = jnp.zeros((8, rows), f32), jnp.zeros((8, rows), f32)
    for n in range(6):
        lead = jnp.where(pack_row == n, joins[n] * leads[n], lead)
        rest = jnp.where(pack_row == n, joins[n] * (1.0 - leads[n]), rest)
    lead_rank = jnp.dot(lead.astype(bf16), ahead, preferred_element_type=f32)
    rest_rank = jnp.dot(rest.astype(bf16), ahead, preferred_element_type=f32)
    rest_rank += jnp.sum(lead, axis=1, keepdims=True)
    places[...] = jnp.where(lead > 0, lead_rank, jnp.where(rest > 0, rest_rank, -1.0))
    mix = mix_ref[...]
    mix_high = mix.astype(bf16).astype(f32)
    mix_low = mix - mix_high
    facts_row = lax.broadcasted_iota(jnp.int32, (16, rows), 0)
    facts = jnp.where(facts_row == 8, 1.0, 0.0)
    known = [ids[0:1].astype(f32), ids[1:2].astype(f32), ranks[0], ranks[1]]
    known += [mix_high[0:1], mix_high[1:2], mix_low[0:1], mix_low[1:2]]
    for n in range(8):
        facts = jnp.where(facts_row == n, known[n], facts)
    facts = facts.astype(bf16)
    chunk_row = lax.broadcasted_iota(jnp.int32, (room, rows), 0).astype(f32)

    def packing(n):
        return (chunk_row == places[n : n + 1, :]).astype(f32).astype(bf16)

    def pack(n, way, entry):
        choose = packing(n)
        for c in range(width // tile):
            cols = pl.ds(c * tile, tile)
            got = jnp.dot(choose, normed[:, cols], preferred_element_type=f32)
            pool[way, entry, :, cols] = got.astype(bf16)

    def pack_meta(n, way, entry):
        got = lax.dot_general(
            facts, packing(n), (((1,), (1,)), ((), ())), preferred_element_type=f32
        )
        out_row = lax.broadcasted_iota(jnp.int32, (8, room), 0)
        found = got[8:9] > 0
        out = jnp.where(out_row == 0, jnp.where(found, got[0:1] * CAP + got[2:3], -1.0), 0.0)
        out = jnp.where(out_row == 1, jnp.where(found, got[1:2] * CAP + got[3:4], -1.0), out)
        out = jnp.where(out_row == 2, got[4:5] + got[6:7], out)
        out = jnp.where(out_row == 3, got[5:6] + got[7:8], out)
        pool_meta[way, entry] = jnp.concatenate([out, jnp.zeros_like(out)], axis=1)

    packs = ((4, opposite_way, 2), (1, 0, 1), (3, 1, 1), (0, 0, 0), (2, 1, 0))
    for n, way, kind in packs:
        pack_meta(n, way, FIRST[kind])
    pack_meta(5, 0, HOME)

    own_rows(0)
    own_rows(1)
    for n, way, kind in packs:
        pack(n, way, FIRST[kind])
        if kind == 2:
            for w in range(2):
                forward(w, 2, 0, start_both)
        else:
            forward(way, kind, 0, start_both)
    pack(5, 0, HOME)

    row_id = lax.broadcasted_iota(jnp.int32, (room, room), 0)
    local_code = (row_id // (2 * CAP)) * CAP + lax.rem(row_id, CAP)
    which_half = lax.rem(row_id, 2 * CAP) // CAP
    base = z * (peers * CAP)

    def paired(back):
        late = (at == SPAN - 1) & ((back == far - 1) | (back == far + 1))
        return jnp.where(late, ring - back, back)

    def locate(back):
        other = back > at + SPAN + SPAN // 2
        d = jnp.where(other, ring - back, back)
        end = jnp.where(other, ends[1], ends[0])
        i = lax.rem(end - d + 3 * SPAN, SPAN)
        crossed = (d + i - end) // SPAN
        first = jnp.where(crossed == 0, FIRST[0], jnp.where(crossed == 1, FIRST[1], FIRST[2]))
        entry = jnp.where(back == 0, HOME, first + d)
        return jnp.where(other, 1, 0), entry

    def matches(way, entry, side):
        code = jnp.where(which_half == side, local_code + base, -2).astype(f32)
        m = pool_meta[way, entry][:, 0:room]
        return code == m[0:1, :], code == m[1:2, :], m

    def pick_of(way, entry, side):
        first_hit, second_hit, _ = matches(way, entry, side)
        return (first_hit | second_hit).astype(f32).astype(bf16)

    def weights_of(way, entry, side):
        first_hit, second_hit, m = matches(way, entry, side)
        w = jnp.where(first_hit, m[2:3, :], 0.0) + jnp.where(second_hit, m[3:4, :], 0.0)
        high = w.astype(bf16)
        return high, (w - high.astype(f32)).astype(bf16)

    def exchange(src, dst, sends, recvs, step, offset):
        u, where = peer(offset)
        return pltpu.make_async_remote_copy(
            src_ref=src.at[step, u],
            dst_ref=dst.at[step, mine],
            send_sem=sends.at[step, offset],
            recv_sem=recvs.at[step, offset],
            device_id=where,
            device_id_type=MESH_ID,
        )

    def pick(step):
        a, b = locate(paired(step)), locate(paired(ring - 1 - step))
        one_a, one_b = pick_of(*a, 0), pick_of(*b, 1)
        for c in range(width // tile):
            cols = pl.ds(c * tile, tile)
            got = jnp.dot(one_a, pool[a[0], a[1], :, cols], preferred_element_type=f32)
            got += jnp.dot(one_b, pool[b[0], b[1], :, cols], preferred_element_type=f32)
            got = got.astype(bf16).reshape(peers, 2 * CAP, tile)
            picked[step, :, :, cols] = got
        for o in range(1, peers):
            exchange(picked, routed, pick_send, pick_recv, step, o).start()
        routed[step, mine] = picked[step, mine]

    def serve(step):
        for o in range(1, peers):
            exchange(picked, routed, pick_send, pick_recv, step, o).wait_recv()
        x = routed[step].reshape(peers * 2 * CAP, width)
        g = jnp.dot(x, gate_w[...], preferred_element_type=f32)
        u = jnp.dot(x, up_w[...], preferred_element_type=f32)
        hidden = (g * (1.0 / (1.0 + jnp.exp(-g))) * u).astype(bf16)
        for c in range(width // tile):
            cols = pl.ds(c * tile, tile)
            y = jnp.dot(hidden, down_w[:, cols], preferred_element_type=f32)
            made[step, :, :, cols] = y.astype(bf16).reshape(peers, 2 * CAP, tile)
        for o in range(1, peers):
            exchange(made, back, back_send, back_recv, step, o).start()
        back[step, mine] = made[step, mine]

    def ring_step(d, _):
        for kind in (2, 1, 0):
            for way in range(2):
                receive(way, kind, d)
                forward(way, kind, d, start_both)

        @pl.when(d <= far - 1)
        def _():
            pick(d - 1)

        @pl.when((d >= 2) & (d <= far))
        def _():
            serve(d - 2)

        return 0

    for load in loads[2:]:
        load.wait()
    lax.fori_loop(1, LAST[2] + 1, ring_step, 0)
    contract = (((0,), (0,)), ((), ()))

    def wait_back(step):
        for o in range(1, peers):
            exchange(made, back, back_send, back_recv, step, o).wait_recv()

    def own_share(way, entry, behind, dst):
        place_of = paired(behind)
        side = jnp.where(place_of >= far, 1, 0)
        step = jnp.where(place_of >= far, ring - 1 - place_of, place_of)
        high, low = weights_of(way, entry, side)
        w = jnp.concatenate([high, low], axis=0)
        for c in range(width // tile):
            cols = pl.ds(c * tile, tile)
            y = back[step, :, :, cols].reshape(room, tile)
            y = jnp.concatenate([y, y], axis=0)
            dst[:, cols] = lax.dot_general(w, y, contract, preferred_element_type=f32)

    def lines(h):
        return pl.ds(h * (room // 2), room // 2)

    def send_sum(way, kind, d, h):
        entry = FIRST[kind] + d
        return pltpu.make_async_remote_copy(
            src_ref=sums.at[way, entry, lines(h)],
            dst_ref=sums.at[way, entry - 1, lines(h)],
            send_sem=sum_send.at[way, entry, h],
            recv_sem=sum_recv.at[way, entry - 1, h],
            device_id=onward[1 - way],
            device_id_type=MESH_ID,
        )

    def gives(way, kind, d, h):
        goes = passes(way, kind, d)
        return goes if h == 0 else goes & ~(is_mine(way, kind, d) & (ends[way] == SPAN - 1))

    def give_back(way, kind, d, act):
        for h in range(2):

            @pl.when(gives(way, kind, d, h))
            def _():
                act(send_sum(way, kind, d, h))

    def sum_entry(way, kind, d, h):
        entry = FIRST[kind] + d
        goes = passes(way, kind, d)
        mine_here = is_mine(way, kind, d)
        comes = ends[way] < SPAN - 1 - h

        @pl.when(goes & (comes | ~mine_here))
        def _():
            send_sum(way, kind, d + 1, h).wait_recv()

        @pl.when(goes & comes & mine_here)
        def _():
            got = sums[way, entry, lines(h)].astype(f32) + own_part[way, lines(h)]
            sums[way, entry, lines(h)] = got.astype(bf16)

        @pl.when(goes & ~comes & mine_here)
        def _():
            sums[way, entry, lines(h)] = own_part[way, lines(h)].astype(bf16)

        @pl.when(gives(way, kind, d, h))
        def _():
            send_sum(way, kind, d, h).start()

    def return_kind(kind, d):
        for way in range(2):

            @pl.when(passes(way, kind, d) & is_mine(way, kind, d))
            def _():
                behind = d if way == 0 else ring - d
                own_share(way, FIRST[kind] + d, behind, own_part.at[way])

        for h in (1, 0):
            for way in range(2):
                sum_entry(way, kind, d, h)

    def place(n, value):
        choose = packing(n)
        for c in range(width // tile):
            cols = pl.ds(c * tile, tile)
            got = lax.dot_general(choose, value(cols), contract, preferred_element_type=f32)
            total[:, cols] += got

    def land(n, way, kind):
        whole, first = forwards(way, kind, 0)

        @pl.when(whole | first)
        def _():
            send_sum(way, kind, 1, 0).wait_recv()

        @pl.when(whole)
        def _():
            send_sum(way, kind, 1, 1).wait_recv()

        @pl.when(first)
        def _():
            sums[way, FIRST[kind], lines(1)] = jnp.zeros((room // 2, width), bf16)

        @pl.when(whole | first)
        def _():
            place(n, lambda cols: sums[way, FIRST[kind], :, cols])

    pick(far - 1)
    wait_back(0)
    own_share(0, HOME, 0, own_part.at[0])
    total[...] = stream[...].astype(f32)
    place(5, lambda cols: own_part[0, :, cols].astype(bf16))
    wait_back(far - 2)
    return_kind(1, LAST[1])
    serve(far - 1)

    def sum_step(i, _):
        r = far - i

        @pl.when((r >= 4) & (r <= far))
        def _():
            wait_back(r - 3)

        @pl.when(r == jnp.where((at == 0) | (at == SPAN - 1), far, far - 1))
        def _():
            wait_back(far - 1)

        return_kind(2, r + 1)

        @pl.when((r >= 1) & (r <= LAST[0]))
        def _():
            return_kind(0, r)

        @pl.when(r >= 3)
        def _():
            return_kind(1, r - 2)

        return 0

    lax.fori_loop(0, far + 1, sum_step, 0)
    for n, way, kind in ((1, 0, 1), (3, 1, 1), (0, 0, 0), (2, 1, 0), (4, 0, 2), (4, 1, 2)):
        land(n, way, kind)
    out_ref[...] = total[...].astype(bf16)

    def drain(d, _):
        for kind in range(3):
            for way in range(2):
                forward(way, kind, d, wait_sent)

                @pl.when(d >= 1)
                def _():
                    give_back(way, kind, d, lambda copy: copy.wait_send())

        return 0

    lax.fori_loop(0, LAST[2] + 1, drain, 0)

    def drain_steps(n, _):
        for o in range(1, peers):
            exchange(picked, routed, pick_send, pick_recv, n, o).wait_send()
            exchange(made, back, back_send, back_recv, n, o).wait_send()
        return 0

    lax.fori_loop(0, far, drain_steps, 0)
    halo.wait_send()
    for h in range(2):
        for way in range(2):
            send_far(way, h).wait_send()
            send_near(way, h).wait_send()


def layer(query, key, value, cosines, sines, sinks, gain, ids, mix, residual, proj, gate, up, down):
    rows, width = residual.shape
    ring = lax.axis_size("sp") // CORES
    xs = lax.axis_size("tp")
    far = ring // 2
    peers = xs * CORES
    hidden = gate.shape[1]
    room = 2 * peers * CAP
    tile = min(512, width)
    bf16, f32 = jnp.bfloat16, jnp.float32
    vmem = pl.BlockSpec(memory_space=pltpu.VMEM)
    smem = pl.BlockSpec(memory_space=pltpu.SMEM)
    hbm = pl.BlockSpec(memory_space=pl.ANY)
    slab = (far, peers, 2 * CAP, width)
    dma = pltpu.SemaphoreType.DMA
    return pl.pallas_call(
        functools.partial(expert_kernel, ring, xs, tile),
        out_shape=jax.ShapeDtypeStruct((rows, width), bf16),
        in_specs=[vmem] * 5 + [smem] + [vmem] * 3 + [hbm] * 5,
        out_specs=vmem,
        scratch_shapes=[
            pltpu.VMEM(query.shape, bf16),
            pltpu.VMEM((2 * HDIM, query.shape[0] + WINDOW), bf16),
            pltpu.VMEM((rows, width), bf16),
            pltpu.VMEM(proj.shape, bf16),
            pltpu.VMEM((3, rows, width), bf16),
            pltpu.VMEM((2, 2, rows // 4, width), bf16),
            pltpu.VMEM((2, 2, rows // 2, width), bf16),
            pltpu.VMEM((rows, width), f32),
            pltpu.VMEM((rows, width), bf16),
            pltpu.VMEM((rows, width), bf16),
            pltpu.VMEM((8, rows), f32),
            pltpu.VMEM((2, ENTRIES, room, width), bf16),
            pltpu.VMEM((rows, width), f32),
            pltpu.VMEM((2, ENTRIES + 1, room, width), bf16),
            pltpu.VMEM((2, ENTRIES + 1, 8, rows), f32),
            pltpu.VMEM(slab, bf16),
            pltpu.VMEM(slab, bf16),
            pltpu.VMEM(slab, bf16),
            pltpu.VMEM(slab, bf16),
            pltpu.VMEM((2, room, width), f32),
            pltpu.VMEM((width, hidden), bf16),
            pltpu.VMEM((width, hidden), bf16),
            pltpu.VMEM((hidden, width), bf16),
            dma((5,)),
            dma((2, ENTRIES)),
            dma((2, ENTRIES)),
            dma((2, ENTRIES)),
            dma((2, ENTRIES)),
            dma((far, peers)),
            dma((far, peers)),
            dma((far, peers)),
            dma((far, peers)),
            dma((2, ENTRIES, 2)),
            dma((2, ENTRIES, 2)),
            dma,
            dma,
            dma((2, 2)),
            dma((2, 2)),
            dma((2, 2)),
            dma((2, 2)),
        ],
        compiler_params=pltpu.CompilerParams(
            collective_id=1, has_side_effects=True, vmem_limit_bytes=60 * 1024 * 1024
        ),
    )(query, key, value, cosines, sines, sinks, gain, ids, mix, residual, proj, gate, up, down)


def per_device(
    query_rows,
    key_rows,
    value_rows,
    sink_logits,
    residual,
    out_weight,
    norm_gain,
    gate_weight,
    up_weight,
    down_weight,
    routes,
    route_weight,
):
    tok_count = query_rows.shape[0]
    positions = lax.axis_index("sp") * tok_count + jnp.arange(tok_count, dtype=jnp.int32)
    half_dim = HDIM // 2
    inverse = rope_base ** (-jnp.arange(half_dim, dtype=jnp.float32) / half_dim)
    angles = positions.astype(jnp.float32)[None, :] * inverse[:, None]
    cosines = jnp.cos(angles)
    sines = jnp.sin(angles)
    return layer(
        query_rows,
        key_rows.T,
        value_rows.T,
        cosines,
        sines,
        sink_logits,
        norm_gain[None, :],
        routes.T,
        route_weight.T,
        residual,
        out_weight,
        gate_weight[0],
        up_weight[0],
        down_weight[0],
    )


def solution(mesh):
    in_specs = (
        P(("grp", "sp"), "tp"),
        P(("grp", "sp"), "tp"),
        P(("grp", "sp"), "tp"),
        P("tp"),
        P(("grp", "sp", "tp"), None),
        P("tp", None),
        P(),
        P(("sp", "tp"), None, None),
        P(("sp", "tp"), None, None),
        P(("sp", "tp"), None, None),
        P(("grp", "sp", "tp"), None),
        P(("grp", "sp", "tp"), None),
    )
    out_specs = P(("grp", "sp", "tp"), None)
    return jax.shard_map(
        per_device, mesh=mesh, in_specs=in_specs, out_specs=out_specs, check_vma=False
    )
```

```python
import functools

import jax
import jax.numpy as jnp
from jax import lax
from jax.experimental import pallas as pl
from jax.experimental.pallas import tpu as pltpu
from jax.sharding import PartitionSpec as P

MESH_ID = pl.DeviceIdType.MESH
HDIM = 64
WINDOW = 128
CAP = 4
CORES = 2
EXPERTS_PER_GROUP = 32
SPAN = 4
FIRST = (0, 4, 12)
LAST = (3, 7, 9)
ENTRIES = 22
HOME = 22


rope_base = 10000.0
norm_eps = 1e-06


def expert_kernel(
    ring,
    xs,
    tile,
    query_ref,
    key_ref,
    value_ref,
    cos_ref,
    sin_ref,
    sink_ref,
    gain_ref,
    ids_ref,
    mix_ref,
    residual_hbm,
    proj_hbm,
    gate_hbm,
    up_hbm,
    down_hbm,
    out_ref,
    rot_q,
    keys_values,
    residual,
    proj_w,
    shares,
    far_in,
    near_in,
    own_share_sum,
    stream,
    unscaled,
    places,
    sums,
    total,
    pool,
    pool_meta,
    picked,
    routed,
    made,
    back,
    own_part,
    gate_w,
    up_w,
    down_w,
    weight_sem,
    pool_send,
    pool_recv,
    meta_send,
    meta_recv,
    pick_send,
    pick_recv,
    back_send,
    back_recv,
    sum_send,
    sum_recv,
    halo_send,
    halo_recv,
    far_send,
    far_recv,
    near_send,
    near_recv,
):
    f32, bf16 = jnp.float32, jnp.bfloat16
    rows, width = residual.shape
    half = rows // 2
    far = ring // 2
    peers = xs * CORES
    sp, tp = lax.axis_index("sp"), lax.axis_index("tp")
    core = lax.rem(sp, CORES)
    z = sp // CORES
    mine = core * xs + tp
    nxt = {"sp": lax.rem(sp + CORES, ring * CORES)}
    prv = {"sp": lax.rem(sp + (ring - 1) * CORES, ring * CORES)}

    def peer(offset):
        u = lax.rem(mine + offset, peers)
        return u, {"sp": z * CORES + u // xs, "tp": lax.rem(u, xs)}

    loads = [
        pltpu.make_async_copy(src, dst, weight_sem.at[i])
        for i, (src, dst) in enumerate(
            (
                (proj_hbm, proj_w),
                (residual_hbm, residual),
                (gate_hbm, gate_w),
                (up_hbm, up_w),
                (down_hbm, down_w),
            )
        )
    ]
    for load in loads:
        load.start()

    barrier = pltpu.get_barrier_semaphore()
    pl.semaphore_signal(barrier, inc=1, device_id=nxt, device_id_type=MESH_ID)
    pl.semaphore_signal(barrier, inc=1, device_id=prv, device_id_type=MESH_ID)
    total_sp = ring * CORES
    after = {"sp": lax.rem(sp + 1, total_sp)}
    across = {"sp": lax.rem(sp + jnp.where(core == 1, 1, total_sp - 1), total_sp)}
    pl.semaphore_signal(barrier, inc=1, device_id=across, device_id_type=MESH_ID)
    for o in range(1, peers):
        pl.semaphore_signal(barrier, inc=1, device_id=peer(o)[1], device_id_type=MESH_ID)

    lane = lax.broadcasted_iota(jnp.int32, (query_ref.shape[1],) * 2, 1)
    line = lax.broadcasted_iota(jnp.int32, (query_ref.shape[1],) * 2, 0)
    low = lax.rem(lane, HDIM) < HDIM // 2
    turn = jnp.where(low & (line == lane + HDIM // 2), -1.0, 0.0)
    turn = (turn + jnp.where((~low) & (line == lane - HDIM // 2), 1.0, 0.0)).astype(bf16)

    def rotated(x, cosines, sines):
        n = x.shape[1]
        swapped = jnp.dot(x, turn[:n, :n], preferred_element_type=f32)
        return (x.astype(f32) * cosines + swapped * sines).astype(bf16)

    tok = query_ref.shape[0]
    k_low = key_ref[0 : HDIM // 2].astype(f32)
    k_high = key_ref[HDIM // 2 :].astype(f32)
    turned_low = k_low * cos_ref[...] - k_high * sin_ref[...]
    turned_high = k_high * cos_ref[...] + k_low * sin_ref[...]
    turned_k = jnp.concatenate([turned_low, turned_high], axis=0)
    keys_values[0:HDIM, WINDOW:] = turned_k.astype(bf16)
    keys_values[HDIM:, WINDOW:] = value_ref[...]
    pl.semaphore_wait(barrier, peers + 2)
    halo = pltpu.make_async_remote_copy(
        src_ref=keys_values.at[:, pl.ds(tok, WINDOW)],
        dst_ref=keys_values.at[:, pl.ds(0, WINDOW)],
        send_sem=halo_send,
        recv_sem=halo_recv,
        device_id=after,
        device_id_type=MESH_ID,
    )
    halo.start()
    repeats = 128 // (HDIM // 2)
    cosines = jnp.concatenate([cos_ref[...]] * repeats, axis=0).T
    sines = jnp.concatenate([sin_ref[...]] * repeats, axis=0).T
    for c in range(query_ref.shape[1] // 128):
        cols = pl.ds(c * 128, 128)
        rot_q[:, cols] = rotated(query_ref[:, cols], cosines, sines)
    halo.wait_recv()

    def part(h):
        return pl.ds(h * half, half)

    def side_cols(h):
        return pl.ds(h * (width // 2), width // 2)

    block, at = z // SPAN, lax.rem(z, SPAN)
    opposite_way = jnp.where(at >= SPAN // 2, 0, 1)
    ends = (at, SPAN - 1 - at)
    onward = (nxt, prv)
    room = 2 * peers * CAP

    def origin(way, d):
        i = lax.rem(ends[way] - d + 3 * SPAN, SPAN)
        return i, (d + i - ends[way]) // SPAN

    def passes(way, kind, d):
        i, crossed = origin(way, d)
        there = (d <= LAST[kind]) & (kind >= crossed)
        return there & (i >= SPAN // 2) if kind == 2 else there

    def is_mine(way, kind, d):
        return origin(way, d)[1] == kind

    def send_chunk(way, kind, d, count, h):
        entry = FIRST[kind] + d
        return pltpu.make_async_remote_copy(
            src_ref=pool.at[way, entry, pl.ds(0, count), side_cols(h)],
            dst_ref=pool.at[way, entry + 1, pl.ds(0, count), side_cols(h)],
            send_sem=pool_send.at[way, entry, h],
            recv_sem=pool_recv.at[way, entry + 1, h],
            device_id=onward[way],
            device_id_type=MESH_ID,
        )

    def send_meta(way, kind, d):
        entry = FIRST[kind] + d
        return pltpu.make_async_remote_copy(
            src_ref=pool_meta.at[way, entry],
            dst_ref=pool_meta.at[way, entry + 1],
            send_sem=meta_send.at[way, entry],
            recv_sem=meta_recv.at[way, entry + 1],
            device_id=onward[way],
            device_id_type=MESH_ID,
        )

    def forwards(way, kind, d):
        goes = passes(way, kind, d)
        mine_here = is_mine(way, kind, d)
        whole = goes & jnp.where(mine_here, ends[way] < SPAN - 2, True)
        return whole, goes & mine_here & (ends[way] == SPAN - 2)

    def forward(way, kind, d, h, act):
        whole, first = forwards(way, kind, d)

        @pl.when(whole)
        def _():
            act(send_chunk(way, kind, d, room, h))

        @pl.when(first)
        def _():
            act(send_chunk(way, kind, d, room // 2, h))

        if h == 1:

            @pl.when(whole | first)
            def _():
                act(send_meta(way, kind, d))

    def begin(copy):
        copy.start()

    def finish(copy):
        copy.wait_send()

    def receive(way, kind, d, h):
        goes = passes(way, kind, d)
        short = is_mine(way, kind, d) & (ends[way] == SPAN - 1)

        @pl.when(goes & ~short)
        def _():
            send_chunk(way, kind, d - 1, room, h).wait_recv()

        @pl.when(goes & short)
        def _():
            send_chunk(way, kind, d - 1, room // 2, h).wait_recv()

        if h == 1:

            @pl.when(goes)
            def _():
                send_meta(way, kind, d - 1).wait_recv()

            @pl.when(goes & short)
            def _():
                pool[way, FIRST[kind] + d, pl.ds(room // 2, room // 2)] = jnp.zeros(
                    (room // 2, width), bf16
                )

    q_at = lax.broadcasted_iota(jnp.int32, (WINDOW, 2 * WINDOW), 0)
    k_at = lax.broadcasted_iota(jnp.int32, (WINDOW, 2 * WINDOW), 1)
    reach = q_at + WINDOW - k_at

    def projected(block):
        start = pl.multiple_of(block * WINDOW, WINDOW)
        first = start + sp * tok
        allowed = (reach >= 0) & (reach < WINDOW) & (k_at + first >= WINDOW)
        k = keys_values[0:HDIM, pl.ds(start, 2 * WINDOW)]
        v = keys_values[HDIM:, pl.ds(start, 2 * WINDOW)]
        q = rot_q[pl.ds(start, WINDOW), :]
        heads = []
        for h in range(q.shape[1] // HDIM):
            qh = q[:, h * HDIM : (h + 1) * HDIM]
            s = jnp.dot(qh, k, preferred_element_type=f32)
            s = jnp.where(allowed, s * HDIM ** (-0.5), -jnp.inf)
            sink = sink_ref[h]
            top = jnp.maximum(jnp.max(s, axis=1, keepdims=True), sink)
            e = jnp.exp(s - top)
            below = jnp.sum(e, axis=1, keepdims=True) + jnp.exp(sink - top)
            p = (e / below).astype(bf16)
            seen = lax.dot_general(p, v, (((1,), (1,)), ((), ())), preferred_element_type=f32)
            heads.append(seen.astype(bf16))
        att = jnp.concatenate(heads, axis=1)
        for c in range(width // tile):
            cols = pl.ds(c * tile, tile)
            yield cols, jnp.dot(att, proj_w[:, cols], preferred_element_type=f32)

    def beside(step):
        return {"tp": lax.rem(tp + step + xs, xs)}

    def send_far(way, h):
        return pltpu.make_async_remote_copy(
            src_ref=shares.at[2, part(way), side_cols(h)],
            dst_ref=far_in.at[way, h],
            send_sem=far_send.at[way, h],
            recv_sem=far_recv.at[way, h],
            device_id=beside(1 - 2 * way),
            device_id_type=MESH_ID,
        )

    def send_near(way, h):
        return pltpu.make_async_remote_copy(
            src_ref=shares.at[way, :, side_cols(h)],
            dst_ref=near_in.at[way, h],
            send_sem=near_send.at[way, h],
            recv_sem=near_recv.at[way, h],
            device_id=beside(1 - 2 * way),
            device_id_type=MESH_ID,
        )

    loads[0].wait()
    for cols, y in projected(lax.rem(tp + 2, xs)):
        shares[2, :, cols] = y.astype(bf16)
    for h in range(2):
        for way in range(2):
            send_far(way, h).start()
    for way in range(2):
        for cols, y in projected(lax.rem(tp + 1 - 2 * way + xs, xs)):
            own_share_sum[:, cols] = y
        for h in range(2):
            send_far(way, h).wait_recv()
            alone, joint, cols = part(1 - way), part(way), side_cols(h)
            shares[way, alone, cols] = own_share_sum[alone, cols].astype(bf16)
            joined = own_share_sum[joint, cols] + far_in[way, h].astype(f32)
            shares[way, joint, cols] = joined.astype(bf16)
            send_near(way, h).start()
    for cols, y in projected(tp):
        own_share_sum[:, cols] = y
    loads[1].wait()

    def own_cols(h):
        for way in range(2):
            send_near(way, h).wait_recv()
        cols = side_cols(h)
        got = near_in[0, h].astype(f32) + near_in[1, h].astype(f32)
        x = residual[:, cols].astype(f32) + (own_share_sum[:, cols] + got)
        stream[:, cols] = x.astype(bf16)

    ids = ids_ref[...]
    expert_at = lax.broadcasted_iota(jnp.int32, (ring * peers, rows), 0)
    token_row = lax.broadcasted_iota(jnp.int32, (rows, rows), 0)
    token_col = lax.broadcasted_iota(jnp.int32, (rows, rows), 1)
    ahead = (token_row < token_col).astype(f32).astype(bf16)
    named = [(expert_at == ids[c : c + 1]).astype(f32) for c in range(2)]
    earlier = jnp.dot((named[0] + named[1]).astype(bf16), ahead, preferred_element_type=f32)
    ranks = [jnp.sum(n * earlier, axis=0, keepdims=True) for n in named]
    group = ids[0:1] // EXPERTS_PER_GROUP
    chip = [ids[c : c + 1] // peers for c in range(2)]
    spot = [lax.rem(c, SPAN) for c in chip]
    blocks = ring // SPAN
    apart = lax.rem(group - block + blocks, blocks)
    top = [(spot[0] == SPAN - 1) | (spot[1] == SPAN - 1), (spot[0] == 0) | (spot[1] == 0)]
    beyond = [(spot[0] > at) | (spot[1] > at), (spot[0] < at) | (spot[1] < at)]
    here = (chip[0] == z) | (chip[1] == z)
    joins = [
        (apart == 0) & beyond[0],
        apart == 1,
        (apart == 0) & beyond[1],
        apart == blocks - 1,
        apart == 2,
        here,
    ]
    joins = [x.astype(f32) for x in joins]
    top = [x.astype(f32) for x in top]
    leads = [top[0], top[0], top[1], top[1], jnp.where(at >= SPAN // 2, top[0], top[1]), top[0]]
    pack_row = lax.broadcasted_iota(jnp.int32, (8, rows), 0)
    lead, rest = jnp.zeros((8, rows), f32), jnp.zeros((8, rows), f32)
    for n in range(6):
        lead = jnp.where(pack_row == n, joins[n] * leads[n], lead)
        rest = jnp.where(pack_row == n, joins[n] * (1.0 - leads[n]), rest)
    lead_rank = jnp.dot(lead.astype(bf16), ahead, preferred_element_type=f32)
    rest_rank = jnp.dot(rest.astype(bf16), ahead, preferred_element_type=f32)
    rest_rank += jnp.sum(lead, axis=1, keepdims=True)
    places[...] = jnp.where(lead > 0, lead_rank, jnp.where(rest > 0, rest_rank, -1.0))
    mix = mix_ref[...]
    mix_high = mix.astype(bf16).astype(f32)
    mix_low = mix - mix_high
    facts_row = lax.broadcasted_iota(jnp.int32, (16, rows), 0)
    facts = jnp.where(facts_row == 8, 1.0, 0.0)
    known = [ids[0:1].astype(f32), ids[1:2].astype(f32), ranks[0], ranks[1]]
    known += [mix_high[0:1], mix_high[1:2], mix_low[0:1], mix_low[1:2]]
    for n in range(8):
        facts = jnp.where(facts_row == n, known[n], facts)
    facts = facts.astype(bf16)
    chunk_row = lax.broadcasted_iota(jnp.int32, (room, rows), 0).astype(f32)

    def packing(n):
        return (chunk_row == places[n : n + 1, :]).astype(f32).astype(bf16)

    def pack(n, way, entry, h):
        choose = packing(n)
        per_side = width // 2 // tile
        for c in range(h * per_side, (h + 1) * per_side):
            cols = pl.ds(c * tile, tile)
            got = jnp.dot(choose, stream[:, cols], preferred_element_type=f32)
            pool[way, entry, :, cols] = got.astype(bf16)

    def pack_meta(n, way, entry):
        got = lax.dot_general(
            facts, packing(n), (((1,), (1,)), ((), ())), preferred_element_type=f32
        )
        out_row = lax.broadcasted_iota(jnp.int32, (8, room), 0)
        found = got[8:9] > 0
        out = jnp.where(out_row == 0, jnp.where(found, got[0:1] * CAP + got[2:3], -1.0), 0.0)
        out = jnp.where(out_row == 1, jnp.where(found, got[1:2] * CAP + got[3:4], -1.0), out)
        out = jnp.where(out_row == 2, got[4:5] + got[6:7], out)
        out = jnp.where(out_row == 3, got[5:6] + got[7:8], out)
        pool_meta[way, entry] = jnp.concatenate([out, jnp.zeros_like(out)], axis=1)

    packs = ((4, opposite_way, 2), (1, 0, 1), (3, 1, 1), (0, 0, 0), (2, 1, 0))
    for n, way, kind in packs:
        pack_meta(n, way, FIRST[kind])
    pack_meta(5, 0, HOME)

    for h in range(2):
        own_cols(h)
        for n, way, kind in packs:
            pack(n, way, FIRST[kind], h)
            for w in range(2) if kind == 2 else (way,):
                forward(w, kind, 0, h, begin)
        pack(5, 0, HOME, h)

    row_id = lax.broadcasted_iota(jnp.int32, (room, room), 0)
    local_code = (row_id // (2 * CAP)) * CAP + lax.rem(row_id, CAP)
    which_half = lax.rem(row_id, 2 * CAP) // CAP
    base = z * (peers * CAP)

    def paired(back):
        late = (at == SPAN - 1) & ((back == far - 1) | (back == far + 1))
        return jnp.where(late, ring - back, back)

    def locate(back):
        other = back > at + SPAN + SPAN // 2
        d = jnp.where(other, ring - back, back)
        end = jnp.where(other, ends[1], ends[0])
        i = lax.rem(end - d + 3 * SPAN, SPAN)
        crossed = (d + i - end) // SPAN
        first = jnp.where(crossed == 0, FIRST[0], jnp.where(crossed == 1, FIRST[1], FIRST[2]))
        entry = jnp.where(back == 0, HOME, first + d)
        return jnp.where(other, 1, 0), entry

    def matches(way, entry, side):
        code = jnp.where(which_half == side, local_code + base, -2).astype(f32)
        m = pool_meta[way, entry][:, 0:room]
        return code == m[0:1, :], code == m[1:2, :], m

    def pick_of(way, entry, side):
        first_hit, second_hit, _ = matches(way, entry, side)
        return (first_hit | second_hit).astype(f32).astype(bf16)

    def weights_of(way, entry, side):
        first_hit, second_hit, m = matches(way, entry, side)
        w = jnp.where(first_hit, m[2:3, :], 0.0) + jnp.where(second_hit, m[3:4, :], 0.0)
        high = w.astype(bf16)
        return high, (w - high.astype(f32)).astype(bf16)

    def exchange(src, dst, sends, recvs, step, offset):
        u, where = peer(offset)
        return pltpu.make_async_remote_copy(
            src_ref=src.at[step, u],
            dst_ref=dst.at[step, mine],
            send_sem=sends.at[step, offset],
            recv_sem=recvs.at[step, offset],
            device_id=where,
            device_id_type=MESH_ID,
        )

    def pick(step):
        a, b = locate(paired(step)), locate(paired(ring - 1 - step))
        one_a, one_b = pick_of(*a, 0), pick_of(*b, 1)
        square = jnp.zeros((room, 1), f32)
        for c in range(width // tile):
            cols = pl.ds(c * tile, tile)
            got = jnp.dot(one_a, pool[a[0], a[1], :, cols], preferred_element_type=f32)
            got += jnp.dot(one_b, pool[b[0], b[1], :, cols], preferred_element_type=f32)
            square += jnp.sum(got * got, axis=1, keepdims=True)
            unscaled[:, cols] = got
        scale = lax.rsqrt(square / width + norm_eps)
        for c in range(width // tile):
            cols = pl.ds(c * tile, tile)
            got = (unscaled[:, cols] * scale * gain_ref[:, cols]).astype(bf16)
            picked[step, :, :, cols] = got.reshape(peers, 2 * CAP, tile)
        for o in range(1, peers):
            exchange(picked, routed, pick_send, pick_recv, step, o).start()
        routed[step, mine] = picked[step, mine]

    def serve(step):
        for o in range(1, peers):
            exchange(picked, routed, pick_send, pick_recv, step, o).wait_recv()
        x = routed[step].reshape(peers * 2 * CAP, width)
        g = jnp.dot(x, gate_w[...], preferred_element_type=f32)
        u = jnp.dot(x, up_w[...], preferred_element_type=f32)
        hidden = (g * (1.0 / (1.0 + jnp.exp(-g))) * u).astype(bf16)
        for c in range(width // tile):
            cols = pl.ds(c * tile, tile)
            y = jnp.dot(hidden, down_w[:, cols], preferred_element_type=f32)
            made[step, :, :, cols] = y.astype(bf16).reshape(peers, 2 * CAP, tile)
        for o in range(1, peers):
            exchange(made, back, back_send, back_recv, step, o).start()
        back[step, mine] = made[step, mine]

    def ring_step(d, _):
        for kind in (2, 1, 0):
            for h in range(2):
                for way in range(2):
                    receive(way, kind, d, h)
                    forward(way, kind, d, h, begin)

        @pl.when(d <= far - 1)
        def _():
            pick(d - 1)

        @pl.when((d >= 2) & (d <= far))
        def _():
            serve(d - 2)

        return 0

    for load in loads[2:]:
        load.wait()
    lax.fori_loop(1, LAST[2] + 1, ring_step, 0)
    contract = (((0,), (0,)), ((), ()))

    def wait_back(step):
        for o in range(1, peers):
            exchange(made, back, back_send, back_recv, step, o).wait_recv()

    def own_share(way, entry, behind, dst):
        place_of = paired(behind)
        side = jnp.where(place_of >= far, 1, 0)
        step = jnp.where(place_of >= far, ring - 1 - place_of, place_of)
        high, low = weights_of(way, entry, side)
        w = jnp.concatenate([high, low], axis=0)
        for c in range(width // tile):
            cols = pl.ds(c * tile, tile)
            y = back[step, :, :, cols].reshape(room, tile)
            y = jnp.concatenate([y, y], axis=0)
            dst[:, cols] = lax.dot_general(w, y, contract, preferred_element_type=f32)

    def lines(h):
        return pl.ds(h * (room // 2), room // 2)

    def send_sum(way, kind, d, h):
        entry = FIRST[kind] + d
        return pltpu.make_async_remote_copy(
            src_ref=sums.at[way, entry, lines(h)],
            dst_ref=sums.at[way, entry - 1, lines(h)],
            send_sem=sum_send.at[way, entry, h],
            recv_sem=sum_recv.at[way, entry - 1, h],
            device_id=onward[1 - way],
            device_id_type=MESH_ID,
        )

    def gives(way, kind, d, h):
        goes = passes(way, kind, d)
        return goes if h == 0 else goes & ~(is_mine(way, kind, d) & (ends[way] == SPAN - 1))

    def give_back(way, kind, d, act):
        for h in range(2):

            @pl.when(gives(way, kind, d, h))
            def _():
                act(send_sum(way, kind, d, h))

    def sum_entry(way, kind, d, h):
        entry = FIRST[kind] + d
        goes = passes(way, kind, d)
        mine_here = is_mine(way, kind, d)
        comes = ends[way] < SPAN - 1 - h

        @pl.when(goes & (comes | ~mine_here))
        def _():
            send_sum(way, kind, d + 1, h).wait_recv()

        @pl.when(goes & comes & mine_here)
        def _():
            got = sums[way, entry, lines(h)].astype(f32) + own_part[way, lines(h)]
            sums[way, entry, lines(h)] = got.astype(bf16)

        @pl.when(goes & ~comes & mine_here)
        def _():
            sums[way, entry, lines(h)] = own_part[way, lines(h)].astype(bf16)

        @pl.when(gives(way, kind, d, h))
        def _():
            send_sum(way, kind, d, h).start()

    def return_kind(kind, d):
        for way in range(2):

            @pl.when(passes(way, kind, d) & is_mine(way, kind, d))
            def _():
                behind = d if way == 0 else ring - d
                own_share(way, FIRST[kind] + d, behind, own_part.at[way])

        for h in (1, 0):
            for way in range(2):
                sum_entry(way, kind, d, h)

    def place(n, value):
        choose = packing(n)
        for c in range(width // tile):
            cols = pl.ds(c * tile, tile)
            got = lax.dot_general(choose, value(cols), contract, preferred_element_type=f32)
            total[:, cols] += got

    def land(n, way, kind):
        whole, first = forwards(way, kind, 0)

        @pl.when(whole | first)
        def _():
            send_sum(way, kind, 1, 0).wait_recv()

        @pl.when(whole)
        def _():
            send_sum(way, kind, 1, 1).wait_recv()

        @pl.when(first)
        def _():
            sums[way, FIRST[kind], lines(1)] = jnp.zeros((room // 2, width), bf16)

        @pl.when(whole | first)
        def _():
            place(n, lambda cols: sums[way, FIRST[kind], :, cols])

    pick(far - 1)
    wait_back(0)
    own_share(0, HOME, 0, own_part.at[0])
    total[...] = stream[...].astype(f32)
    place(5, lambda cols: own_part[0, :, cols].astype(bf16))
    wait_back(far - 2)
    return_kind(1, LAST[1])
    serve(far - 1)

    def sum_step(i, _):
        r = far - i

        @pl.when((r >= 4) & (r <= far))
        def _():
            wait_back(r - 3)

        @pl.when(r == jnp.where((at == 0) | (at == SPAN - 1), far, far - 1))
        def _():
            wait_back(far - 1)

        return_kind(2, r + 1)

        @pl.when((r >= 1) & (r <= LAST[0]))
        def _():
            return_kind(0, r)

        @pl.when(r >= 3)
        def _():
            return_kind(1, r - 2)

        return 0

    lax.fori_loop(0, far + 1, sum_step, 0)
    for n, way, kind in ((1, 0, 1), (3, 1, 1), (0, 0, 0), (2, 1, 0), (4, 0, 2), (4, 1, 2)):
        land(n, way, kind)
    out_ref[...] = total[...].astype(bf16)

    def drain(d, _):
        for kind in range(3):
            for way in range(2):
                for h in range(2):
                    forward(way, kind, d, h, finish)

                @pl.when(d >= 1)
                def _():
                    give_back(way, kind, d, lambda copy: copy.wait_send())

        return 0

    lax.fori_loop(0, LAST[2] + 1, drain, 0)

    def drain_steps(n, _):
        for o in range(1, peers):
            exchange(picked, routed, pick_send, pick_recv, n, o).wait_send()
            exchange(made, back, back_send, back_recv, n, o).wait_send()
        return 0

    lax.fori_loop(0, far, drain_steps, 0)
    halo.wait_send()
    for h in range(2):
        for way in range(2):
            send_far(way, h).wait_send()
            send_near(way, h).wait_send()


def layer(query, key, value, cosines, sines, sinks, gain, ids, mix, residual, proj, gate, up, down):
    rows, width = residual.shape
    ring = lax.axis_size("sp") // CORES
    xs = lax.axis_size("tp")
    far = ring // 2
    peers = xs * CORES
    hidden = gate.shape[1]
    room = 2 * peers * CAP
    tile = min(512, width // 2)
    bf16, f32 = jnp.bfloat16, jnp.float32
    vmem = pl.BlockSpec(memory_space=pltpu.VMEM)
    smem = pl.BlockSpec(memory_space=pltpu.SMEM)
    hbm = pl.BlockSpec(memory_space=pl.ANY)
    slab = (far, peers, 2 * CAP, width)
    dma = pltpu.SemaphoreType.DMA
    return pl.pallas_call(
        functools.partial(expert_kernel, ring, xs, tile),
        out_shape=jax.ShapeDtypeStruct((rows, width), bf16),
        in_specs=[vmem] * 5 + [smem] + [vmem] * 3 + [hbm] * 5,
        out_specs=vmem,
        scratch_shapes=[
            pltpu.VMEM(query.shape, bf16),
            pltpu.VMEM((2 * HDIM, query.shape[0] + WINDOW), bf16),
            pltpu.VMEM((rows, width), bf16),
            pltpu.VMEM(proj.shape, bf16),
            pltpu.VMEM((3, rows, width), bf16),
            pltpu.VMEM((2, 2, rows // 2, width // 2), bf16),
            pltpu.VMEM((2, 2, rows, width // 2), bf16),
            pltpu.VMEM((rows, width), f32),
            pltpu.VMEM((rows, width), bf16),
            pltpu.VMEM((room, width), f32),
            pltpu.VMEM((8, rows), f32),
            pltpu.VMEM((2, ENTRIES, room, width), bf16),
            pltpu.VMEM((rows, width), f32),
            pltpu.VMEM((2, ENTRIES + 1, room, width), bf16),
            pltpu.VMEM((2, ENTRIES + 1, 8, rows), f32),
            pltpu.VMEM(slab, bf16),
            pltpu.VMEM(slab, bf16),
            pltpu.VMEM(slab, bf16),
            pltpu.VMEM(slab, bf16),
            pltpu.VMEM((2, room, width), f32),
            pltpu.VMEM((width, hidden), bf16),
            pltpu.VMEM((width, hidden), bf16),
            pltpu.VMEM((hidden, width), bf16),
            dma((5,)),
            dma((2, ENTRIES, 2)),
            dma((2, ENTRIES, 2)),
            dma((2, ENTRIES)),
            dma((2, ENTRIES)),
            dma((far, peers)),
            dma((far, peers)),
            dma((far, peers)),
            dma((far, peers)),
            dma((2, ENTRIES, 2)),
            dma((2, ENTRIES, 2)),
            dma,
            dma,
            dma((2, 2)),
            dma((2, 2)),
            dma((2, 2)),
            dma((2, 2)),
        ],
        compiler_params=pltpu.CompilerParams(
            collective_id=1, has_side_effects=True, vmem_limit_bytes=60 * 1024 * 1024
        ),
    )(query, key, value, cosines, sines, sinks, gain, ids, mix, residual, proj, gate, up, down)


def per_device(
    query_rows,
    key_rows,
    value_rows,
    sink_logits,
    residual,
    out_weight,
    norm_gain,
    gate_weight,
    up_weight,
    down_weight,
    routes,
    route_weight,
):
    tok_count = query_rows.shape[0]
    positions = lax.axis_index("sp") * tok_count + jnp.arange(tok_count, dtype=jnp.int32)
    half_dim = HDIM // 2
    inverse = rope_base ** (-jnp.arange(half_dim, dtype=jnp.float32) / half_dim)
    angles = positions.astype(jnp.float32)[None, :] * inverse[:, None]
    cosines = jnp.cos(angles)
    sines = jnp.sin(angles)
    return layer(
        query_rows,
        key_rows.T,
        value_rows.T,
        cosines,
        sines,
        sink_logits,
        norm_gain[None, :],
        routes.T,
        route_weight.T,
        residual,
        out_weight,
        gate_weight[0],
        up_weight[0],
        down_weight[0],
    )


def solution(mesh):
    in_specs = (
        P(("grp", "sp"), "tp"),
        P(("grp", "sp"), "tp"),
        P(("grp", "sp"), "tp"),
        P("tp"),
        P(("grp", "sp", "tp"), None),
        P("tp", None),
        P(),
        P(("sp", "tp"), None, None),
        P(("sp", "tp"), None, None),
        P(("sp", "tp"), None, None),
        P(("grp", "sp", "tp"), None),
        P(("grp", "sp", "tp"), None),
    )
    out_specs = P(("grp", "sp", "tp"), None)
    return jax.shard_map(
        per_device, mesh=mesh, in_specs=in_specs, out_specs=out_specs, check_vma=False
    )
```

```python
import functools

import jax
import jax.numpy as jnp
from jax import lax
from jax.experimental import pallas as pl
from jax.experimental.pallas import tpu as pltpu
from jax.sharding import PartitionSpec as P

MESH_ID = pl.DeviceIdType.MESH
HDIM = 64
WINDOW = 128
CAP = 4
CORES = 2
EXPERTS_PER_GROUP = 32
SPAN = 4
FIRST = (0, 4, 12)
LAST = (3, 7, 9)
ENTRIES = 22
HOME = 22


rope_base = 10000.0
norm_eps = 1e-06


def expert_kernel(
    ring,
    xs,
    tile,
    query_ref,
    key_ref,
    value_ref,
    cos_ref,
    sin_ref,
    sink_ref,
    gain_ref,
    ids_ref,
    mix_ref,
    residual_hbm,
    proj_hbm,
    gate_hbm,
    up_hbm,
    down_hbm,
    out_ref,
    rot_q,
    keys_values,
    residual,
    proj_w,
    shares,
    far_in,
    near_in,
    own_share_sum,
    stream,
    unscaled,
    places,
    sums,
    total,
    pool,
    pool_meta,
    picked,
    routed,
    made,
    back,
    own_part,
    gate_w,
    up_w,
    down_w,
    weight_sem,
    pool_send,
    pool_recv,
    meta_send,
    meta_recv,
    pick_send,
    pick_recv,
    back_send,
    back_recv,
    sum_send,
    sum_recv,
    halo_send,
    halo_recv,
    far_send,
    far_recv,
    near_send,
    near_recv,
):
    f32, bf16 = jnp.float32, jnp.bfloat16
    rows, width = residual.shape
    half = rows // 2
    far = ring // 2
    peers = xs * CORES
    sp, tp = lax.axis_index("sp"), lax.axis_index("tp")
    core = lax.rem(sp, CORES)
    z = sp // CORES
    mine = core * xs + tp
    nxt = {"sp": lax.rem(sp + CORES, ring * CORES)}
    prv = {"sp": lax.rem(sp + (ring - 1) * CORES, ring * CORES)}

    far_first = sorted(range(1, peers), key=lambda o: -min(o % xs, xs - o % xs))

    def peer(offset):
        u = lax.rem(mine + offset, peers)
        return u, {"sp": z * CORES + u // xs, "tp": lax.rem(u, xs)}

    loads = [
        pltpu.make_async_copy(src, dst, weight_sem.at[i])
        for i, (src, dst) in enumerate(
            (
                (proj_hbm, proj_w),
                (residual_hbm, residual),
                (gate_hbm, gate_w),
                (up_hbm, up_w),
                (down_hbm, down_w),
            )
        )
    ]
    for load in loads:
        load.start()

    barrier = pltpu.get_barrier_semaphore()
    pl.semaphore_signal(barrier, inc=1, device_id=nxt, device_id_type=MESH_ID)
    pl.semaphore_signal(barrier, inc=1, device_id=prv, device_id_type=MESH_ID)
    total_sp = ring * CORES
    after = {"sp": lax.rem(sp + 1, total_sp)}
    across = {"sp": lax.rem(sp + jnp.where(core == 1, 1, total_sp - 1), total_sp)}
    pl.semaphore_signal(barrier, inc=1, device_id=across, device_id_type=MESH_ID)
    for o in range(1, peers):
        pl.semaphore_signal(barrier, inc=1, device_id=peer(o)[1], device_id_type=MESH_ID)

    lane = lax.broadcasted_iota(jnp.int32, (query_ref.shape[1],) * 2, 1)
    line = lax.broadcasted_iota(jnp.int32, (query_ref.shape[1],) * 2, 0)
    low = lax.rem(lane, HDIM) < HDIM // 2
    turn = jnp.where(low & (line == lane + HDIM // 2), -1.0, 0.0)
    turn = (turn + jnp.where((~low) & (line == lane - HDIM // 2), 1.0, 0.0)).astype(bf16)

    def rotated(x, cosines, sines):
        n = x.shape[1]
        swapped = jnp.dot(x, turn[:n, :n], preferred_element_type=f32)
        return (x.astype(f32) * cosines + swapped * sines).astype(bf16)

    tok = query_ref.shape[0]
    k_low = key_ref[0 : HDIM // 2].astype(f32)
    k_high = key_ref[HDIM // 2 :].astype(f32)
    turned_low = k_low * cos_ref[...] - k_high * sin_ref[...]
    turned_high = k_high * cos_ref[...] + k_low * sin_ref[...]
    turned_k = jnp.concatenate([turned_low, turned_high], axis=0)
    keys_values[0:HDIM, WINDOW:] = turned_k.astype(bf16)
    keys_values[HDIM:, WINDOW:] = value_ref[...]
    pl.semaphore_wait(barrier, peers + 2)
    halo = pltpu.make_async_remote_copy(
        src_ref=keys_values.at[:, pl.ds(tok, WINDOW)],
        dst_ref=keys_values.at[:, pl.ds(0, WINDOW)],
        send_sem=halo_send,
        recv_sem=halo_recv,
        device_id=after,
        device_id_type=MESH_ID,
    )
    halo.start()
    repeats = 128 // (HDIM // 2)
    cosines = jnp.concatenate([cos_ref[...]] * repeats, axis=0).T
    sines = jnp.concatenate([sin_ref[...]] * repeats, axis=0).T
    for c in range(query_ref.shape[1] // 128):
        cols = pl.ds(c * 128, 128)
        rot_q[:, cols] = rotated(query_ref[:, cols], cosines, sines)
    halo.wait_recv()

    def part(h):
        return pl.ds(h * half, half)

    def side_cols(h):
        return pl.ds(h * (width // 2), width // 2)

    block, at = z // SPAN, lax.rem(z, SPAN)
    opposite_way = jnp.where(at >= SPAN // 2, 0, 1)
    ends = (at, SPAN - 1 - at)
    onward = (nxt, prv)
    room = 2 * peers * CAP

    def origin(way, d):
        i = lax.rem(ends[way] - d + 3 * SPAN, SPAN)
        return i, (d + i - ends[way]) // SPAN

    def passes(way, kind, d):
        i, crossed = origin(way, d)
        there = (d <= LAST[kind]) & (kind >= crossed)
        return there & (i >= SPAN // 2) if kind == 2 else there

    def is_mine(way, kind, d):
        return origin(way, d)[1] == kind

    def send_chunk(way, kind, d, count, h):
        entry = FIRST[kind] + d
        return pltpu.make_async_remote_copy(
            src_ref=pool.at[way, entry, pl.ds(0, count), side_cols(h)],
            dst_ref=pool.at[way, entry + 1, pl.ds(0, count), side_cols(h)],
            send_sem=pool_send.at[way, entry, h],
            recv_sem=pool_recv.at[way, entry + 1, h],
            device_id=onward[way],
            device_id_type=MESH_ID,
        )

    def send_meta(way, kind, d):
        entry = FIRST[kind] + d
        return pltpu.make_async_remote_copy(
            src_ref=pool_meta.at[way, entry],
            dst_ref=pool_meta.at[way, entry + 1],
            send_sem=meta_send.at[way, entry],
            recv_sem=meta_recv.at[way, entry + 1],
            device_id=onward[way],
            device_id_type=MESH_ID,
        )

    def forwards(way, kind, d):
        goes = passes(way, kind, d)
        mine_here = is_mine(way, kind, d)
        whole = goes & jnp.where(mine_here, ends[way] < SPAN - 2, True)
        return whole, goes & mine_here & (ends[way] == SPAN - 2)

    def forward(way, kind, d, h, act):
        whole, first = forwards(way, kind, d)

        @pl.when(whole)
        def _():
            act(send_chunk(way, kind, d, room, h))

        @pl.when(first)
        def _():
            act(send_chunk(way, kind, d, room // 2, h))

        if h == 1:

            @pl.when(whole | first)
            def _():
                act(send_meta(way, kind, d))

    def begin(copy):
        copy.start()

    def finish(copy):
        copy.wait_send()

    def receive(way, kind, d, h):
        goes = passes(way, kind, d)
        short = is_mine(way, kind, d) & (ends[way] == SPAN - 1)

        @pl.when(goes & ~short)
        def _():
            send_chunk(way, kind, d - 1, room, h).wait_recv()

        @pl.when(goes & short)
        def _():
            send_chunk(way, kind, d - 1, room // 2, h).wait_recv()

        if h == 1:

            @pl.when(goes)
            def _():
                send_meta(way, kind, d - 1).wait_recv()

            @pl.when(goes & short)
            def _():
                pool[way, FIRST[kind] + d, pl.ds(room // 2, room // 2)] = jnp.zeros(
                    (room // 2, width), bf16
                )

    q_at = lax.broadcasted_iota(jnp.int32, (WINDOW, 2 * WINDOW), 0)
    k_at = lax.broadcasted_iota(jnp.int32, (WINDOW, 2 * WINDOW), 1)
    reach = q_at + WINDOW - k_at

    def projected(block):
        start = pl.multiple_of(block * WINDOW, WINDOW)
        first = start + sp * tok
        allowed = (reach >= 0) & (reach < WINDOW) & (k_at + first >= WINDOW)
        k = keys_values[0:HDIM, pl.ds(start, 2 * WINDOW)]
        v = keys_values[HDIM:, pl.ds(start, 2 * WINDOW)]
        q = rot_q[pl.ds(start, WINDOW), :]
        heads = []
        for h in range(q.shape[1] // HDIM):
            qh = q[:, h * HDIM : (h + 1) * HDIM]
            s = jnp.dot(qh, k, preferred_element_type=f32)
            s = jnp.where(allowed, s * HDIM ** (-0.5), -jnp.inf)
            sink = sink_ref[h]
            top = jnp.maximum(jnp.max(s, axis=1, keepdims=True), sink)
            e = jnp.exp(s - top)
            below = jnp.sum(e, axis=1, keepdims=True) + jnp.exp(sink - top)
            p = (e / below).astype(bf16)
            seen = lax.dot_general(p, v, (((1,), (1,)), ((), ())), preferred_element_type=f32)
            heads.append(seen.astype(bf16))
        att = jnp.concatenate(heads, axis=1)
        for c in range(width // tile):
            cols = pl.ds(c * tile, tile)
            yield cols, jnp.dot(att, proj_w[:, cols], preferred_element_type=f32)

    def beside(step):
        return {"tp": lax.rem(tp + step + xs, xs)}

    def send_far(way, h):
        return pltpu.make_async_remote_copy(
            src_ref=shares.at[2, part(way), side_cols(h)],
            dst_ref=far_in.at[way, h],
            send_sem=far_send.at[way, h],
            recv_sem=far_recv.at[way, h],
            device_id=beside(1 - 2 * way),
            device_id_type=MESH_ID,
        )

    def send_near(way, h):
        return pltpu.make_async_remote_copy(
            src_ref=shares.at[way, :, side_cols(h)],
            dst_ref=near_in.at[way, h],
            send_sem=near_send.at[way, h],
            recv_sem=near_recv.at[way, h],
            device_id=beside(1 - 2 * way),
            device_id_type=MESH_ID,
        )

    loads[0].wait()
    per_side = width // 2 // tile
    for c, (cols, y) in enumerate(projected(lax.rem(tp + 2, xs))):
        shares[2, :, cols] = y.astype(bf16)
        if (c + 1) % per_side == 0:
            for way in range(2):
                send_far(way, c // per_side).start()
    for way in range(2):
        for c, (cols, y) in enumerate(projected(lax.rem(tp + 1 - 2 * way + xs, xs))):
            own_share_sum[:, cols] = y
            if (c + 1) % per_side == 0:
                h = c // per_side
                send_far(way, h).wait_recv()
                alone, joint, side = part(1 - way), part(way), side_cols(h)
                shares[way, alone, side] = own_share_sum[alone, side].astype(bf16)
                joined = own_share_sum[joint, side] + far_in[way, h].astype(f32)
                shares[way, joint, side] = joined.astype(bf16)
                send_near(way, h).start()
    for cols, y in projected(tp):
        own_share_sum[:, cols] = y
    loads[1].wait()

    def own_cols(h):
        for way in range(2):
            send_near(way, h).wait_recv()
        cols = side_cols(h)
        got = near_in[0, h].astype(f32) + near_in[1, h].astype(f32)
        x = residual[:, cols].astype(f32) + (own_share_sum[:, cols] + got)
        stream[:, cols] = x.astype(bf16)

    ids = ids_ref[...]
    expert_at = lax.broadcasted_iota(jnp.int32, (ring * peers, rows), 0)
    token_row = lax.broadcasted_iota(jnp.int32, (rows, rows), 0)
    token_col = lax.broadcasted_iota(jnp.int32, (rows, rows), 1)
    ahead = (token_row < token_col).astype(f32).astype(bf16)
    named = [(expert_at == ids[c : c + 1]).astype(f32) for c in range(2)]
    earlier = jnp.dot((named[0] + named[1]).astype(bf16), ahead, preferred_element_type=f32)
    ranks = [jnp.sum(n * earlier, axis=0, keepdims=True) for n in named]
    group = ids[0:1] // EXPERTS_PER_GROUP
    chip = [ids[c : c + 1] // peers for c in range(2)]
    spot = [lax.rem(c, SPAN) for c in chip]
    blocks = ring // SPAN
    apart = lax.rem(group - block + blocks, blocks)
    top = [(spot[0] == SPAN - 1) | (spot[1] == SPAN - 1), (spot[0] == 0) | (spot[1] == 0)]
    beyond = [(spot[0] > at) | (spot[1] > at), (spot[0] < at) | (spot[1] < at)]
    here = (chip[0] == z) | (chip[1] == z)
    joins = [
        (apart == 0) & beyond[0],
        apart == 1,
        (apart == 0) & beyond[1],
        apart == blocks - 1,
        apart == 2,
        here,
    ]
    joins = [x.astype(f32) for x in joins]
    top = [x.astype(f32) for x in top]
    leads = [top[0], top[0], top[1], top[1], jnp.where(at >= SPAN // 2, top[0], top[1]), top[0]]
    pack_row = lax.broadcasted_iota(jnp.int32, (8, rows), 0)
    lead, rest = jnp.zeros((8, rows), f32), jnp.zeros((8, rows), f32)
    for n in range(6):
        lead = jnp.where(pack_row == n, joins[n] * leads[n], lead)
        rest = jnp.where(pack_row == n, joins[n] * (1.0 - leads[n]), rest)
    lead_rank = jnp.dot(lead.astype(bf16), ahead, preferred_element_type=f32)
    rest_rank = jnp.dot(rest.astype(bf16), ahead, preferred_element_type=f32)
    rest_rank += jnp.sum(lead, axis=1, keepdims=True)
    places[...] = jnp.where(lead > 0, lead_rank, jnp.where(rest > 0, rest_rank, -1.0))
    mix = mix_ref[...]
    mix_high = mix.astype(bf16).astype(f32)
    mix_low = mix - mix_high
    facts_row = lax.broadcasted_iota(jnp.int32, (16, rows), 0)
    facts = jnp.where(facts_row == 8, 1.0, 0.0)
    known = [ids[0:1].astype(f32), ids[1:2].astype(f32), ranks[0], ranks[1]]
    known += [mix_high[0:1], mix_high[1:2], mix_low[0:1], mix_low[1:2]]
    for n in range(8):
        facts = jnp.where(facts_row == n, known[n], facts)
    facts = facts.astype(bf16)
    chunk_row = lax.broadcasted_iota(jnp.int32, (room, rows), 0).astype(f32)

    def packing(n):
        return (chunk_row == places[n : n + 1, :]).astype(f32).astype(bf16)

    def pack(n, way, entry, h):
        choose = packing(n)
        for c in range(h * per_side, (h + 1) * per_side):
            cols = pl.ds(c * tile, tile)
            got = jnp.dot(choose, stream[:, cols], preferred_element_type=f32)
            pool[way, entry, :, cols] = got.astype(bf16)

    def pack_meta(n, way, entry):
        got = lax.dot_general(
            facts, packing(n), (((1,), (1,)), ((), ())), preferred_element_type=f32
        )
        out_row = lax.broadcasted_iota(jnp.int32, (8, room), 0)
        found = got[8:9] > 0
        out = jnp.where(out_row == 0, jnp.where(found, got[0:1] * CAP + got[2:3], -1.0), 0.0)
        out = jnp.where(out_row == 1, jnp.where(found, got[1:2] * CAP + got[3:4], -1.0), out)
        out = jnp.where(out_row == 2, got[4:5] + got[6:7], out)
        out = jnp.where(out_row == 3, got[5:6] + got[7:8], out)
        pool_meta[way, entry] = jnp.concatenate([out, jnp.zeros_like(out)], axis=1)

    packs = ((4, opposite_way, 2), (1, 0, 1), (3, 1, 1), (0, 0, 0), (2, 1, 0))
    for n, way, kind in packs:
        pack_meta(n, way, FIRST[kind])
    pack_meta(5, 0, HOME)

    for h in range(2):
        own_cols(h)
        for n, way, kind in packs:
            pack(n, way, FIRST[kind], h)
            for w in range(2) if kind == 2 else (way,):
                forward(w, kind, 0, h, begin)
        pack(5, 0, HOME, h)

    row_id = lax.broadcasted_iota(jnp.int32, (room, room), 0)
    local_code = (row_id // (2 * CAP)) * CAP + lax.rem(row_id, CAP)
    which_half = lax.rem(row_id, 2 * CAP) // CAP
    base = z * (peers * CAP)

    def paired(back):
        late = (at == SPAN - 1) & ((back == far - 1) | (back == far + 1))
        return jnp.where(late, ring - back, back)

    def locate(back):
        other = back > at + SPAN + SPAN // 2
        d = jnp.where(other, ring - back, back)
        end = jnp.where(other, ends[1], ends[0])
        i = lax.rem(end - d + 3 * SPAN, SPAN)
        crossed = (d + i - end) // SPAN
        first = jnp.where(crossed == 0, FIRST[0], jnp.where(crossed == 1, FIRST[1], FIRST[2]))
        entry = jnp.where(back == 0, HOME, first + d)
        return jnp.where(other, 1, 0), entry

    def matches(way, entry, side):
        code = jnp.where(which_half == side, local_code + base, -2).astype(f32)
        m = pool_meta[way, entry][:, 0:room]
        return code == m[0:1, :], code == m[1:2, :], m

    def pick_of(way, entry, side):
        first_hit, second_hit, _ = matches(way, entry, side)
        return (first_hit | second_hit).astype(f32).astype(bf16)

    def weights_of(way, entry, side):
        first_hit, second_hit, m = matches(way, entry, side)
        w = jnp.where(first_hit, m[2:3, :], 0.0) + jnp.where(second_hit, m[3:4, :], 0.0)
        high = w.astype(bf16)
        return high, (w - high.astype(f32)).astype(bf16)

    def exchange(src, dst, sends, recvs, step, offset):
        u, where = peer(offset)
        return pltpu.make_async_remote_copy(
            src_ref=src.at[step, u],
            dst_ref=dst.at[step, mine],
            send_sem=sends.at[step, offset],
            recv_sem=recvs.at[step, offset],
            device_id=where,
            device_id_type=MESH_ID,
        )

    def pick(step):
        a, b = locate(paired(step)), locate(paired(ring - 1 - step))
        one_a, one_b = pick_of(*a, 0), pick_of(*b, 1)
        square = jnp.zeros((room, 1), f32)
        for c in range(width // tile):
            cols = pl.ds(c * tile, tile)
            got = jnp.dot(one_a, pool[a[0], a[1], :, cols], preferred_element_type=f32)
            got += jnp.dot(one_b, pool[b[0], b[1], :, cols], preferred_element_type=f32)
            square += jnp.sum(got * got, axis=1, keepdims=True)
            unscaled[:, cols] = got
        scale = lax.rsqrt(square / width + norm_eps)
        for c in range(width // tile):
            cols = pl.ds(c * tile, tile)
            got = (unscaled[:, cols] * scale * gain_ref[:, cols]).astype(bf16)
            picked[step, :, :, cols] = got.reshape(peers, 2 * CAP, tile)
        for o in far_first:
            exchange(picked, routed, pick_send, pick_recv, step, o).start()
        routed[step, mine] = picked[step, mine]

    def serve(step):
        for o in range(1, peers):
            exchange(picked, routed, pick_send, pick_recv, step, o).wait_recv()
        x = routed[step].reshape(peers * 2 * CAP, width)
        g = jnp.dot(x, gate_w[...], preferred_element_type=f32)
        u = jnp.dot(x, up_w[...], preferred_element_type=f32)
        hidden = (g * (1.0 / (1.0 + jnp.exp(-g))) * u).astype(bf16)
        for c in range(width // tile):
            cols = pl.ds(c * tile, tile)
            y = jnp.dot(hidden, down_w[:, cols], preferred_element_type=f32)
            made[step, :, :, cols] = y.astype(bf16).reshape(peers, 2 * CAP, tile)
        for o in far_first:
            exchange(made, back, back_send, back_recv, step, o).start()
        back[step, mine] = made[step, mine]

    def ring_step(d, _):
        for kind in (2, 1, 0):
            for h in range(2):
                for way in range(2):
                    receive(way, kind, d, h)
                    forward(way, kind, d, h, begin)

        @pl.when(d <= far - 1)
        def _():
            pick(d - 1)

        @pl.when((d >= 2) & (d <= far))
        def _():
            serve(d - 2)

        return 0

    for load in loads[2:]:
        load.wait()
    lax.fori_loop(1, LAST[2] + 1, ring_step, 0)
    contract = (((0,), (0,)), ((), ()))

    def wait_back(step):
        for o in range(1, peers):
            exchange(made, back, back_send, back_recv, step, o).wait_recv()

    def own_share(way, entry, behind, dst):
        place_of = paired(behind)
        side = jnp.where(place_of >= far, 1, 0)
        step = jnp.where(place_of >= far, ring - 1 - place_of, place_of)
        high, low = weights_of(way, entry, side)
        w = jnp.concatenate([high, low], axis=0)
        for c in range(width // tile):
            cols = pl.ds(c * tile, tile)
            y = back[step, :, :, cols].reshape(room, tile)
            y = jnp.concatenate([y, y], axis=0)
            dst[:, cols] = lax.dot_general(w, y, contract, preferred_element_type=f32)

    def lines(h):
        return pl.ds(h * (room // 2), room // 2)

    def send_sum(way, kind, d, h):
        entry = FIRST[kind] + d
        return pltpu.make_async_remote_copy(
            src_ref=sums.at[way, entry, lines(h)],
            dst_ref=sums.at[way, entry - 1, lines(h)],
            send_sem=sum_send.at[way, entry, h],
            recv_sem=sum_recv.at[way, entry - 1, h],
            device_id=onward[1 - way],
            device_id_type=MESH_ID,
        )

    def gives(way, kind, d, h):
        goes = passes(way, kind, d)
        return goes if h == 0 else goes & ~(is_mine(way, kind, d) & (ends[way] == SPAN - 1))

    def give_back(way, kind, d, act):
        for h in range(2):

            @pl.when(gives(way, kind, d, h))
            def _():
                act(send_sum(way, kind, d, h))

    def sum_entry(way, kind, d, h):
        entry = FIRST[kind] + d
        goes = passes(way, kind, d)
        mine_here = is_mine(way, kind, d)
        comes = ends[way] < SPAN - 1 - h

        @pl.when(goes & (comes | ~mine_here))
        def _():
            send_sum(way, kind, d + 1, h).wait_recv()

        @pl.when(goes & comes & mine_here)
        def _():
            got = sums[way, entry, lines(h)].astype(f32) + own_part[way, lines(h)]
            sums[way, entry, lines(h)] = got.astype(bf16)

        @pl.when(goes & ~comes & mine_here)
        def _():
            sums[way, entry, lines(h)] = own_part[way, lines(h)].astype(bf16)

        @pl.when(gives(way, kind, d, h))
        def _():
            send_sum(way, kind, d, h).start()

    def return_kind(kind, d):
        for way in range(2):

            @pl.when(passes(way, kind, d) & is_mine(way, kind, d))
            def _():
                behind = d if way == 0 else ring - d
                own_share(way, FIRST[kind] + d, behind, own_part.at[way])

        for h in (1, 0):
            for way in range(2):
                sum_entry(way, kind, d, h)

    def place(n, value):
        choose = packing(n)
        for c in range(width // tile):
            cols = pl.ds(c * tile, tile)
            got = lax.dot_general(choose, value(cols), contract, preferred_element_type=f32)
            total[:, cols] += got

    def land(n, way, kind):
        whole, first = forwards(way, kind, 0)

        @pl.when(whole | first)
        def _():
            send_sum(way, kind, 1, 0).wait_recv()

        @pl.when(whole)
        def _():
            send_sum(way, kind, 1, 1).wait_recv()

        @pl.when(first)
        def _():
            sums[way, FIRST[kind], lines(1)] = jnp.zeros((room // 2, width), bf16)

        @pl.when(whole | first)
        def _():
            place(n, lambda cols: sums[way, FIRST[kind], :, cols])

    pick(far - 1)
    wait_back(0)
    own_share(0, HOME, 0, own_part.at[0])
    total[...] = stream[...].astype(f32)
    place(5, lambda cols: own_part[0, :, cols].astype(bf16))
    wait_back(far - 2)
    return_kind(1, LAST[1])
    serve(far - 1)

    def sum_step(i, _):
        r = far - i

        @pl.when((r >= 4) & (r <= far))
        def _():
            wait_back(r - 3)

        @pl.when(r == jnp.where((at == 0) | (at == SPAN - 1), far, far - 1))
        def _():
            wait_back(far - 1)

        return_kind(2, r + 1)

        @pl.when((r >= 1) & (r <= LAST[0]))
        def _():
            return_kind(0, r)

        @pl.when(r >= 3)
        def _():
            return_kind(1, r - 2)

        return 0

    lax.fori_loop(0, far + 1, sum_step, 0)
    for n, way, kind in ((1, 0, 1), (3, 1, 1), (0, 0, 0), (2, 1, 0), (4, 0, 2), (4, 1, 2)):
        land(n, way, kind)
    out_ref[...] = total[...].astype(bf16)

    def drain(d, _):
        for kind in range(3):
            for way in range(2):
                for h in range(2):
                    forward(way, kind, d, h, finish)

                @pl.when(d >= 1)
                def _():
                    give_back(way, kind, d, lambda copy: copy.wait_send())

        return 0

    lax.fori_loop(0, LAST[2] + 1, drain, 0)

    def drain_steps(n, _):
        for o in range(1, peers):
            exchange(picked, routed, pick_send, pick_recv, n, o).wait_send()
            exchange(made, back, back_send, back_recv, n, o).wait_send()
        return 0

    lax.fori_loop(0, far, drain_steps, 0)
    halo.wait_send()
    for h in range(2):
        for way in range(2):
            send_far(way, h).wait_send()
            send_near(way, h).wait_send()


def layer(query, key, value, cosines, sines, sinks, gain, ids, mix, residual, proj, gate, up, down):
    rows, width = residual.shape
    ring = lax.axis_size("sp") // CORES
    xs = lax.axis_size("tp")
    far = ring // 2
    peers = xs * CORES
    hidden = gate.shape[1]
    room = 2 * peers * CAP
    tile = min(512, width // 2)
    bf16, f32 = jnp.bfloat16, jnp.float32
    vmem = pl.BlockSpec(memory_space=pltpu.VMEM)
    smem = pl.BlockSpec(memory_space=pltpu.SMEM)
    hbm = pl.BlockSpec(memory_space=pl.ANY)
    slab = (far, peers, 2 * CAP, width)
    dma = pltpu.SemaphoreType.DMA
    return pl.pallas_call(
        functools.partial(expert_kernel, ring, xs, tile),
        out_shape=jax.ShapeDtypeStruct((rows, width), bf16),
        in_specs=[vmem] * 5 + [smem] + [vmem] * 3 + [hbm] * 5,
        out_specs=vmem,
        scratch_shapes=[
            pltpu.VMEM(query.shape, bf16),
            pltpu.VMEM((2 * HDIM, query.shape[0] + WINDOW), bf16),
            pltpu.VMEM((rows, width), bf16),
            pltpu.VMEM(proj.shape, bf16),
            pltpu.VMEM((3, rows, width), bf16),
            pltpu.VMEM((2, 2, rows // 2, width // 2), bf16),
            pltpu.VMEM((2, 2, rows, width // 2), bf16),
            pltpu.VMEM((rows, width), f32),
            pltpu.VMEM((rows, width), bf16),
            pltpu.VMEM((room, width), f32),
            pltpu.VMEM((8, rows), f32),
            pltpu.VMEM((2, ENTRIES, room, width), bf16),
            pltpu.VMEM((rows, width), f32),
            pltpu.VMEM((2, ENTRIES + 1, room, width), bf16),
            pltpu.VMEM((2, ENTRIES + 1, 8, rows), f32),
            pltpu.VMEM(slab, bf16),
            pltpu.VMEM(slab, bf16),
            pltpu.VMEM(slab, bf16),
            pltpu.VMEM(slab, bf16),
            pltpu.VMEM((2, room, width), f32),
            pltpu.VMEM((width, hidden), bf16),
            pltpu.VMEM((width, hidden), bf16),
            pltpu.VMEM((hidden, width), bf16),
            dma((5,)),
            dma((2, ENTRIES, 2)),
            dma((2, ENTRIES, 2)),
            dma((2, ENTRIES)),
            dma((2, ENTRIES)),
            dma((far, peers)),
            dma((far, peers)),
            dma((far, peers)),
            dma((far, peers)),
            dma((2, ENTRIES, 2)),
            dma((2, ENTRIES, 2)),
            dma,
            dma,
            dma((2, 2)),
            dma((2, 2)),
            dma((2, 2)),
            dma((2, 2)),
        ],
        compiler_params=pltpu.CompilerParams(
            collective_id=1, has_side_effects=True, vmem_limit_bytes=60 * 1024 * 1024
        ),
    )(query, key, value, cosines, sines, sinks, gain, ids, mix, residual, proj, gate, up, down)


def per_device(
    query_rows,
    key_rows,
    value_rows,
    sink_logits,
    residual,
    out_weight,
    norm_gain,
    gate_weight,
    up_weight,
    down_weight,
    routes,
    route_weight,
):
    tok_count = query_rows.shape[0]
    positions = lax.axis_index("sp") * tok_count + jnp.arange(tok_count, dtype=jnp.int32)
    half_dim = HDIM // 2
    inverse = rope_base ** (-jnp.arange(half_dim, dtype=jnp.float32) / half_dim)
    angles = positions.astype(jnp.float32)[None, :] * inverse[:, None]
    cosines = jnp.cos(angles)
    sines = jnp.sin(angles)
    return layer(
        query_rows,
        key_rows.T,
        value_rows.T,
        cosines,
        sines,
        sink_logits,
        norm_gain[None, :],
        routes.T,
        route_weight.T,
        residual,
        out_weight,
        gate_weight[0],
        up_weight[0],
        down_weight[0],
    )


def solution(mesh):
    in_specs = (
        P(("grp", "sp"), "tp"),
        P(("grp", "sp"), "tp"),
        P(("grp", "sp"), "tp"),
        P("tp"),
        P(("grp", "sp", "tp"), None),
        P("tp", None),
        P(),
        P(("sp", "tp"), None, None),
        P(("sp", "tp"), None, None),
        P(("sp", "tp"), None, None),
        P(("grp", "sp", "tp"), None),
        P(("grp", "sp", "tp"), None),
    )
    out_specs = P(("grp", "sp", "tp"), None)
    return jax.shard_map(
        per_device, mesh=mesh, in_specs=in_specs, out_specs=out_specs, check_vma=False
    )
```

```python
import functools

import jax
import jax.numpy as jnp
from jax import lax
from jax.experimental import pallas as pl
from jax.experimental.pallas import tpu as pltpu
from jax.sharding import PartitionSpec as P

MESH_ID = pl.DeviceIdType.MESH
HDIM = 64
WINDOW = 128
CAP = 4
CORES = 2
EXPERTS_PER_GROUP = 32
SPAN = 4
FIRST = (0, 4, 12)
LAST = (3, 7, 9)
ENTRIES = 22
HOME = 22


rope_base = 10000.0
norm_eps = 1e-06


def expert_kernel(
    ring,
    xs,
    tile,
    query_ref,
    key_ref,
    value_ref,
    cos_ref,
    sin_ref,
    sink_ref,
    gain_ref,
    ids_ref,
    mix_ref,
    residual_hbm,
    proj_hbm,
    gate_hbm,
    up_hbm,
    down_hbm,
    out_ref,
    rot_q,
    keys_values,
    residual,
    proj_w,
    shares,
    far_in,
    near_in,
    own_share_sum,
    stream,
    unscaled,
    places,
    sums,
    total,
    pool,
    pool_meta,
    picked,
    routed,
    made,
    back,
    own_part,
    gate_w,
    up_w,
    down_w,
    weight_sem,
    pool_send,
    pool_recv,
    meta_send,
    meta_recv,
    pick_send,
    pick_recv,
    back_send,
    back_recv,
    sum_send,
    sum_recv,
    halo_send,
    halo_recv,
    far_send,
    far_recv,
    near_send,
    near_recv,
):
    f32, bf16 = jnp.float32, jnp.bfloat16
    rows, width = residual.shape
    half = rows // 2
    far = ring // 2
    peers = xs * CORES
    sp, tp = lax.axis_index("sp"), lax.axis_index("tp")
    core = lax.rem(sp, CORES)
    z = sp // CORES
    mine = core * xs + tp
    nxt = {"sp": lax.rem(sp + CORES, ring * CORES)}
    prv = {"sp": lax.rem(sp + (ring - 1) * CORES, ring * CORES)}

    far_first = sorted(range(1, peers), key=lambda o: -min(o % xs, xs - o % xs))

    def peer(offset):
        u = lax.rem(mine + offset, peers)
        return u, {"sp": z * CORES + u // xs, "tp": lax.rem(u, xs)}

    loads = [
        pltpu.make_async_copy(src, dst, weight_sem.at[i])
        for i, (src, dst) in enumerate(
            (
                (proj_hbm, proj_w),
                (residual_hbm, residual),
                (gate_hbm, gate_w),
                (up_hbm, up_w),
                (down_hbm, down_w),
            )
        )
    ]
    for load in loads:
        load.start()

    barrier = pltpu.get_barrier_semaphore()
    pl.semaphore_signal(barrier, inc=1, device_id=nxt, device_id_type=MESH_ID)
    pl.semaphore_signal(barrier, inc=1, device_id=prv, device_id_type=MESH_ID)
    total_sp = ring * CORES
    after = {"sp": lax.rem(sp + 1, total_sp)}
    across = {"sp": lax.rem(sp + jnp.where(core == 1, 1, total_sp - 1), total_sp)}
    pl.semaphore_signal(barrier, inc=1, device_id=across, device_id_type=MESH_ID)
    for o in range(1, peers):
        pl.semaphore_signal(barrier, inc=1, device_id=peer(o)[1], device_id_type=MESH_ID)

    lane = lax.broadcasted_iota(jnp.int32, (query_ref.shape[1],) * 2, 1)
    line = lax.broadcasted_iota(jnp.int32, (query_ref.shape[1],) * 2, 0)
    low = lax.rem(lane, HDIM) < HDIM // 2
    turn = jnp.where(low & (line == lane + HDIM // 2), -1.0, 0.0)
    turn = (turn + jnp.where((~low) & (line == lane - HDIM // 2), 1.0, 0.0)).astype(bf16)

    def rotated(x, cosines, sines):
        n = x.shape[1]
        swapped = jnp.dot(x, turn[:n, :n], preferred_element_type=f32)
        return (x.astype(f32) * cosines + swapped * sines).astype(bf16)

    tok = query_ref.shape[0]
    k_low = key_ref[0 : HDIM // 2].astype(f32)
    k_high = key_ref[HDIM // 2 :].astype(f32)
    turned_low = k_low * cos_ref[...] - k_high * sin_ref[...]
    turned_high = k_high * cos_ref[...] + k_low * sin_ref[...]
    turned_k = jnp.concatenate([turned_low, turned_high], axis=0)
    keys_values[0:HDIM, WINDOW:] = turned_k.astype(bf16)
    keys_values[HDIM:, WINDOW:] = value_ref[...]
    pl.semaphore_wait(barrier, peers + 2)
    halo = pltpu.make_async_remote_copy(
        src_ref=keys_values.at[:, pl.ds(tok, WINDOW)],
        dst_ref=keys_values.at[:, pl.ds(0, WINDOW)],
        send_sem=halo_send,
        recv_sem=halo_recv,
        device_id=after,
        device_id_type=MESH_ID,
    )
    halo.start()
    repeats = 128 // (HDIM // 2)
    cosines = jnp.concatenate([cos_ref[...]] * repeats, axis=0).T
    sines = jnp.concatenate([sin_ref[...]] * repeats, axis=0).T
    for c in range(query_ref.shape[1] // 128):
        cols = pl.ds(c * 128, 128)
        rot_q[:, cols] = rotated(query_ref[:, cols], cosines, sines)

    def part(h):
        return pl.ds(h * half, half)

    def side_cols(h):
        return pl.ds(h * (width // 2), width // 2)

    block, at = z // SPAN, lax.rem(z, SPAN)
    opposite_way = jnp.where(at >= SPAN // 2, 0, 1)
    ends = (at, SPAN - 1 - at)
    onward = (nxt, prv)
    room = 2 * peers * CAP

    def origin(way, d):
        i = lax.rem(ends[way] - d + 3 * SPAN, SPAN)
        return i, (d + i - ends[way]) // SPAN

    def passes(way, kind, d):
        i, crossed = origin(way, d)
        there = (d <= LAST[kind]) & (kind >= crossed)
        return there & (i >= SPAN // 2) if kind == 2 else there

    def is_mine(way, kind, d):
        return origin(way, d)[1] == kind

    def send_chunk(way, kind, d, count, h):
        entry = FIRST[kind] + d
        return pltpu.make_async_remote_copy(
            src_ref=pool.at[way, entry, pl.ds(0, count), side_cols(h)],
            dst_ref=pool.at[way, entry + 1, pl.ds(0, count), side_cols(h)],
            send_sem=pool_send.at[way, entry, h],
            recv_sem=pool_recv.at[way, entry + 1, h],
            device_id=onward[way],
            device_id_type=MESH_ID,
        )

    def send_meta(way, kind, d):
        entry = FIRST[kind] + d
        return pltpu.make_async_remote_copy(
            src_ref=pool_meta.at[way, entry],
            dst_ref=pool_meta.at[way, entry + 1],
            send_sem=meta_send.at[way, entry],
            recv_sem=meta_recv.at[way, entry + 1],
            device_id=onward[way],
            device_id_type=MESH_ID,
        )

    def forwards(way, kind, d):
        goes = passes(way, kind, d)
        mine_here = is_mine(way, kind, d)
        whole = goes & jnp.where(mine_here, ends[way] < SPAN - 2, True)
        return whole, goes & mine_here & (ends[way] == SPAN - 2)

    def forward(way, kind, d, h, act):
        whole, first = forwards(way, kind, d)

        @pl.when(whole)
        def _():
            act(send_chunk(way, kind, d, room, h))

        @pl.when(first)
        def _():
            act(send_chunk(way, kind, d, room // 2, h))

        if h == 1:

            @pl.when(whole | first)
            def _():
                act(send_meta(way, kind, d))

    def begin(copy):
        copy.start()

    def finish(copy):
        copy.wait_send()

    def receive(way, kind, d, h):
        goes = passes(way, kind, d)
        short = is_mine(way, kind, d) & (ends[way] == SPAN - 1)

        @pl.when(goes & ~short)
        def _():
            send_chunk(way, kind, d - 1, room, h).wait_recv()

        @pl.when(goes & short)
        def _():
            send_chunk(way, kind, d - 1, room // 2, h).wait_recv()

        if h == 1:

            @pl.when(goes)
            def _():
                send_meta(way, kind, d - 1).wait_recv()

            @pl.when(goes & short)
            def _():
                pool[way, FIRST[kind] + d, pl.ds(room // 2, room // 2)] = jnp.zeros(
                    (room // 2, width), bf16
                )

    q_at = lax.broadcasted_iota(jnp.int32, (WINDOW, 2 * WINDOW), 0)
    k_at = lax.broadcasted_iota(jnp.int32, (WINDOW, 2 * WINDOW), 1)
    reach = q_at + WINDOW - k_at

    def projected(rank):

        @pl.when(rank == 0)
        def _():
            halo.wait_recv()

        start = pl.multiple_of(rank * WINDOW, WINDOW)
        first = start + sp * tok
        allowed = (reach >= 0) & (reach < WINDOW) & (k_at + first >= WINDOW)
        k = keys_values[0:HDIM, pl.ds(start, 2 * WINDOW)]
        v = keys_values[HDIM:, pl.ds(start, 2 * WINDOW)]
        q = rot_q[pl.ds(start, WINDOW), :]
        heads = []
        for h in range(q.shape[1] // HDIM):
            qh = q[:, h * HDIM : (h + 1) * HDIM]
            s = jnp.dot(qh, k, preferred_element_type=f32)
            s = jnp.where(allowed, s * HDIM ** (-0.5), -jnp.inf)
            sink = sink_ref[h]
            top = jnp.maximum(jnp.max(s, axis=1, keepdims=True), sink)
            e = jnp.exp(s - top)
            below = jnp.sum(e, axis=1, keepdims=True) + jnp.exp(sink - top)
            p = (e / below).astype(bf16)
            seen = lax.dot_general(p, v, (((1,), (1,)), ((), ())), preferred_element_type=f32)
            heads.append(seen.astype(bf16))
        att = jnp.concatenate(heads, axis=1)
        for c in range(width // tile):
            cols = pl.ds(c * tile, tile)
            yield cols, jnp.dot(att, proj_w[:, cols], preferred_element_type=f32)

    def beside(step):
        return {"tp": lax.rem(tp + step + xs, xs)}

    def send_far(way, h):
        return pltpu.make_async_remote_copy(
            src_ref=shares.at[2, part(way), side_cols(h)],
            dst_ref=far_in.at[way, h],
            send_sem=far_send.at[way, h],
            recv_sem=far_recv.at[way, h],
            device_id=beside(1 - 2 * way),
            device_id_type=MESH_ID,
        )

    def send_near(way, h):
        return pltpu.make_async_remote_copy(
            src_ref=shares.at[way, :, side_cols(h)],
            dst_ref=near_in.at[way, h],
            send_sem=near_send.at[way, h],
            recv_sem=near_recv.at[way, h],
            device_id=beside(1 - 2 * way),
            device_id_type=MESH_ID,
        )

    loads[0].wait()
    per_side = width // 2 // tile
    for c, (cols, y) in enumerate(projected(lax.rem(tp + 2, xs))):
        shares[2, :, cols] = y.astype(bf16)
        if (c + 1) % per_side == 0:
            for way in range(2):
                send_far(way, c // per_side).start()
    for way in range(2):
        for c, (cols, y) in enumerate(projected(lax.rem(tp + 1 - 2 * way + xs, xs))):
            own_share_sum[:, cols] = y
            if (c + 1) % per_side == 0:
                h = c // per_side
                send_far(way, h).wait_recv()
                alone, joint, side = part(1 - way), part(way), side_cols(h)
                shares[way, alone, side] = own_share_sum[alone, side].astype(bf16)
                joined = own_share_sum[joint, side] + far_in[way, h].astype(f32)
                shares[way, joint, side] = joined.astype(bf16)
                send_near(way, h).start()
    for cols, y in projected(tp):
        own_share_sum[:, cols] = y
    loads[1].wait()

    def own_cols(h):
        for way in range(2):
            send_near(way, h).wait_recv()
        cols = side_cols(h)
        got = near_in[0, h].astype(f32) + near_in[1, h].astype(f32)
        x = residual[:, cols].astype(f32) + (own_share_sum[:, cols] + got)
        stream[:, cols] = x.astype(bf16)

    ids = ids_ref[...]
    expert_at = lax.broadcasted_iota(jnp.int32, (ring * peers, rows), 0)
    token_row = lax.broadcasted_iota(jnp.int32, (rows, rows), 0)
    token_col = lax.broadcasted_iota(jnp.int32, (rows, rows), 1)
    ahead = (token_row < token_col).astype(f32).astype(bf16)
    named = [(expert_at == ids[c : c + 1]).astype(f32) for c in range(2)]
    earlier = jnp.dot((named[0] + named[1]).astype(bf16), ahead, preferred_element_type=f32)
    ranks = [jnp.sum(n * earlier, axis=0, keepdims=True) for n in named]
    group = ids[0:1] // EXPERTS_PER_GROUP
    chip = [ids[c : c + 1] // peers for c in range(2)]
    spot = [lax.rem(c, SPAN) for c in chip]
    blocks = ring // SPAN
    apart = lax.rem(group - block + blocks, blocks)
    top = [(spot[0] == SPAN - 1) | (spot[1] == SPAN - 1), (spot[0] == 0) | (spot[1] == 0)]
    beyond = [(spot[0] > at) | (spot[1] > at), (spot[0] < at) | (spot[1] < at)]
    here = (chip[0] == z) | (chip[1] == z)
    joins = [
        (apart == 0) & beyond[0],
        apart == 1,
        (apart == 0) & beyond[1],
        apart == blocks - 1,
        apart == 2,
        here,
    ]
    joins = [x.astype(f32) for x in joins]
    top = [x.astype(f32) for x in top]
    leads = [top[0], top[0], top[1], top[1], jnp.where(at >= SPAN // 2, top[0], top[1]), top[0]]
    pack_row = lax.broadcasted_iota(jnp.int32, (8, rows), 0)
    lead, rest = jnp.zeros((8, rows), f32), jnp.zeros((8, rows), f32)
    for n in range(6):
        lead = jnp.where(pack_row == n, joins[n] * leads[n], lead)
        rest = jnp.where(pack_row == n, joins[n] * (1.0 - leads[n]), rest)
    lead_rank = jnp.dot(lead.astype(bf16), ahead, preferred_element_type=f32)
    rest_rank = jnp.dot(rest.astype(bf16), ahead, preferred_element_type=f32)
    rest_rank += jnp.sum(lead, axis=1, keepdims=True)
    places[...] = jnp.where(lead > 0, lead_rank, jnp.where(rest > 0, rest_rank, -1.0))
    mix = mix_ref[...]
    mix_high = mix.astype(bf16).astype(f32)
    mix_low = mix - mix_high
    facts_row = lax.broadcasted_iota(jnp.int32, (16, rows), 0)
    facts = jnp.where(facts_row == 8, 1.0, 0.0)
    known = [ids[0:1].astype(f32), ids[1:2].astype(f32), ranks[0], ranks[1]]
    known += [mix_high[0:1], mix_high[1:2], mix_low[0:1], mix_low[1:2]]
    for n in range(8):
        facts = jnp.where(facts_row == n, known[n], facts)
    facts = facts.astype(bf16)
    chunk_row = lax.broadcasted_iota(jnp.int32, (room, rows), 0).astype(f32)

    def packing(n):
        return (chunk_row == places[n : n + 1, :]).astype(f32).astype(bf16)

    def pack(n, way, entry, h):
        choose = packing(n)
        for c in range(h * per_side, (h + 1) * per_side):
            cols = pl.ds(c * tile, tile)
            got = jnp.dot(choose, stream[:, cols], preferred_element_type=f32)
            pool[way, entry, :, cols] = got.astype(bf16)

    def pack_meta(n, way, entry):
        got = lax.dot_general(
            facts, packing(n), (((1,), (1,)), ((), ())), preferred_element_type=f32
        )
        out_row = lax.broadcasted_iota(jnp.int32, (8, room), 0)
        found = got[8:9] > 0
        out = jnp.where(out_row == 0, jnp.where(found, got[0:1] * CAP + got[2:3], -1.0), 0.0)
        out = jnp.where(out_row == 1, jnp.where(found, got[1:2] * CAP + got[3:4], -1.0), out)
        out = jnp.where(out_row == 2, got[4:5] + got[6:7], out)
        out = jnp.where(out_row == 3, got[5:6] + got[7:8], out)
        pool_meta[way, entry] = jnp.concatenate([out, jnp.zeros_like(out)], axis=1)

    packs = ((4, opposite_way, 2), (1, 0, 1), (3, 1, 1), (0, 0, 0), (2, 1, 0))
    for n, way, kind in packs:
        pack_meta(n, way, FIRST[kind])
    pack_meta(5, 0, HOME)

    for h in range(2):
        own_cols(h)
        for n, way, kind in packs:
            pack(n, way, FIRST[kind], h)
            for w in range(2) if kind == 2 else (way,):
                forward(w, kind, 0, h, begin)
        pack(5, 0, HOME, h)

    row_id = lax.broadcasted_iota(jnp.int32, (room, room), 0)
    local_code = (row_id // (2 * CAP)) * CAP + lax.rem(row_id, CAP)
    which_half = lax.rem(row_id, 2 * CAP) // CAP
    base = z * (peers * CAP)

    def paired(back):
        late = (at == SPAN - 1) & ((back == far - 1) | (back == far + 1))
        return jnp.where(late, ring - back, back)

    def locate(back):
        other = back > at + SPAN + SPAN // 2
        d = jnp.where(other, ring - back, back)
        end = jnp.where(other, ends[1], ends[0])
        i = lax.rem(end - d + 3 * SPAN, SPAN)
        crossed = (d + i - end) // SPAN
        first = jnp.where(crossed == 0, FIRST[0], jnp.where(crossed == 1, FIRST[1], FIRST[2]))
        entry = jnp.where(back == 0, HOME, first + d)
        return jnp.where(other, 1, 0), entry

    def matches(way, entry, side):
        code = jnp.where(which_half == side, local_code + base, -2).astype(f32)
        m = pool_meta[way, entry][:, 0:room]
        return code == m[0:1, :], code == m[1:2, :], m

    def pick_of(way, entry, side):
        first_hit, second_hit, _ = matches(way, entry, side)
        return (first_hit | second_hit).astype(f32).astype(bf16)

    def weights_of(way, entry, side):
        first_hit, second_hit, m = matches(way, entry, side)
        w = jnp.where(first_hit, m[2:3, :], 0.0) + jnp.where(second_hit, m[3:4, :], 0.0)
        high = w.astype(bf16)
        return high, (w - high.astype(f32)).astype(bf16)

    def exchange(src, dst, sends, recvs, step, offset):
        u, where = peer(offset)
        return pltpu.make_async_remote_copy(
            src_ref=src.at[step, u],
            dst_ref=dst.at[step, mine],
            send_sem=sends.at[step, offset],
            recv_sem=recvs.at[step, offset],
            device_id=where,
            device_id_type=MESH_ID,
        )

    def pick(step):
        a, b = locate(paired(step)), locate(paired(ring - 1 - step))
        one_a, one_b = pick_of(*a, 0), pick_of(*b, 1)
        square = jnp.zeros((room, 1), f32)
        for c in range(width // tile):
            cols = pl.ds(c * tile, tile)
            got = jnp.dot(one_a, pool[a[0], a[1], :, cols], preferred_element_type=f32)
            got += jnp.dot(one_b, pool[b[0], b[1], :, cols], preferred_element_type=f32)
            square += jnp.sum(got * got, axis=1, keepdims=True)
            unscaled[:, cols] = got
        scale = lax.rsqrt(square / width + norm_eps)
        for c in range(width // tile):
            cols = pl.ds(c * tile, tile)
            got = (unscaled[:, cols] * scale * gain_ref[:, cols]).astype(bf16)
            picked[step, :, :, cols] = got.reshape(peers, 2 * CAP, tile)
        for o in far_first:
            exchange(picked, routed, pick_send, pick_recv, step, o).start()
        routed[step, mine] = picked[step, mine]

    def serve(step):
        for o in range(1, peers):
            exchange(picked, routed, pick_send, pick_recv, step, o).wait_recv()
        x = routed[step].reshape(peers * 2 * CAP, width)
        g = jnp.dot(x, gate_w[...], preferred_element_type=f32)
        u = jnp.dot(x, up_w[...], preferred_element_type=f32)
        hidden = (g * (1.0 / (1.0 + jnp.exp(-g))) * u).astype(bf16)
        for c in range(width // tile):
            cols = pl.ds(c * tile, tile)
            y = jnp.dot(hidden, down_w[:, cols], preferred_element_type=f32)
            made[step, :, :, cols] = y.astype(bf16).reshape(peers, 2 * CAP, tile)
        for o in far_first:
            exchange(made, back, back_send, back_recv, step, o).start()
        back[step, mine] = made[step, mine]

    def ring_step(d, _):
        for kind in (2, 1, 0):
            for h in range(2):
                for way in range(2):
                    receive(way, kind, d, h)
                    forward(way, kind, d, h, begin)

        @pl.when(d <= far - 1)
        def _():
            pick(d - 1)

        @pl.when((d >= 2) & (d <= far))
        def _():
            serve(d - 2)

        return 0

    for load in loads[2:]:
        load.wait()
    lax.fori_loop(1, LAST[2] + 1, ring_step, 0)
    contract = (((0,), (0,)), ((), ()))

    def wait_back(step):
        for o in range(1, peers):
            exchange(made, back, back_send, back_recv, step, o).wait_recv()

    def own_share(way, entry, behind, dst):
        place_of = paired(behind)
        side = jnp.where(place_of >= far, 1, 0)
        step = jnp.where(place_of >= far, ring - 1 - place_of, place_of)
        high, low = weights_of(way, entry, side)
        w = jnp.concatenate([high, low], axis=0)
        for c in range(width // tile):
            cols = pl.ds(c * tile, tile)
            y = back[step, :, :, cols].reshape(room, tile)
            y = jnp.concatenate([y, y], axis=0)
            dst[:, cols] = lax.dot_general(w, y, contract, preferred_element_type=f32)

    def lines(h):
        return pl.ds(h * (room // 2), room // 2)

    def send_sum(way, kind, d, h):
        entry = FIRST[kind] + d
        return pltpu.make_async_remote_copy(
            src_ref=sums.at[way, entry, lines(h)],
            dst_ref=sums.at[way, entry - 1, lines(h)],
            send_sem=sum_send.at[way, entry, h],
            recv_sem=sum_recv.at[way, entry - 1, h],
            device_id=onward[1 - way],
            device_id_type=MESH_ID,
        )

    def gives(way, kind, d, h):
        goes = passes(way, kind, d)
        return goes if h == 0 else goes & ~(is_mine(way, kind, d) & (ends[way] == SPAN - 1))

    def give_back(way, kind, d, act):
        for h in range(2):

            @pl.when(gives(way, kind, d, h))
            def _():
                act(send_sum(way, kind, d, h))

    def sum_entry(way, kind, d, h):
        entry = FIRST[kind] + d
        goes = passes(way, kind, d)
        mine_here = is_mine(way, kind, d)
        comes = ends[way] < SPAN - 1 - h

        @pl.when(goes & (comes | ~mine_here))
        def _():
            send_sum(way, kind, d + 1, h).wait_recv()

        @pl.when(goes & comes & mine_here)
        def _():
            got = sums[way, entry, lines(h)].astype(f32) + own_part[way, lines(h)]
            sums[way, entry, lines(h)] = got.astype(bf16)

        @pl.when(goes & ~comes & mine_here)
        def _():
            sums[way, entry, lines(h)] = own_part[way, lines(h)].astype(bf16)

        @pl.when(gives(way, kind, d, h))
        def _():
            send_sum(way, kind, d, h).start()

    def return_kind(kind, d):
        for way in range(2):

            @pl.when(passes(way, kind, d) & is_mine(way, kind, d))
            def _():
                behind = d if way == 0 else ring - d
                own_share(way, FIRST[kind] + d, behind, own_part.at[way])

        for h in (1, 0):
            for way in range(2):
                sum_entry(way, kind, d, h)

    def place(n, value):
        choose = packing(n)
        for c in range(width // tile):
            cols = pl.ds(c * tile, tile)
            got = lax.dot_general(choose, value(cols), contract, preferred_element_type=f32)
            total[:, cols] += got

    def land(n, way, kind):
        whole, first = forwards(way, kind, 0)

        @pl.when(whole | first)
        def _():
            send_sum(way, kind, 1, 0).wait_recv()

        @pl.when(whole)
        def _():
            send_sum(way, kind, 1, 1).wait_recv()

        @pl.when(first)
        def _():
            sums[way, FIRST[kind], lines(1)] = jnp.zeros((room // 2, width), bf16)

        @pl.when(whole | first)
        def _():
            place(n, lambda cols: sums[way, FIRST[kind], :, cols])

    pick(far - 1)
    wait_back(0)
    own_share(0, HOME, 0, own_part.at[0])
    total[...] = stream[...].astype(f32)
    place(5, lambda cols: own_part[0, :, cols].astype(bf16))
    wait_back(far - 2)
    return_kind(1, LAST[1])
    serve(far - 1)

    def sum_step(i, _):
        r = far - i

        @pl.when((r >= 4) & (r <= far))
        def _():
            wait_back(r - 3)

        @pl.when(r == jnp.where((at == 0) | (at == SPAN - 1), far, far - 1))
        def _():
            wait_back(far - 1)

        return_kind(2, r + 1)

        @pl.when((r >= 1) & (r <= LAST[0]))
        def _():
            return_kind(0, r)

        @pl.when(r >= 3)
        def _():
            return_kind(1, r - 2)

        return 0

    lax.fori_loop(0, far + 1, sum_step, 0)
    for n, way, kind in ((1, 0, 1), (3, 1, 1), (0, 0, 0), (2, 1, 0), (4, 0, 2), (4, 1, 2)):
        land(n, way, kind)
    out_ref[...] = total[...].astype(bf16)

    def drain(d, _):
        for kind in range(3):
            for way in range(2):
                for h in range(2):
                    forward(way, kind, d, h, finish)

                @pl.when(d >= 1)
                def _():
                    give_back(way, kind, d, lambda copy: copy.wait_send())

        return 0

    lax.fori_loop(0, LAST[2] + 1, drain, 0)

    def drain_steps(n, _):
        for o in range(1, peers):
            exchange(picked, routed, pick_send, pick_recv, n, o).wait_send()
            exchange(made, back, back_send, back_recv, n, o).wait_send()
        return 0

    lax.fori_loop(0, far, drain_steps, 0)
    halo.wait_send()
    for h in range(2):
        for way in range(2):
            send_far(way, h).wait_send()
            send_near(way, h).wait_send()


def layer(query, key, value, cosines, sines, sinks, gain, ids, mix, residual, proj, gate, up, down):
    rows, width = residual.shape
    ring = lax.axis_size("sp") // CORES
    xs = lax.axis_size("tp")
    far = ring // 2
    peers = xs * CORES
    hidden = gate.shape[1]
    room = 2 * peers * CAP
    tile = min(512, width // 2)
    bf16, f32 = jnp.bfloat16, jnp.float32
    vmem = pl.BlockSpec(memory_space=pltpu.VMEM)
    smem = pl.BlockSpec(memory_space=pltpu.SMEM)
    hbm = pl.BlockSpec(memory_space=pl.ANY)
    slab = (far, peers, 2 * CAP, width)
    dma = pltpu.SemaphoreType.DMA
    return pl.pallas_call(
        functools.partial(expert_kernel, ring, xs, tile),
        out_shape=jax.ShapeDtypeStruct((rows, width), bf16),
        in_specs=[vmem] * 5 + [smem] + [vmem] * 3 + [hbm] * 5,
        out_specs=vmem,
        scratch_shapes=[
            pltpu.VMEM(query.shape, bf16),
            pltpu.VMEM((2 * HDIM, query.shape[0] + WINDOW), bf16),
            pltpu.VMEM((rows, width), bf16),
            pltpu.VMEM(proj.shape, bf16),
            pltpu.VMEM((3, rows, width), bf16),
            pltpu.VMEM((2, 2, rows // 2, width // 2), bf16),
            pltpu.VMEM((2, 2, rows, width // 2), bf16),
            pltpu.VMEM((rows, width), f32),
            pltpu.VMEM((rows, width), bf16),
            pltpu.VMEM((room, width), f32),
            pltpu.VMEM((8, rows), f32),
            pltpu.VMEM((2, ENTRIES, room, width), bf16),
            pltpu.VMEM((rows, width), f32),
            pltpu.VMEM((2, ENTRIES + 1, room, width), bf16),
            pltpu.VMEM((2, ENTRIES + 1, 8, rows), f32),
            pltpu.VMEM(slab, bf16),
            pltpu.VMEM(slab, bf16),
            pltpu.VMEM(slab, bf16),
            pltpu.VMEM(slab, bf16),
            pltpu.VMEM((2, room, width), f32),
            pltpu.VMEM((width, hidden), bf16),
            pltpu.VMEM((width, hidden), bf16),
            pltpu.VMEM((hidden, width), bf16),
            dma((5,)),
            dma((2, ENTRIES, 2)),
            dma((2, ENTRIES, 2)),
            dma((2, ENTRIES)),
            dma((2, ENTRIES)),
            dma((far, peers)),
            dma((far, peers)),
            dma((far, peers)),
            dma((far, peers)),
            dma((2, ENTRIES, 2)),
            dma((2, ENTRIES, 2)),
            dma,
            dma,
            dma((2, 2)),
            dma((2, 2)),
            dma((2, 2)),
            dma((2, 2)),
        ],
        compiler_params=pltpu.CompilerParams(
            collective_id=1, has_side_effects=True, vmem_limit_bytes=60 * 1024 * 1024
        ),
    )(query, key, value, cosines, sines, sinks, gain, ids, mix, residual, proj, gate, up, down)


def per_device(
    query_rows,
    key_rows,
    value_rows,
    sink_logits,
    residual,
    out_weight,
    norm_gain,
    gate_weight,
    up_weight,
    down_weight,
    routes,
    route_weight,
):
    tok_count = query_rows.shape[0]
    positions = lax.axis_index("sp") * tok_count + jnp.arange(tok_count, dtype=jnp.int32)
    half_dim = HDIM // 2
    inverse = rope_base ** (-jnp.arange(half_dim, dtype=jnp.float32) / half_dim)
    angles = positions.astype(jnp.float32)[None, :] * inverse[:, None]
    cosines = jnp.cos(angles)
    sines = jnp.sin(angles)
    return layer(
        query_rows,
        key_rows.T,
        value_rows.T,
        cosines,
        sines,
        sink_logits,
        norm_gain[None, :],
        routes.T,
        route_weight.T,
        residual,
        out_weight,
        gate_weight[0],
        up_weight[0],
        down_weight[0],
    )


def solution(mesh):
    in_specs = (
        P(("grp", "sp"), "tp"),
        P(("grp", "sp"), "tp"),
        P(("grp", "sp"), "tp"),
        P("tp"),
        P(("grp", "sp", "tp"), None),
        P("tp", None),
        P(),
        P(("sp", "tp"), None, None),
        P(("sp", "tp"), None, None),
        P(("sp", "tp"), None, None),
        P(("grp", "sp", "tp"), None),
        P(("grp", "sp", "tp"), None),
    )
    out_specs = P(("grp", "sp", "tp"), None)
    return jax.shard_map(
        per_device, mesh=mesh, in_specs=in_specs, out_specs=out_specs, check_vma=False
    )
```
